32 devices in a mesh: sp: 8 (over z, x), tp: 4 (over y, core).
Axes of the slice: x: 2, y: 2, z: 4, core: 2. Of those that a mesh axis runs over, the one named last changes fastest.
Arguments:
- query_proj: bfloat16 [4096, 1024], P('sp', 'tp'), may hold values from -6 to 6
- projected_keys: bfloat16 [4096, 512], P('sp', 'tp'), may hold values from -6 to 6
- projected_values: bfloat16 [4096, 512], P('sp', 'tp'), may hold values from -6 to 6
- residual: bfloat16 [4096, 2048], P(('sp', 'tp')), may hold values from -6 to 6
- out_weight: bfloat16 [1024, 2048], replicated, may hold values from -0.1875 to 0.1875
- mix_gain: float32 [2048], replicated, may hold values from 0.1 to 1.9
- norm_gain: float32 [2048], replicated, may hold values from 0.1 to 1.9
- route_expert: int32 [4096, 2], P(('sp', 'tp')), may hold values from 0 to 31, all different within a row; in each aligned block of 128 rows (0 to 127, 128 to 255, ...) at most 16 rows name the same one
- route_weight: float32 [4096, 2], P(('sp', 'tp')), may hold values from 0.2 to 1
- expert_gate: bfloat16 [32, 2048, 1024], P(('sp', 'tp')), may hold values from -0.125 to 0.125
- expert_up: bfloat16 [32, 2048, 1024], P(('sp', 'tp')), may hold values from -0.125 to 0.125
- expert_down: bfloat16 [32, 1024, 2048], P(('sp', 'tp')), may hold values from -0.1875 to 0.1875
Outputs:
- output: bfloat16 [4096, 2048], P(('sp', 'tp'))
The draws below stay inside these ranges and needn't reach their ends.
Inputs may be any that keep to these rules, and one draw needn't show every extreme that they name: `route_expert`: each row names 2 different experts. The rows of one device (aligned blocks of 128 rows) name any one expert at most 16 times, and in some blocks some expert is named exactly 16 times.
All inputs are finite; a program needn't handle non-finite values.
Results may differ from the reference program's by a relative error of at most 0.015.
Values may be sent and summed in bfloat16 or wider, within the bound.
No kernel may reach another device: no remote copies, remote signals or barrier semaphores. Data moves between devices by JAX's collectives and lax.ppermute only.
A program may use at most 128 MiB of HBM per device.

```python
import math
import jax
import jax.numpy as jnp
import numpy as np
from jax import lax

D = 2048
QUERY_HEADS = 16
KEY_VALUE_HEADS = 8
HEAD_SIZE = 64
FF = 1024
TOP = 2
GRID_W = 64
ROWS = 128
SEQUENCE_TOKENS = 4096
EXPERTS = 32
CAP = 16
N_SP = 8
N_TP = 4


def block_levels(own_key, shape, cuts, low, top_value):
    def one(dim, shards_of):
        heights = jax.random.uniform(jax.random.fold_in(jax.random.fold_in(own_key, 6), dim), (shards_of,), jnp.float32, low / len(cuts), top_value / len(cuts))
        return jnp.repeat(jnp.exp(heights), shape[dim] // shards_of).reshape((-1,) + (1,) * (len(shape) - dim - 1))

    gain = one(*cuts[0])
    for cut in cuts[1:]:
        gain = gain * one(*cut)
    return gain


def deal_out(key, own, number, rows, count, top, bound, skew):
    ranking = jax.random.permutation(key, count)
    heavy_load, common = shares(count, rows * top, bound, skew, True), shares(count, rows * top, bound, skew, False)
    places = jnp.arange(count)

    def named(lengths, rotation):
        used = int((lengths > 0).sum())
        fixed = max(1, used // 4)
        moved = fixed + (places - fixed + rotation * (used - fixed)) % max(1, count - fixed)
        return jnp.zeros((count,), jnp.int32).at[ranking[jnp.where(places < fixed, places, moved)]].set(jnp.asarray(lengths, jnp.int32))

    lengths = jnp.where(number % 4 == 0, named(heavy_load, number // 4), named(common, number - number // 4 - 1))
    mixed = jax.random.permutation(jax.random.fold_in(own, 3), count)
    source_of, taker = mixed[0:count // 2 * 2:2], mixed[1:count // 2 * 2:2]
    margin = jnp.minimum(lengths[source_of] - 1, bound - lengths[taker]) // 2
    margin = jnp.where((source_of == ranking[0]) | (taker == ranking[0]) | (lengths[taker] == 0), 0, jnp.maximum(margin, 0))
    moved = jax.random.randint(jax.random.fold_in(own, 4), (count // 2,), 0, 1 << 20) % (margin + 1)
    lengths = lengths.at[source_of].add(-moved).at[taker].add(moved)
    labels = jnp.searchsorted(jnp.cumsum(lengths), jnp.arange(rows * top), side="right").astype(jnp.int32)
    grid = labels.reshape(top, rows).T
    grid = grid[jax.random.permutation(jax.random.fold_in(own, 1), rows)]
    rotation = jax.random.randint(jax.random.fold_in(own, 2), (rows, 1), 0, top)
    return jnp.take_along_axis(grid, (jnp.arange(top)[None, :] + rotation) % top, axis=1)


def shares(amount, total, reach, slope, full):
    weights = [(1 << 20) // math.isqrt(grade ** slope) + 1 for grade in range(1, amount + 1)]
    largest = reach if full else min(reach, max(-(-total // amount), total * weights[0] // sum(weights)))
    least = 1 if total - largest >= amount - 1 else 0
    given, spare = [largest] + [least] * (amount - 1), total - largest - least * (amount - 1)
    while spare > 0:
        candidates = [i for i in range(1, amount) if given[i] < largest] or [i for i in range(1, amount) if given[i] < reach]
        pool, budget = sum([weights[i] for i in candidates]), spare
        for i in candidates:
            more = min(reach - given[i], max(1, budget * weights[i] // pool), spare)
            given[i] = given[i] + more
            spare = spare - more
    return np.array(given)


def bell_draw(rng, dims, deviation, most, pieces=(), kind=jnp.bfloat16):
    entries = jax.random.normal(rng, dims, jnp.float32) * deviation
    if len(pieces) > 0:
        entries = block_levels(rng, dims, pieces, -0.22, 0.18) * entries
    return jnp.clip(entries, min=-most, max=most).astype(kind)


def setup_inputs(seed: int = 0) -> dict:
    key_list = jax.random.split(jax.random.key(seed), 13)
    query_proj = bell_draw(key_list[0], (SEQUENCE_TOKENS, QUERY_HEADS * HEAD_SIZE), 1.0, 6.0, ((0, 8), (1, 4)))
    projected_keys = bell_draw(key_list[1], (SEQUENCE_TOKENS, KEY_VALUE_HEADS * HEAD_SIZE), 1.0, 6.0, ((0, 8), (1, 4)))
    projected_values = bell_draw(key_list[2], (SEQUENCE_TOKENS, KEY_VALUE_HEADS * HEAD_SIZE), 1.0, 6.0, ((0, 8), (1, 4)))
    residual = bell_draw(key_list[3], (SEQUENCE_TOKENS, D), 1.0, 6.0, ((0, 32),))
    out_weight = bell_draw(key_list[4], (QUERY_HEADS * HEAD_SIZE, D), (QUERY_HEADS * HEAD_SIZE) ** -0.5, 0.1875)
    mix_gain = jnp.clip(1.0 + 0.18 * jax.random.normal(key_list[5], (D,), jnp.float32), 0.1, 1.9)
    norm_gain = jnp.clip(1.0 + 0.18 * jax.random.normal(key_list[6], (D,), jnp.float32), 0.1, 1.9)
    route_expert_keys = jax.random.split(jax.random.fold_in(key_list[7], 1), SEQUENCE_TOKENS // ROWS)
    route_expert_turns = jax.random.permutation(jax.random.fold_in(key_list[7], 3), SEQUENCE_TOKENS // ROWS)
    route_expert = jax.vmap(lambda own, number: deal_out(jax.random.fold_in(key_list[7], 2), own, number, ROWS, EXPERTS, TOP, CAP, 2))(route_expert_keys, route_expert_turns).reshape((SEQUENCE_TOKENS, TOP))
    route_weight = jnp.clip(0.2 + 0.8 * jax.random.uniform(key_list[8], (SEQUENCE_TOKENS, TOP), jnp.float32) ** block_levels(key_list[8], (SEQUENCE_TOKENS, TOP), ((0, 32),), -0.2, 0.2), 0.2, 1.0)
    expert_gate = bell_draw(key_list[9], (EXPERTS, D, FF), D ** -0.5, 0.125, ((0, 32),))
    expert_up = bell_draw(key_list[10], (EXPERTS, D, FF), D ** -0.5, 0.125, ((0, 32),))
    expert_down = bell_draw(key_list[11], (EXPERTS, FF, D), FF ** -0.5, 0.1875, ((0, 32),))
    return dict(query_proj=query_proj, projected_keys=projected_keys, projected_values=projected_values, residual=residual, out_weight=out_weight, mix_gain=mix_gain, norm_gain=norm_gain, route_expert=route_expert, route_weight=route_weight, expert_gate=expert_gate, expert_up=expert_up, expert_down=expert_down)


epsilon = 1e-06
base_theta = 10000.0

def unit_length_rows(values):
    values = values.astype(jnp.float32)
    return values * lax.rsqrt(lax.optimization_barrier(jnp.mean(values * values, axis=-1, keepdims=True)) + epsilon)

def rotary_embed(head_vecs, offset):
    row_count = head_vecs.shape[0]
    quarter = head_vecs.shape[-1] // 4
    places = offset + jnp.arange(row_count, dtype=jnp.int32)
    grid_row = (places // GRID_W).astype(jnp.float32)
    grid_col = (places % GRID_W).astype(jnp.float32)
    frequency = base_theta ** (-jnp.arange(quarter, dtype=jnp.float32) / quarter)
    row_angle = grid_row[:, None, None] * frequency
    col_angle = grid_col[:, None, None] * frequency
    row_cos, row_sin = (jnp.cos(row_angle), jnp.sin(row_angle))
    col_cos, col_sin = (jnp.cos(col_angle), jnp.sin(col_angle))
    row_first = head_vecs[..., :quarter]
    row_second = head_vecs[..., quarter:2 * quarter]
    col_first = head_vecs[..., 2 * quarter:3 * quarter]
    col_second = head_vecs[..., 3 * quarter:]
    return jnp.concatenate([row_first * row_cos - row_second * row_sin, row_second * row_cos + row_first * row_sin, col_first * col_cos - col_second * col_sin, col_second * col_cos + col_first * col_sin], axis=-1)

def reference(query_proj, projected_keys, projected_values, residual, out_weight, mix_gain, norm_gain, route_expert, route_weight, expert_gate, expert_up, expert_down):
    query_group = QUERY_HEADS // KEY_VALUE_HEADS
    query_prepared = rotary_embed(unit_length_rows(query_proj.reshape(SEQUENCE_TOKENS, QUERY_HEADS, HEAD_SIZE)), 0).astype(jnp.bfloat16)
    query_prepared = query_prepared.reshape(SEQUENCE_TOKENS, KEY_VALUE_HEADS, query_group, HEAD_SIZE)
    key_prepared = rotary_embed(unit_length_rows(projected_keys.reshape(SEQUENCE_TOKENS, KEY_VALUE_HEADS, HEAD_SIZE)), 0).astype(jnp.bfloat16)
    k_wide = key_prepared.astype(jnp.float32)
    value_broad = projected_values.reshape(SEQUENCE_TOKENS, KEY_VALUE_HEADS, HEAD_SIZE).astype(jnp.float32)
    scale = HEAD_SIZE ** (-0.5)
    model_width = math.gcd(SEQUENCE_TOKENS, 256)

    def attend(q_block):
        scores = jnp.einsum('thgd,nhd->thgn', q_block.astype(jnp.float32), k_wide) * scale
        weights = jnp.exp(scores)
        totals = lax.optimization_barrier(jnp.sum(weights, axis=-1))
        weights_low = lax.optimization_barrier(weights.astype(jnp.bfloat16))
        sums = jnp.einsum('thgn,nhd->thgd', weights_low.astype(jnp.float32), value_broad)
        return (sums / totals[..., None]).astype(jnp.bfloat16)
    block_list = query_prepared.reshape(SEQUENCE_TOKENS // model_width, model_width, KEY_VALUE_HEADS, query_group, HEAD_SIZE)
    attended = lax.map(attend, block_list).reshape(SEQUENCE_TOKENS, QUERY_HEADS * HEAD_SIZE)
    mixed = jnp.dot(attended, out_weight, preferred_element_type=jnp.float32)
    stream = (residual.astype(jnp.float32) + unit_length_rows(mixed) * mix_gain).astype(jnp.bfloat16)
    normed = (unit_length_rows(stream) * norm_gain).astype(jnp.bfloat16)
    limit = N_SP * N_TP * CAP
    flat_expert = route_expert.reshape(-1).astype(jnp.int32)
    order = jnp.argsort(flat_expert, stable=True).astype(jnp.int32)
    counts = lax.optimization_barrier(jnp.sum((flat_expert[:, None] == jnp.arange(EXPERTS, dtype=jnp.int32)[None, :]).astype(jnp.int32), axis=0))
    starts = (jnp.cumsum(counts) - counts).astype(jnp.int32)
    padded = jnp.concatenate([order, jnp.zeros((limit,), jnp.int32)])

    def one_expert(index):
        chosen = lax.dynamic_slice_in_dim(padded, starts[index], limit)
        rows_in = normed[chosen // TOP]
        gate_pre = jnp.dot(rows_in, expert_gate[index], preferred_element_type=jnp.float32)
        up_pre = jnp.dot(rows_in, expert_up[index], preferred_element_type=jnp.float32)
        expert_act = (jax.nn.silu(gate_pre) * up_pre).astype(jnp.bfloat16)
        return jnp.dot(expert_act, expert_down[index], preferred_element_type=jnp.float32).astype(jnp.bfloat16)
    results = lax.map(one_expert, jnp.arange(EXPERTS, dtype=jnp.int32))
    position = jnp.argsort(order, stable=True).astype(jnp.int32)
    rank = (position - starts[flat_expert]).astype(jnp.int32)
    picked = results[flat_expert, rank].reshape(SEQUENCE_TOKENS, TOP, D)
    combined = lax.optimization_barrier(jnp.sum(picked.astype(jnp.float32) * route_weight[:, :, None], axis=1))
    return (stream.astype(jnp.float32) + combined).astype(jnp.bfloat16)
```

```python
import functools
import math

import jax
import jax.numpy as jnp
from jax import lax
from jax.experimental import pallas as pl
from jax.experimental.pallas import tpu as pltpu
from jax.sharding import PartitionSpec as P

HEAD_SIZE = 64
GRID_W = 64
HALF_KEYS = 256
ONES_ROWS = 16

epsilon = 1e-06
base_theta = 10000.0

VMEM = pl.BlockSpec(memory_space=pltpu.VMEM)


def unit_length_rows(values):
    values = values.astype(jnp.float32)
    return values * lax.rsqrt(jnp.mean(values * values, axis=-1, keepdims=True) + epsilon)


def rotation_tables(tok_count, offset, lanes):
    quarter = HEAD_SIZE // 4
    lane = jnp.arange(lanes, dtype=jnp.int32) % HEAD_SIZE
    places = offset + jnp.arange(tok_count, dtype=jnp.int32)
    grid_row = (places // GRID_W).astype(jnp.float32)[:, None]
    grid_col = (places % GRID_W).astype(jnp.float32)[:, None]
    frequency = base_theta ** (-(lane % quarter).astype(jnp.float32) / quarter)
    angle = jnp.where((lane < 2 * quarter)[None, :], grid_row, grid_col) * frequency[None, :]
    sign = jnp.where((lane // quarter) % 2 == 0, -1.0, 1.0).astype(jnp.float32)
    return jnp.cos(angle), jnp.sin(angle) * sign[None, :]


def prepare_kernel(q_ref, k_ref, v_ref, cos_ref, sin_ref, q_out, kv_out):
    tok_count, lanes = k_ref.shape
    rows = lax.broadcasted_iota(jnp.int32, (lanes, lanes), 0)
    cols = lax.broadcasted_iota(jnp.int32, (lanes, lanes), 1)
    same_head = (rows // HEAD_SIZE) == (cols // HEAD_SIZE)
    mean_mat = jnp.where(same_head, 1.0 / HEAD_SIZE, 0.0).astype(jnp.bfloat16)
    swap_mat = jnp.where((rows ^ (HEAD_SIZE // 4)) == cols, 1.0, 0.0).astype(jnp.bfloat16)

    def ready(raw, factor):
        wide = raw.astype(jnp.float32)
        square = wide * wide
        high = square.astype(jnp.bfloat16)
        low = (square - high.astype(jnp.float32)).astype(jnp.bfloat16)
        mean = jnp.dot(high, mean_mat, preferred_element_type=jnp.float32) + jnp.dot(
            low, mean_mat, preferred_element_type=jnp.float32
        )
        swapped = jnp.dot(raw, swap_mat, preferred_element_type=jnp.float32)
        length = lax.rsqrt(mean + epsilon) * factor
        return (wide * cos_ref[...] + swapped * sin_ref[...]) * length

    factor = math.log2(math.e) * HEAD_SIZE ** (-0.5)
    group = q_ref.shape[1] // lanes
    q_out[...] = jnp.zeros_like(q_out)
    for block in range(group):
        turned = ready(q_ref[:, block * lanes : (block + 1) * lanes], factor).T
        for inner in range(lanes // HEAD_SIZE):
            head = block * (lanes // HEAD_SIZE) + inner
            kv_head = head // group
            q_out[
                kv_head * HEAD_SIZE : (kv_head + 1) * HEAD_SIZE,
                head * tok_count : (head + 1) * tok_count,
            ] = turned[inner * HEAD_SIZE : (inner + 1) * HEAD_SIZE].astype(jnp.bfloat16)
    keys = ready(k_ref[...], 1.0).astype(jnp.bfloat16)
    for half in range(tok_count // HALF_KEYS):
        begin = half * HALF_KEYS
        kv_out[half, :HALF_KEYS, :] = keys[begin : begin + HALF_KEYS]
        for part in range(HALF_KEYS // lanes):
            start = begin + part * lanes
            at = HALF_KEYS + part * lanes
            kv_out[half, at : at + lanes, :] = (
                v_ref[start : start + lanes, :].astype(jnp.float32).T.astype(jnp.bfloat16)
            )


def attend_kernel(chunk_count, first, last, *refs):
    q_ref = refs[0]
    chunks = refs[1 : 1 + chunk_count]
    acc_in = None if first else refs[1 + chunk_count]
    out_ref = refs[-1]
    lanes, columns = q_ref.shape
    width = 256
    kv_heads = lanes // HEAD_SIZE
    halves = [(c, i) for c in chunks for i in range(c.shape[0])]
    ones = jnp.ones((ONES_ROWS, HALF_KEYS), jnp.bfloat16)
    for block in range(columns // width):
        kv_head = block // (columns // width // kv_heads)
        q_block = q_ref[:, block * width : (block + 1) * width]
        total = None if first else acc_in[:, block * width : (block + 1) * width]
        for chunk, half in halves:
            scores = jnp.dot(
                chunk[half, :HALF_KEYS, :], q_block, preferred_element_type=jnp.float32
            )
            weights = jnp.exp2(scores).astype(jnp.bfloat16)
            values = jnp.concatenate(
                [
                    chunk[
                        half,
                        pl.ds(HALF_KEYS + part * lanes + kv_head * HEAD_SIZE, HEAD_SIZE),
                        :,
                    ]
                    for part in range(HALF_KEYS // lanes)
                ],
                axis=1,
            )
            values = jnp.concatenate([values, ones], axis=0)
            piece = jnp.dot(values, weights, preferred_element_type=jnp.float32)
            total = piece if total is None else total + piece
        if not last:
            out_ref[:, block * width : (block + 1) * width] = total
        else:
            tp, head_rows, per = out_ref.shape
            tok_count = tp * per
            ready = (total[:HEAD_SIZE] / total[HEAD_SIZE : HEAD_SIZE + 1]).astype(jnp.bfloat16)
            head = block * width // tok_count
            for piece in range(width // per):
                slot = (block * width + piece * per - head * tok_count) // per
                out_ref[slot, head * HEAD_SIZE : (head + 1) * HEAD_SIZE, :] = ready[
                    :, piece * per : (piece + 1) * per
                ]


def attend(q_ready, chunks, acc, final_shape):
    first, last = acc is None, final_shape is not None
    lanes, columns = q_ready.shape
    rows = HEAD_SIZE + ONES_ROWS
    key_count = sum(c.shape[0] for c in chunks) * HALF_KEYS
    shape = (
        jax.ShapeDtypeStruct(final_shape, jnp.bfloat16)
        if last
        else jax.ShapeDtypeStruct((rows, columns), jnp.float32)
    )
    operands = [q_ready, *chunks] + ([] if first else [acc])
    aliases = {} if (first or last) else {len(operands) - 1: 0}
    return pl.pallas_call(
        functools.partial(attend_kernel, len(chunks), first, last),
        out_shape=shape,
        in_specs=[VMEM] * len(operands),
        out_specs=VMEM,
        input_output_aliases=aliases,
        cost_estimate=pl.CostEstimate(
            flops=2 * key_count * columns * (256 + 256),
            bytes_accessed=key_count * 1024,
            transcendentals=key_count * columns,
        ),
        compiler_params=pltpu.CompilerParams(vmem_limit_bytes=24 * 1024 * 1024),
    )(*operands)


def local(
    sp_size,
    tp_size,
    query_proj,
    projected_keys,
    projected_values,
    residual,
    out_weight,
    mix_gain,
    norm_gain,
    route_expert,
    route_weight,
    expert_gate,
    expert_up,
    expert_down,
):
    tok_count, lanes = projected_keys.shape
    q_heads = query_proj.shape[1] // HEAD_SIZE
    model_width = residual.shape[1]
    offset = lax.axis_index("sp") * tok_count
    cos_table, sin_table = rotation_tables(tok_count, offset, lanes)
    q_ready, kv_own = pl.pallas_call(
        prepare_kernel,
        out_shape=(
            jax.ShapeDtypeStruct((lanes, q_heads * tok_count), jnp.bfloat16),
            jax.ShapeDtypeStruct((tok_count // HALF_KEYS, 2 * HALF_KEYS, lanes), jnp.bfloat16),
        ),
        in_specs=[VMEM] * 5,
        out_specs=(VMEM, VMEM),
        cost_estimate=pl.CostEstimate(
            flops=2 * tok_count * 512 * 512, bytes_accessed=1 << 20, transcendentals=0
        ),
        compiler_params=pltpu.CompilerParams(vmem_limit_bytes=24 * 1024 * 1024),
    )(query_proj, projected_keys, projected_values, cos_table, sin_table)

    order = list(range(0, sp_size, 2)) + list(range(sp_size - 1, 0, -2))
    ahead = [(order[i], order[(i + 1) % sp_size]) for i in range(sp_size)]
    behind = [(b, a) for a, b in ahead]
    final_shape = (tp_size, q_heads * HEAD_SIZE, tok_count // tp_size)
    steps = sp_size // 2
    acc = None
    from_left = from_right = kv_own
    held = [kv_own]
    for step in range(steps):
        if step == steps - 1:
            halves = kv_own.shape[0]
            from_left, from_right = from_left[: halves // 2], from_right[halves // 2 :]
        next_left = lax.ppermute(from_left, "sp", ahead)
        next_right = lax.ppermute(from_right, "sp", behind)
        acc = attend(q_ready, held, acc, None)
        from_left, from_right = next_left, next_right
        held = [from_left, from_right]
    attended = attend(q_ready, held, acc, final_shape)
    by_token = lax.all_to_all(attended, "tp", split_axis=0, concat_axis=0, tiled=True)
    by_token = by_token.reshape(-1, by_token.shape[-1])
    mixed = lax.dot_general(
        by_token, out_weight, (((0,), (0,)), ((), ())), preferred_element_type=jnp.float32
    )
    stream = (residual.astype(jnp.float32) + unit_length_rows(mixed) * mix_gain).astype(
        jnp.bfloat16
    )
    normed = (unit_length_rows(stream) * norm_gain).astype(jnp.bfloat16)
    row_count = normed.shape[0]
    top_count = route_expert.shape[1]
    experts = sp_size * tp_size
    capacity = max(2, 2 * top_count * row_count // experts)
    flat_expert = route_expert.T.reshape(-1)
    onehot = flat_expert[:, None] == jnp.arange(experts, dtype=jnp.int32)[None, :]
    onehot_low = onehot.astype(jnp.bfloat16)
    pairs = flat_expert.shape[0]
    before = (
        jnp.arange(pairs, dtype=jnp.int32)[None, :] < jnp.arange(pairs, dtype=jnp.int32)[:, None]
    ).astype(jnp.bfloat16)
    earlier = jnp.dot(before, onehot_low, preferred_element_type=jnp.float32)
    slot_rank = jnp.sum(jnp.where(onehot, earlier, 0.0), axis=1).astype(jnp.int32)
    target = flat_expert * capacity + slot_rank
    slots_total = experts * capacity
    chosen = target[:, None] == jnp.arange(slots_total, dtype=jnp.int32)[None, :]
    chosen = chosen.reshape(top_count, row_count, slots_total)
    placing = jnp.any(chosen, axis=0).astype(jnp.bfloat16)
    outgoing = lax.dot_general(
        placing, normed, (((0,), (0,)), ((), ())), preferred_element_type=jnp.float32
    ).astype(jnp.bfloat16)
    outgoing = outgoing.reshape(experts, capacity, model_width)
    gate_mat = expert_gate[0]
    up_mat = expert_up[0]
    down_mat = expert_down[0]
    slots = lax.all_to_all(outgoing, ("sp", "tp"), split_axis=0, concat_axis=0, tiled=True)
    flat_rows = slots.reshape(-1, slots.shape[-1])
    gate_pre = jnp.dot(flat_rows, gate_mat, preferred_element_type=jnp.float32)
    up_pre = jnp.dot(flat_rows, up_mat, preferred_element_type=jnp.float32)
    expert_act = (jax.nn.silu(gate_pre) * up_pre).astype(jnp.bfloat16)
    done = jnp.dot(expert_act, down_mat, preferred_element_type=jnp.float32).astype(jnp.bfloat16)
    answered = done.reshape(slots.shape)
    returned = lax.all_to_all(answered, ("sp", "tp"), split_axis=0, concat_axis=0, tiled=True)
    returned = returned.reshape(slots_total, model_width)
    combined = stream.astype(jnp.float32)
    for k in range(top_count):
        picked = jnp.dot(
            chosen[k].astype(jnp.bfloat16), returned, preferred_element_type=jnp.float32
        )
        combined = combined + picked * route_weight[:, k : k + 1]
    return combined.astype(jnp.bfloat16)


def solution(mesh):
    return jax.shard_map(
        functools.partial(local, mesh.shape["sp"], mesh.shape["tp"]),
        mesh=mesh,
        in_specs=(
            P("sp", "tp"),
            P("sp", "tp"),
            P("sp", "tp"),
            P(("sp", "tp"), None),
            P(),
            P(),
            P(),
            P(("sp", "tp"), None),
            P(("sp", "tp"), None),
            P(("sp", "tp"), None, None),
            P(("sp", "tp"), None, None),
            P(("sp", "tp"), None, None),
        ),
        out_specs=P(("sp", "tp"), None),
        check_vma=False,
    )
```

```python
import functools
import math

import jax
import jax.numpy as jnp
from jax import lax
from jax.experimental import pallas as pl
from jax.experimental.pallas import tpu as pltpu
from jax.sharding import PartitionSpec as P

HEAD_SIZE = 64
GRID_W = 64
HALF_KEYS = 256
ONES_ROWS = 16

epsilon = 1e-06
base_theta = 10000.0

VMEM = pl.BlockSpec(memory_space=pltpu.VMEM)
ANY = pl.BlockSpec(memory_space=pl.ANY)


def rotation_tables(first_row, row_count, lanes):
    quarter = HEAD_SIZE // 4
    lane = jnp.arange(lanes, dtype=jnp.int32) % HEAD_SIZE
    index = jnp.arange(row_count + GRID_W, dtype=jnp.int32)
    place = jnp.where(index < row_count, first_row + index, index - row_count)
    frequency = base_theta ** (-(lane % quarter).astype(jnp.float32) / quarter)
    angle = place.astype(jnp.float32)[:, None] * frequency[None, :]
    sign = jnp.where((lane // quarter) % 2 == 0, -1.0, 1.0).astype(jnp.float32)
    return jnp.cos(angle), jnp.sin(angle) * sign[None, :]


def prepare_kernel(q_hbm, k_hbm, v_hbm, cos_ref, sin_ref, q_out, kv_out, q_ref, k_ref, v_ref, sems):
    copies = [
        pltpu.make_async_copy(src, dst, sems.at[i])
        for i, (src, dst) in enumerate(((k_hbm, k_ref), (v_hbm, v_ref), (q_hbm, q_ref)))
    ]
    for copy in copies:
        copy.start()
    tok_count, lanes = k_ref.shape
    grid_rows = tok_count // GRID_W
    rows = lax.broadcasted_iota(jnp.int32, (lanes, lanes), 0)
    cols = lax.broadcasted_iota(jnp.int32, (lanes, lanes), 1)
    same_head = (rows // HEAD_SIZE) == (cols // HEAD_SIZE)
    mean_mat = jnp.where(same_head, 1.0 / HEAD_SIZE, 0.0).astype(jnp.bfloat16)
    swap_mat = jnp.where((rows ^ (HEAD_SIZE // 4)) == cols, 1.0, 0.0).astype(jnp.bfloat16)
    lane = lax.broadcasted_iota(jnp.int32, (grid_rows, GRID_W, lanes), 2)
    by_row = (lane % HEAD_SIZE) < HEAD_SIZE // 2

    def table(ref):
        row_part = ref[:grid_rows, :][:, None, :]
        col_part = ref[grid_rows:, :][None, :, :]
        return jnp.where(by_row, row_part, col_part).reshape(tok_count, lanes)

    cos, sin = table(cos_ref), table(sin_ref)

    def ready(raw, factor):
        wide = raw.astype(jnp.float32)
        square = wide * wide
        high = square.astype(jnp.bfloat16)
        low = (square - high.astype(jnp.float32)).astype(jnp.bfloat16)
        mean = jnp.dot(high, mean_mat, preferred_element_type=jnp.float32) + jnp.dot(
            low, mean_mat, preferred_element_type=jnp.float32
        )
        swapped = jnp.dot(raw, swap_mat, preferred_element_type=jnp.float32)
        length = lax.rsqrt(mean + epsilon) * factor
        return (wide * cos + swapped * sin) * length

    for copy in copies:
        copy.wait()
    keys = ready(k_ref[...], 1.0).astype(jnp.bfloat16)
    for half in range(tok_count // HALF_KEYS):
        begin = half * HALF_KEYS
        kv_out[half, :HALF_KEYS, :] = keys[begin : begin + HALF_KEYS]
        for part in range(HALF_KEYS // lanes):
            start = begin + part * lanes
            at = HALF_KEYS + part * lanes
            kv_out[half, at : at + lanes, :] = (
                v_ref[start : start + lanes, :].astype(jnp.float32).T.astype(jnp.bfloat16)
            )
    factor = math.log2(math.e) * HEAD_SIZE ** (-0.5)
    group = q_ref.shape[1] // lanes
    q_out[...] = jnp.zeros_like(q_out)
    for block in range(group):
        turned = ready(q_ref[:, block * lanes : (block + 1) * lanes], factor).T
        for inner in range(lanes // HEAD_SIZE):
            head = block * (lanes // HEAD_SIZE) + inner
            kv_head = head // group
            q_out[
                kv_head * HEAD_SIZE : (kv_head + 1) * HEAD_SIZE,
                head * tok_count : (head + 1) * tok_count,
            ] = turned[inner * HEAD_SIZE : (inner + 1) * HEAD_SIZE].astype(jnp.bfloat16)


def attend_kernel(chunk_count, first, last, *refs):
    q_ref = refs[0]
    chunks = refs[1 : 1 + chunk_count]
    acc_in = None if first else refs[1 + chunk_count]
    out_refs = refs[1 + chunk_count + (0 if first else 1) :]
    lanes, columns = q_ref.shape
    width = min(512, columns)
    blocks = columns // width
    kv_heads = lanes // HEAD_SIZE
    halves = [(c, i) for c in chunks for i in range(c.shape[0])]
    ones = jnp.ones((ONES_ROWS, HALF_KEYS), jnp.bfloat16)
    waiting = None
    for block in range(blocks + 1):
        weights = []
        total = None
        for index, (chunk, half) in enumerate(halves):
            if block < blocks:
                scores = jnp.dot(
                    chunk[half, :HALF_KEYS, :],
                    q_ref[:, block * width : (block + 1) * width],
                    preferred_element_type=jnp.float32,
                )
                weights.append(jnp.exp2(scores).astype(jnp.bfloat16))
            if waiting is not None:
                kv_head = (block - 1) * kv_heads // blocks
                values = jnp.concatenate(
                    [
                        chunk[
                            half,
                            pl.ds(HALF_KEYS + part * lanes + kv_head * HEAD_SIZE, HEAD_SIZE),
                            :,
                        ]
                        for part in range(HALF_KEYS // lanes)
                    ],
                    axis=1,
                )
                values = jnp.concatenate([values, ones], axis=0)
                piece = jnp.dot(values, waiting[index], preferred_element_type=jnp.float32)
                total = piece if total is None else total + piece
        if waiting is not None:
            at = (block - 1) * width
            if not first:
                total = total + acc_in[:, at : at + width]
            if not last:
                out_refs[0][:, at : at + width] = total
            else:
                turn = out_refs[-1]
                tp, head_rows, per = turn.shape
                tok_count = tp * per
                ready = (total[:HEAD_SIZE] / total[HEAD_SIZE : HEAD_SIZE + 1]).astype(jnp.bfloat16)
                for piece in range(width // per):
                    head, place = divmod(at + piece * per, tok_count)
                    turn[place // per, head * HEAD_SIZE : (head + 1) * HEAD_SIZE, :] = ready[
                        :, piece * per : (piece + 1) * per
                    ]
        waiting = weights
    if last:
        me = lax.axis_index("tp")
        turn = out_refs[-1]
        rel = 0
        for out in out_refs[:-1]:
            for j in range(out.shape[0]):
                out[j] = turn[me ^ rel]
                rel += 1


def attend(q_ready, chunks, acc, tp_size=None):
    first, last = acc is None, tp_size is not None
    lanes, columns = q_ready.shape
    rows = HEAD_SIZE + ONES_ROWS
    key_count = sum(c.shape[0] for c in chunks) * HALF_KEYS
    scratch = []
    if last:
        tok_count = chunks[0].shape[0] * HALF_KEYS * 2
        head_rows = columns // tok_count * HEAD_SIZE
        block = (head_rows, tok_count // tp_size)
        sizes = [1] + [1 << b for b in range(tp_size.bit_length() - 1)]
        shape = [jax.ShapeDtypeStruct((n, *block), jnp.bfloat16) for n in sizes]
        scratch = [pltpu.VMEM((tp_size, *block), jnp.bfloat16)]
    else:
        shape = [jax.ShapeDtypeStruct((rows, columns), jnp.float32)]
    operands = [q_ready, *chunks] + ([] if first else [acc])
    aliases = {} if (first or last) else {len(operands) - 1: 0}
    out = pl.pallas_call(
        functools.partial(attend_kernel, len(chunks), first, last),
        out_shape=shape,
        in_specs=[VMEM] * len(operands),
        out_specs=[VMEM] * len(shape),
        scratch_shapes=scratch,
        input_output_aliases=aliases,
        cost_estimate=pl.CostEstimate(
            flops=2 * key_count * columns * 512,
            bytes_accessed=key_count * 1024,
            transcendentals=key_count * columns,
        ),
        compiler_params=pltpu.CompilerParams(vmem_limit_bytes=24 * 1024 * 1024),
    )(*operands)
    return out if last else out[0]


def hypercube_exchange(pieces, tp_size):
    held = []
    for bit in reversed(range(tp_size.bit_length() - 1)):
        pairs = [(i, i ^ (1 << bit)) for i in range(tp_size)]
        half = 1 << bit
        moved = [(half, lax.ppermute(pieces[1 + bit], "tp", pairs))]
        kept = []
        for source, block in held:
            moved.append((source ^ half, lax.ppermute(block[half:], "tp", pairs)))
            kept.append((source, block[:half]))
        held = kept + moved
    return [pieces[0]] + [block for _, block in sorted(held, key=lambda item: item[0])]


def out_kernel(tp_size, *refs):
    blocks = refs[:tp_size]
    w_ref, res_ref, mix_ref, norm_ref, target_ref = refs[tp_size : tp_size + 5]
    stream_ref, out_ref, mixed_ref, normed_ref = refs[tp_size + 5 :]
    me = lax.axis_index("tp")
    _, head_rows, row_count = blocks[0].shape
    width = w_ref.shape[1]
    step = min(512, width)
    turned = [b[0].astype(jnp.float32).T.astype(jnp.bfloat16) for b in blocks]
    power = jnp.zeros((row_count, 1), jnp.float32)
    for at in range(0, width, step):
        mixed = jnp.zeros((row_count, step), jnp.float32)
        for rel in range(tp_size):
            begin = pl.multiple_of((me ^ rel) * head_rows, head_rows)
            mixed = mixed + jnp.dot(
                turned[rel],
                w_ref[pl.ds(begin, head_rows), at : at + step],
                preferred_element_type=jnp.float32,
            )
        mixed_ref[:, at : at + step] = mixed
        power = power + jnp.sum(mixed * mixed, axis=1, keepdims=True)
    scale = lax.rsqrt(power / width + epsilon)
    power = jnp.zeros((row_count, 1), jnp.float32)
    for at in range(0, width, step):
        cols = slice(at, at + step)
        stream = (
            res_ref[:, cols].astype(jnp.float32) + mixed_ref[:, cols] * scale * mix_ref[:, cols]
        ).astype(jnp.bfloat16)
        stream_ref[:, cols] = stream
        wide = stream.astype(jnp.float32)
        power = power + jnp.sum(wide * wide, axis=1, keepdims=True)
    scale = lax.rsqrt(power / width + epsilon)
    for at in range(0, width, step):
        cols = slice(at, at + step)
        wide = stream_ref[:, cols].astype(jnp.float32)
        normed_ref[:, cols] = (wide * scale * norm_ref[:, cols]).astype(jnp.bfloat16)
    slots = lax.broadcasted_iota(jnp.int32, (out_ref.shape[0], row_count), 0)
    hit = slots == target_ref[0:1, :]
    for k in range(1, target_ref.shape[0]):
        hit = hit | (slots == target_ref[k : k + 1, :])
    placing = jnp.where(hit, 1.0, 0.0).astype(jnp.bfloat16)
    for at in range(0, width, step):
        cols = slice(at, at + step)
        out_ref[:, cols] = jnp.dot(
            placing, normed_ref[:, cols], preferred_element_type=jnp.float32
        ).astype(jnp.bfloat16)


def expert_kernel(rows_ref, gate_ref, up_ref, down_ref, out_ref, act_ref):
    hidden = gate_ref.shape[1]
    width = down_ref.shape[1]
    step = min(256, hidden)
    for at in range(0, hidden, step):
        cols = slice(at, at + step)
        gate = jnp.dot(rows_ref[...], gate_ref[:, cols], preferred_element_type=jnp.float32)
        up = jnp.dot(rows_ref[...], up_ref[:, cols], preferred_element_type=jnp.float32)
        act_ref[:, cols] = (gate / (1.0 + jnp.exp(-gate)) * up).astype(jnp.bfloat16)
    step = min(512, width)
    for at in range(0, width, step):
        cols = slice(at, at + step)
        out_ref[:, cols] = jnp.dot(
            act_ref[...], down_ref[:, cols], preferred_element_type=jnp.float32
        ).astype(jnp.bfloat16)


def local(
    sp_size,
    tp_size,
    query_proj,
    projected_keys,
    projected_values,
    residual,
    out_weight,
    mix_gain,
    norm_gain,
    route_expert,
    route_weight,
    expert_gate,
    expert_up,
    expert_down,
):
    tok_count, lanes = projected_keys.shape
    q_heads = query_proj.shape[1] // HEAD_SIZE
    model_width = residual.shape[1]
    grid_rows = tok_count // GRID_W
    cos_table, sin_table = rotation_tables(lax.axis_index("sp") * grid_rows, grid_rows, lanes)
    q_ready, kv_own = pl.pallas_call(
        prepare_kernel,
        out_shape=(
            jax.ShapeDtypeStruct((lanes, q_heads * tok_count), jnp.bfloat16),
            jax.ShapeDtypeStruct((tok_count // HALF_KEYS, 2 * HALF_KEYS, lanes), jnp.bfloat16),
        ),
        in_specs=[ANY] * 3 + [VMEM] * 2,
        out_specs=(VMEM, VMEM),
        scratch_shapes=[
            pltpu.VMEM(query_proj.shape, jnp.bfloat16),
            pltpu.VMEM(projected_keys.shape, jnp.bfloat16),
            pltpu.VMEM(projected_values.shape, jnp.bfloat16),
            pltpu.SemaphoreType.DMA((3,)),
        ],
        cost_estimate=pl.CostEstimate(
            flops=2 * tok_count * 512 * 512, bytes_accessed=1 << 20, transcendentals=0
        ),
        compiler_params=pltpu.CompilerParams(vmem_limit_bytes=32 * 1024 * 1024),
    )(query_proj, projected_keys, projected_values, cos_table, sin_table)

    order = list(range(0, sp_size, 2)) + list(range(sp_size - 1, 0, -2))
    ahead = [(order[i], order[(i + 1) % sp_size]) for i in range(sp_size)]
    behind = [(b, a) for a, b in ahead]
    steps = sp_size // 2
    acc = None
    from_left = from_right = kv_own
    held = [kv_own]
    for step in range(steps):
        if step == steps - 1:
            halves = kv_own.shape[0]
            from_left, from_right = from_left[: halves // 2], from_right[halves // 2 :]
        next_left = lax.ppermute(from_left, "sp", ahead)
        next_right = lax.ppermute(from_right, "sp", behind)
        acc = attend(q_ready, held, acc)
        from_left, from_right = next_left, next_right
        held = [from_left, from_right]
    pieces = attend(q_ready, held, acc, tp_size)
    blocks = hypercube_exchange(pieces, tp_size)

    row_count = residual.shape[0]
    top_count = route_expert.shape[1]
    experts = sp_size * tp_size
    capacity = max(2, 2 * top_count * row_count // experts)
    slots_total = experts * capacity
    flat_expert = route_expert.T.reshape(-1)
    onehot = flat_expert[:, None] == jnp.arange(experts, dtype=jnp.int32)[None, :]
    pairs = flat_expert.shape[0]
    before = (
        jnp.arange(pairs, dtype=jnp.int32)[None, :] < jnp.arange(pairs, dtype=jnp.int32)[:, None]
    ).astype(jnp.bfloat16)
    earlier = jnp.dot(before, onehot.astype(jnp.bfloat16), preferred_element_type=jnp.float32)
    slot_rank = jnp.sum(jnp.where(onehot, earlier, 0.0), axis=1).astype(jnp.int32)
    target = (flat_expert * capacity + slot_rank).reshape(top_count, row_count)

    stream, outgoing = pl.pallas_call(
        functools.partial(out_kernel, tp_size),
        out_shape=(
            jax.ShapeDtypeStruct((row_count, model_width), jnp.bfloat16),
            jax.ShapeDtypeStruct((slots_total, model_width), jnp.bfloat16),
        ),
        in_specs=[VMEM] * (tp_size + 5),
        out_specs=(VMEM, VMEM),
        scratch_shapes=[
            pltpu.VMEM((row_count, model_width), jnp.float32),
            pltpu.VMEM((row_count, model_width), jnp.bfloat16),
        ],
        cost_estimate=pl.CostEstimate(
            flops=2 * row_count * model_width * (out_weight.shape[0] + slots_total),
            bytes_accessed=8 << 20,
            transcendentals=0,
        ),
        compiler_params=pltpu.CompilerParams(vmem_limit_bytes=12 * 1024 * 1024),
    )(*blocks, out_weight, residual, mix_gain[None, :], norm_gain[None, :], target)

    outgoing = outgoing.reshape(experts, capacity, model_width)
    slots = lax.all_to_all(outgoing, ("sp", "tp"), split_axis=0, concat_axis=0, tiled=True)
    flat_rows = slots.reshape(-1, model_width)
    hidden = expert_gate.shape[2]
    done = pl.pallas_call(
        expert_kernel,
        out_shape=jax.ShapeDtypeStruct(flat_rows.shape, jnp.bfloat16),
        in_specs=[VMEM] * 4,
        out_specs=VMEM,
        scratch_shapes=[pltpu.VMEM((flat_rows.shape[0], hidden), jnp.bfloat16)],
        cost_estimate=pl.CostEstimate(
            flops=6 * flat_rows.shape[0] * model_width * hidden,
            bytes_accessed=16 << 20,
            transcendentals=flat_rows.shape[0] * hidden,
        ),
        compiler_params=pltpu.CompilerParams(vmem_limit_bytes=24 * 1024 * 1024),
    )(flat_rows, expert_gate[0], expert_up[0], expert_down[0])
    answered = done.reshape(slots.shape)
    returned = lax.all_to_all(answered, ("sp", "tp"), split_axis=0, concat_axis=0, tiled=True)
    returned = returned.reshape(slots_total, model_width)
    chosen = target[:, :, None] == jnp.arange(slots_total, dtype=jnp.int32)[None, None, :]
    combined = stream.astype(jnp.float32)
    for k in range(top_count):
        picked = jnp.dot(
            chosen[k].astype(jnp.bfloat16), returned, preferred_element_type=jnp.float32
        )
        combined = combined + picked * route_weight[:, k : k + 1]
    return combined.astype(jnp.bfloat16)


def solution(mesh):
    return jax.shard_map(
        functools.partial(local, mesh.shape["sp"], mesh.shape["tp"]),
        mesh=mesh,
        in_specs=(
            P("sp", "tp"),
            P("sp", "tp"),
            P("sp", "tp"),
            P(("sp", "tp"), None),
            P(),
            P(),
            P(),
            P(("sp", "tp"), None),
            P(("sp", "tp"), None),
            P(("sp", "tp"), None, None),
            P(("sp", "tp"), None, None),
            P(("sp", "tp"), None, None),
        ),
        out_specs=P(("sp", "tp"), None),
        check_vma=False,
    )
```

```python
import functools
import math

import jax
import jax.numpy as jnp
from jax import lax
from jax.experimental import pallas as pl
from jax.experimental.pallas import tpu as pltpu
from jax.sharding import Mesh
from jax.sharding import PartitionSpec as P

HEAD_SIZE = 64
GRID_W = 64
HALF_KEYS = 256
ONES_ROWS = 16

epsilon = 1e-06
base_theta = 10000.0

SP = ("hf", "q")
ALL = ("hf", "q", "tp")
HALF = ("q", "tp")

VMEM = pl.BlockSpec(memory_space=pltpu.VMEM)
HBM = pl.BlockSpec(memory_space=pltpu.HBM)


def rotation_tables(first_row, row_count, lanes):
    quarter = HEAD_SIZE // 4
    lane = jnp.arange(lanes, dtype=jnp.int32) % HEAD_SIZE
    index = jnp.arange(row_count + GRID_W, dtype=jnp.int32)
    place = jnp.where(index < row_count, first_row + index, index - row_count)
    frequency = base_theta ** (-(lane % quarter).astype(jnp.float32) / quarter)
    angle = place.astype(jnp.float32)[:, None] * frequency[None, :]
    sign = jnp.where((lane // quarter) % 2 == 0, -1.0, 1.0).astype(jnp.float32)
    return jnp.cos(angle), jnp.sin(angle) * sign[None, :]


def prepare_kernel(q_hbm, k_hbm, v_hbm, cos_ref, sin_ref, q_out, kv_out, q_ref, k_ref, v_ref, sems):
    copies = [
        pltpu.make_async_copy(src, dst, sems.at[i])
        for i, (src, dst) in enumerate(((k_hbm, k_ref), (v_hbm, v_ref), (q_hbm, q_ref)))
    ]
    for copy in copies:
        copy.start()
    tok_count, lanes = k_ref.shape
    grid_rows = tok_count // GRID_W
    rows = lax.broadcasted_iota(jnp.int32, (lanes, lanes), 0)
    cols = lax.broadcasted_iota(jnp.int32, (lanes, lanes), 1)
    same_head = (rows // HEAD_SIZE) == (cols // HEAD_SIZE)
    mean_mat = jnp.where(same_head, 1.0 / HEAD_SIZE, 0.0).astype(jnp.bfloat16)
    swap_mat = jnp.where((rows ^ (HEAD_SIZE // 4)) == cols, 1.0, 0.0).astype(jnp.bfloat16)
    lane = lax.broadcasted_iota(jnp.int32, (grid_rows, GRID_W, lanes), 2)
    by_row = (lane % HEAD_SIZE) < HEAD_SIZE // 2

    def table(ref):
        row_part = ref[:grid_rows, :][:, None, :]
        col_part = ref[grid_rows:, :][None, :, :]
        return jnp.where(by_row, row_part, col_part).reshape(tok_count, lanes)

    cos, sin = table(cos_ref), table(sin_ref)

    def ready(raw, factor):
        wide = raw.astype(jnp.float32)
        square = wide * wide
        high = square.astype(jnp.bfloat16)
        low = (square - high.astype(jnp.float32)).astype(jnp.bfloat16)
        mean = jnp.dot(high, mean_mat, preferred_element_type=jnp.float32) + jnp.dot(
            low, mean_mat, preferred_element_type=jnp.float32
        )
        swapped = jnp.dot(raw, swap_mat, preferred_element_type=jnp.float32)
        length = lax.rsqrt(mean + epsilon) * factor
        return (wide * cos + swapped * sin) * length

    for copy in copies:
        copy.wait()
    keys = ready(k_ref[...], 1.0).astype(jnp.bfloat16)
    for half in range(tok_count // HALF_KEYS):
        begin = half * HALF_KEYS
        kv_out[half, :HALF_KEYS, :] = keys[begin : begin + HALF_KEYS]
        for part in range(HALF_KEYS // lanes):
            start = begin + part * lanes
            at = HALF_KEYS + part * lanes
            kv_out[half, at : at + lanes, :] = (
                v_ref[start : start + lanes, :].astype(jnp.float32).T.astype(jnp.bfloat16)
            )
    factor = math.log2(math.e) * HEAD_SIZE ** (-0.5)
    group = q_ref.shape[1] // lanes
    q_out[...] = jnp.zeros_like(q_out)
    for block in range(group):
        turned = ready(q_ref[:, block * lanes : (block + 1) * lanes], factor).T
        for inner in range(lanes // HEAD_SIZE):
            head = block * (lanes // HEAD_SIZE) + inner
            kv_head = head // group
            q_out[
                kv_head * HEAD_SIZE : (kv_head + 1) * HEAD_SIZE,
                head * tok_count : (head + 1) * tok_count,
            ] = turned[inner * HEAD_SIZE : (inner + 1) * HEAD_SIZE].astype(jnp.bfloat16)


def attend_kernel(chunk_count, first, last, *refs):
    q_ref = refs[0]
    chunks = refs[1 : 1 + chunk_count]
    acc_in = None if first else refs[1 + chunk_count]
    out_refs = refs[1 + chunk_count + (0 if first else 1) :]
    lanes, columns = q_ref.shape
    width = min(512, columns)
    blocks = columns // width
    kv_heads = lanes // HEAD_SIZE
    halves = [(c, i) for c in chunks for i in range(c.shape[0])]
    ones = jnp.ones((ONES_ROWS, HALF_KEYS), jnp.bfloat16)
    waiting = None
    for block in range(blocks + 1):
        weights = []
        total = None
        for index, (chunk, half) in enumerate(halves):
            if block < blocks:
                scores = jnp.dot(
                    chunk[half, :HALF_KEYS, :],
                    q_ref[:, block * width : (block + 1) * width],
                    preferred_element_type=jnp.float32,
                )
                weights.append(jnp.exp2(scores).astype(jnp.bfloat16))
            if waiting is not None:
                kv_head = (block - 1) * kv_heads // blocks
                values = jnp.concatenate(
                    [
                        chunk[
                            half,
                            pl.ds(HALF_KEYS + part * lanes + kv_head * HEAD_SIZE, HEAD_SIZE),
                            :,
                        ]
                        for part in range(HALF_KEYS // lanes)
                    ],
                    axis=1,
                )
                values = jnp.concatenate([values, ones], axis=0)
                piece = jnp.dot(values, waiting[index], preferred_element_type=jnp.float32)
                total = piece if total is None else total + piece
        if waiting is not None:
            at = (block - 1) * width
            if not first:
                total = total + acc_in[:, at : at + width]
            if not last:
                out_refs[0][:, at : at + width] = total
            else:
                turn = out_refs[-1]
                tp, head_rows, per = turn.shape
                tok_count = tp * per
                ready = (total[:HEAD_SIZE] / total[HEAD_SIZE : HEAD_SIZE + 1]).astype(jnp.bfloat16)
                for piece in range(width // per):
                    head, place = divmod(at + piece * per, tok_count)
                    turn[place // per, head * HEAD_SIZE : (head + 1) * HEAD_SIZE, :] = ready[
                        :, piece * per : (piece + 1) * per
                    ]
        waiting = weights
    if last:
        me = lax.axis_index("tp")
        turn = out_refs[-1]
        rel = 0
        for out in out_refs[:-1]:
            for j in range(out.shape[0]):
                out[j] = turn[me ^ rel]
                rel += 1


def attend(q_ready, chunks, acc, tp_size=None):
    first, last = acc is None, tp_size is not None
    lanes, columns = q_ready.shape
    rows = HEAD_SIZE + ONES_ROWS
    key_count = sum(c.shape[0] for c in chunks) * HALF_KEYS
    scratch = []
    if last:
        tok_count = chunks[0].shape[0] * HALF_KEYS * 2
        head_rows = columns // tok_count * HEAD_SIZE
        block = (head_rows, tok_count // tp_size)
        sizes = [1] + [1 << b for b in range(tp_size.bit_length() - 1)]
        shape = [jax.ShapeDtypeStruct((n, *block), jnp.bfloat16) for n in sizes]
        scratch = [pltpu.VMEM((tp_size, *block), jnp.bfloat16)]
    else:
        shape = [jax.ShapeDtypeStruct((rows, columns), jnp.float32)]
    operands = [q_ready, *chunks] + ([] if first else [acc])
    aliases = {} if (first or last) else {len(operands) - 1: 0}
    out = pl.pallas_call(
        functools.partial(attend_kernel, len(chunks), first, last),
        out_shape=shape,
        in_specs=[VMEM] * len(operands),
        out_specs=[VMEM] * len(shape),
        scratch_shapes=scratch,
        input_output_aliases=aliases,
        cost_estimate=pl.CostEstimate(
            flops=2 * key_count * columns * 512,
            bytes_accessed=key_count * 1024,
            transcendentals=key_count * columns,
        ),
        compiler_params=pltpu.CompilerParams(vmem_limit_bytes=24 * 1024 * 1024),
    )(*operands)
    return out if last else out[0]


def hypercube_exchange(pieces, tp_size):
    held = []
    for bit in reversed(range(tp_size.bit_length() - 1)):
        pairs = [(i, i ^ (1 << bit)) for i in range(tp_size)]
        half = 1 << bit
        moved = [(half, lax.ppermute(pieces[1 + bit], "tp", pairs))]
        kept = []
        for source, block in held:
            moved.append((source ^ half, lax.ppermute(block[half:], "tp", pairs)))
            kept.append((source, block[:half]))
        held = kept + moved
    return [pieces[0]] + [block for _, block in sorted(held, key=lambda item: item[0])]


def out_kernel(tp_size, *refs):
    blocks = refs[:tp_size]
    w_ref, res_ref, mix_ref, norm_ref, target_ref = refs[tp_size : tp_size + 5]
    stream_ref, normed_ref, out_ref, mixed_ref = refs[tp_size + 5 :]
    me = lax.axis_index("tp")
    _, head_rows, row_count = blocks[0].shape
    width = w_ref.shape[1]
    step = min(512, width)
    turned = [b[0].astype(jnp.float32).T.astype(jnp.bfloat16) for b in blocks]
    power = jnp.zeros((row_count, 1), jnp.float32)
    for at in range(0, width, step):
        mixed = jnp.zeros((row_count, step), jnp.float32)
        for rel in range(tp_size):
            begin = pl.multiple_of((me ^ rel) * head_rows, head_rows)
            mixed = mixed + jnp.dot(
                turned[rel],
                w_ref[pl.ds(begin, head_rows), at : at + step],
                preferred_element_type=jnp.float32,
            )
        mixed_ref[:, at : at + step] = mixed
        power = power + jnp.sum(mixed * mixed, axis=1, keepdims=True)
    scale = lax.rsqrt(power / width + epsilon)
    power = jnp.zeros((row_count, 1), jnp.float32)
    for at in range(0, width, step):
        cols = slice(at, at + step)
        stream = (
            res_ref[:, cols].astype(jnp.float32) + mixed_ref[:, cols] * scale * mix_ref[:, cols]
        ).astype(jnp.bfloat16)
        stream_ref[:, cols] = stream
        wide = stream.astype(jnp.float32)
        power = power + jnp.sum(wide * wide, axis=1, keepdims=True)
    scale = lax.rsqrt(power / width + epsilon)
    for at in range(0, width, step):
        cols = slice(at, at + step)
        wide = stream_ref[:, cols].astype(jnp.float32)
        normed_ref[:, cols] = (wide * scale * norm_ref[:, cols]).astype(jnp.bfloat16)
    fill_slots(normed_ref, target_ref, out_ref)


def fill_slots(rows_ref, target_ref, out_ref):
    row_count, width = rows_ref.shape
    step = min(512, width)
    slots = lax.broadcasted_iota(jnp.int32, (out_ref.shape[0], row_count), 0).astype(jnp.float32)
    hit = slots == target_ref[0:1, :]
    for k in range(1, target_ref.shape[0]):
        hit = hit | (slots == target_ref[k : k + 1, :])
    placing = jnp.where(hit, 1.0, 0.0).astype(jnp.bfloat16)
    for at in range(0, width, step):
        cols = slice(at, at + step)
        out_ref[:, cols] = jnp.dot(
            placing, rows_ref[:, cols], preferred_element_type=jnp.float32
        ).astype(jnp.bfloat16)


def gather_kernel(base_count, *refs):
    bases = refs[:base_count]
    slots_ref, target_ref, weight_ref, out_ref = refs[base_count:]
    row_count, width = out_ref.shape
    step = min(512, width)
    slots = lax.broadcasted_iota(jnp.int32, (row_count, slots_ref.shape[0]), 1).astype(jnp.float32)
    top_count = target_ref.shape[1]
    picks = [
        jnp.where(slots == target_ref[:, k : k + 1], 1.0, 0.0).astype(jnp.bfloat16)
        for k in range(top_count)
    ]
    for at in range(0, width, step):
        cols = slice(at, at + step)
        total = None
        for base in bases:
            piece = base[:, cols].astype(jnp.float32)
            total = piece if total is None else total + piece
        for k in range(top_count):
            row = jnp.dot(picks[k], slots_ref[:, cols], preferred_element_type=jnp.float32)
            row = row * weight_ref[:, k : k + 1]
            total = row if total is None else total + row
        out_ref[:, cols] = total.astype(out_ref.dtype)


def expert_kernel(rows_ref, gate_ref, up_ref, down_ref, out_ref, act_ref):
    hidden = gate_ref.shape[1]
    width = down_ref.shape[1]
    step = min(256, hidden)
    for at in range(0, hidden, step):
        cols = slice(at, at + step)
        gate = jnp.dot(rows_ref[...], gate_ref[:, cols], preferred_element_type=jnp.float32)
        up = jnp.dot(rows_ref[...], up_ref[:, cols], preferred_element_type=jnp.float32)
        act_ref[:, cols] = (gate / (1.0 + jnp.exp(-gate)) * up).astype(jnp.bfloat16)
    step = min(512, width)
    for at in range(0, width, step):
        cols = slice(at, at + step)
        out_ref[:, cols] = jnp.dot(
            act_ref[...], down_ref[:, cols], preferred_element_type=jnp.float32
        ).astype(jnp.bfloat16)


def local(
    sp_size,
    tp_size,
    query_proj,
    projected_keys,
    projected_values,
    residual,
    out_weight,
    mix_gain,
    norm_gain,
    route_expert,
    route_weight,
    expert_gate,
    expert_up,
    expert_down,
):
    tok_count, lanes = projected_keys.shape
    q_heads = query_proj.shape[1] // HEAD_SIZE
    model_width = residual.shape[1]
    grid_rows = tok_count // GRID_W
    cos_table, sin_table = rotation_tables(lax.axis_index(SP) * grid_rows, grid_rows, lanes)
    q_ready, kv_own = pl.pallas_call(
        prepare_kernel,
        out_shape=(
            jax.ShapeDtypeStruct((lanes, q_heads * tok_count), jnp.bfloat16),
            jax.ShapeDtypeStruct((tok_count // HALF_KEYS, 2 * HALF_KEYS, lanes), jnp.bfloat16),
        ),
        in_specs=[HBM] * 3 + [VMEM] * 2,
        out_specs=(VMEM, VMEM),
        scratch_shapes=[
            pltpu.VMEM(query_proj.shape, jnp.bfloat16),
            pltpu.VMEM(projected_keys.shape, jnp.bfloat16),
            pltpu.VMEM(projected_values.shape, jnp.bfloat16),
            pltpu.SemaphoreType.DMA((3,)),
        ],
        cost_estimate=pl.CostEstimate(
            flops=2 * tok_count * 512 * 512, bytes_accessed=1 << 20, transcendentals=0
        ),
        compiler_params=pltpu.CompilerParams(vmem_limit_bytes=32 * 1024 * 1024),
    )(query_proj, projected_keys, projected_values, cos_table, sin_table)

    order = list(range(0, sp_size, 2)) + list(range(sp_size - 1, 0, -2))
    ahead = [(order[i], order[(i + 1) % sp_size]) for i in range(sp_size)]
    behind = [(b, a) for a, b in ahead]
    steps = sp_size // 2
    acc = None
    from_left = from_right = kv_own
    held = [kv_own]
    for step in range(steps):
        if step == steps - 1:
            halves = kv_own.shape[0]
            from_left, from_right = from_left[: halves // 2], from_right[halves // 2 :]
        next_left = lax.ppermute(from_left, SP, ahead)
        next_right = lax.ppermute(from_right, SP, behind)
        acc = attend(q_ready, held, acc)
        from_left, from_right = next_left, next_right
        held = [from_left, from_right]
    pieces = attend(q_ready, held, acc, tp_size)
    blocks = hypercube_exchange(pieces, tp_size)

    row_count = residual.shape[0]
    top_count = route_expert.shape[1]
    experts = sp_size * tp_size
    capacity = max(2, 2 * top_count * row_count // experts)
    slots_total = experts * capacity
    flat_expert = route_expert.T.reshape(-1)
    onehot = flat_expert[:, None] == jnp.arange(experts, dtype=jnp.int32)[None, :]
    pairs = flat_expert.shape[0]
    before = (
        jnp.arange(pairs, dtype=jnp.int32)[None, :] < jnp.arange(pairs, dtype=jnp.int32)[:, None]
    ).astype(jnp.bfloat16)
    earlier = jnp.dot(before, onehot.astype(jnp.bfloat16), preferred_element_type=jnp.float32)
    slot_rank = jnp.sum(jnp.where(onehot, earlier, 0.0), axis=1).astype(jnp.int32)
    half_slots = slots_total // 2
    target = (flat_expert * capacity + slot_rank).astype(jnp.float32)
    target = target.reshape(top_count, row_count)
    first_slot = (lax.axis_index("hf") * half_slots).astype(jnp.float32)
    mirror = [(0, 1), (1, 0)]
    with jax.named_scope("tables"):
        far = lax.ppermute(jnp.concatenate([target, route_weight.T], axis=0), "hf", mirror)
    far_target = far[:top_count] - first_slot
    far_weight = far[top_count:].T
    own_target = target - first_slot

    rows_shape = jax.ShapeDtypeStruct((row_count, model_width), jnp.bfloat16)
    slots_shape = jax.ShapeDtypeStruct((half_slots, model_width), jnp.bfloat16)
    stream, normed, own_out = pl.pallas_call(
        functools.partial(out_kernel, tp_size),
        out_shape=(rows_shape, rows_shape, slots_shape),
        in_specs=[VMEM] * (tp_size + 5),
        out_specs=(VMEM, VMEM, VMEM),
        scratch_shapes=[pltpu.VMEM((row_count, model_width), jnp.float32)],
        cost_estimate=pl.CostEstimate(
            flops=2 * row_count * model_width * (out_weight.shape[0] + half_slots),
            bytes_accessed=8 << 20,
            transcendentals=0,
        ),
        compiler_params=pltpu.CompilerParams(vmem_limit_bytes=12 * 1024 * 1024),
    )(*blocks, out_weight, residual, mix_gain[None, :], norm_gain[None, :], own_target)

    def exchange(slots):
        blocks = slots.reshape(experts // 2, capacity, model_width)
        blocks = lax.all_to_all(blocks, HALF, split_axis=0, concat_axis=0, tiled=True)
        return blocks.reshape(half_slots, model_width)

    def expert(slots):
        hidden = expert_gate.shape[2]
        return pl.pallas_call(
            expert_kernel,
            out_shape=slots_shape,
            in_specs=[VMEM] * 4,
            out_specs=VMEM,
            scratch_shapes=[pltpu.VMEM((half_slots, hidden), jnp.bfloat16)],
            cost_estimate=pl.CostEstimate(
                flops=6 * half_slots * model_width * hidden,
                bytes_accessed=14 << 20,
                transcendentals=half_slots * hidden,
            ),
            compiler_params=pltpu.CompilerParams(vmem_limit_bytes=16 * 1024 * 1024),
        )(slots, expert_gate[0], expert_up[0], expert_down[0])

    def gather(bases, slots, target, weight):
        return pl.pallas_call(
            functools.partial(gather_kernel, len(bases)),
            out_shape=rows_shape,
            in_specs=[VMEM] * (len(bases) + 3),
            out_specs=VMEM,
            cost_estimate=pl.CostEstimate(
                flops=4 * row_count * half_slots * model_width,
                bytes_accessed=3 << 20,
                transcendentals=0,
            ),
            compiler_params=pltpu.CompilerParams(vmem_limit_bytes=12 * 1024 * 1024),
        )(*bases, slots, target.T, weight)

    with jax.named_scope("mirror_out"):
        far_rows = lax.ppermute(normed, "hf", mirror)
    with jax.named_scope("own_out"):
        own_in = exchange(own_out)
    far_out = pl.pallas_call(
        fill_slots,
        out_shape=slots_shape,
        in_specs=[VMEM] * 2,
        out_specs=VMEM,
        cost_estimate=pl.CostEstimate(
            flops=2 * row_count * half_slots * model_width,
            bytes_accessed=2 << 20,
            transcendentals=0,
        ),
        compiler_params=pltpu.CompilerParams(vmem_limit_bytes=12 * 1024 * 1024),
    )(far_rows, far_target)
    with jax.named_scope("far_out"):
        far_in = exchange(far_out)
    own_done = expert(own_in)
    far_done = expert(far_in)
    with jax.named_scope("far_back"):
        far_answer = exchange(far_done)
    far_sum = gather([], far_answer, far_target, far_weight)
    with jax.named_scope("mirror_back"):
        returned = lax.ppermute(far_sum, "hf", mirror)
    with jax.named_scope("own_back"):
        own_answer = exchange(own_done)
    return gather([stream, returned], own_answer, own_target, route_weight)


def solution(mesh):
    sp_size, tp_size = mesh.shape["sp"], mesh.shape["tp"]
    split = Mesh(mesh.devices.reshape(2, sp_size // 2, tp_size), ALL)
    return jax.shard_map(
        functools.partial(local, sp_size, tp_size),
        mesh=split,
        in_specs=(
            P(SP, "tp"),
            P(SP, "tp"),
            P(SP, "tp"),
            P(ALL, None),
            P(),
            P(),
            P(),
            P(ALL, None),
            P(ALL, None),
            P(ALL, None, None),
            P(ALL, None, None),
            P(ALL, None, None),
        ),
        out_specs=P(ALL, None),
        check_vma=False,
    )
```

```python
import functools
import math

import jax
import jax.numpy as jnp
from jax import lax
from jax.experimental import pallas as pl
from jax.experimental.pallas import tpu as pltpu
from jax.sharding import Mesh
from jax.sharding import PartitionSpec as P


HEAD_SIZE = 64
GRID_W = 64
HALF_KEYS = 256
ONES_ROWS = 16

epsilon = 1e-06
base_theta = 10000.0

SP = ("hf", "q")
ALL = ("hf", "q", "tp")
HALF = ("q", "tp")

VMEM = pl.BlockSpec(memory_space=pltpu.VMEM)
HBM = pl.BlockSpec(memory_space=pltpu.HBM)


def rotation_tables(first_row, row_count, lanes):
    quarter = HEAD_SIZE // 4
    lane = jnp.arange(lanes, dtype=jnp.int32) % HEAD_SIZE
    index = jnp.arange(row_count + GRID_W, dtype=jnp.int32)
    place = jnp.where(index < row_count, first_row + index, index - row_count)
    frequency = base_theta ** (-(lane % quarter).astype(jnp.float32) / quarter)
    angle = place.astype(jnp.float32)[:, None] * frequency[None, :]
    sign = jnp.where((lane // quarter) % 2 == 0, -1.0, 1.0).astype(jnp.float32)
    return jnp.cos(angle), jnp.sin(angle) * sign[None, :]


def prepare_kernel(q_hbm, k_hbm, v_hbm, cos_ref, sin_ref, q_out, kv_out, q_ref, k_ref, v_ref, sems):
    copies = [
        pltpu.make_async_copy(src, dst, sems.at[i])
        for i, (src, dst) in enumerate(((k_hbm, k_ref), (v_hbm, v_ref), (q_hbm, q_ref)))
    ]
    for copy in copies:
        copy.start()
    tok_count, lanes = k_ref.shape
    grid_rows = tok_count // GRID_W
    rows = lax.broadcasted_iota(jnp.int32, (lanes, lanes), 0)
    cols = lax.broadcasted_iota(jnp.int32, (lanes, lanes), 1)
    same_head = (rows // HEAD_SIZE) == (cols // HEAD_SIZE)
    mean_mat = jnp.where(same_head, 1.0 / HEAD_SIZE, 0.0).astype(jnp.bfloat16)
    swap_mat = jnp.where((rows ^ (HEAD_SIZE // 4)) == cols, 1.0, 0.0).astype(jnp.bfloat16)
    lane = lax.broadcasted_iota(jnp.int32, (grid_rows, GRID_W, lanes), 2)
    by_row = (lane % HEAD_SIZE) < HEAD_SIZE // 2

    def table(ref):
        row_part = ref[:grid_rows, :][:, None, :]
        col_part = ref[grid_rows:, :][None, :, :]
        return jnp.where(by_row, row_part, col_part).reshape(tok_count, lanes)

    cos, sin = table(cos_ref), table(sin_ref)

    def ready(raw, factor):
        wide = raw.astype(jnp.float32)
        square = wide * wide
        high = square.astype(jnp.bfloat16)
        low = (square - high.astype(jnp.float32)).astype(jnp.bfloat16)
        mean = jnp.dot(high, mean_mat, preferred_element_type=jnp.float32) + jnp.dot(
            low, mean_mat, preferred_element_type=jnp.float32
        )
        swapped = jnp.dot(raw, swap_mat, preferred_element_type=jnp.float32)
        length = lax.rsqrt(mean + epsilon) * factor
        return (wide * cos + swapped * sin) * length

    for copy in copies:
        copy.wait()
    keys = ready(k_ref[...], 1.0).astype(jnp.bfloat16)
    for half in range(tok_count // HALF_KEYS):
        begin = half * HALF_KEYS
        kv_out[half, :HALF_KEYS, :] = keys[begin : begin + HALF_KEYS]
        for part in range(HALF_KEYS // lanes):
            start = begin + part * lanes
            at = HALF_KEYS + part * lanes
            kv_out[half, at : at + lanes, :] = (
                v_ref[start : start + lanes, :].astype(jnp.float32).T.astype(jnp.bfloat16)
            )
    factor = math.log2(math.e) * HEAD_SIZE ** (-0.5)
    group = q_ref.shape[1] // lanes
    q_out[...] = jnp.zeros_like(q_out)
    for block in range(group):
        turned = ready(q_ref[:, block * lanes : (block + 1) * lanes], factor).T
        for inner in range(lanes // HEAD_SIZE):
            head = block * (lanes // HEAD_SIZE) + inner
            kv_head = head // group
            q_out[
                kv_head * HEAD_SIZE : (kv_head + 1) * HEAD_SIZE,
                head * tok_count : (head + 1) * tok_count,
            ] = turned[inner * HEAD_SIZE : (inner + 1) * HEAD_SIZE].astype(jnp.bfloat16)


def attend_kernel(chunk_count, first, last, staged, after, *refs):
    if staged:
        stage = pltpu.make_async_copy(refs[-4], refs[-2], refs[-1])
        stage.start()
        refs = refs[:-4] + (refs[-3],)
    if after:
        refs = refs[: 2 + chunk_count] + refs[3 + chunk_count :]
    q_ref = refs[0]
    chunks = refs[1 : 1 + chunk_count]
    acc_in = None if first else refs[1 + chunk_count]
    out_refs = refs[1 + chunk_count + (0 if first else 1) :]
    lanes, columns = q_ref.shape
    width = min(512, columns)
    blocks = columns // width
    kv_heads = lanes // HEAD_SIZE
    halves = [(c, i) for c in chunks for i in range(c.shape[0])]
    ones = jnp.ones((ONES_ROWS, HALF_KEYS), jnp.bfloat16)
    waiting = None
    for block in range(blocks + 1):
        weights = []
        total = None
        for index, (chunk, half) in enumerate(halves):
            if block < blocks:
                scores = jnp.dot(
                    chunk[half, :HALF_KEYS, :],
                    q_ref[:, block * width : (block + 1) * width],
                    preferred_element_type=jnp.float32,
                )
                weights.append(jnp.exp2(scores).astype(jnp.bfloat16))
            if waiting is not None:
                kv_head = (block - 1) * kv_heads // blocks
                values = jnp.concatenate(
                    [
                        chunk[
                            half,
                            pl.ds(HALF_KEYS + part * lanes + kv_head * HEAD_SIZE, HEAD_SIZE),
                            :,
                        ]
                        for part in range(HALF_KEYS // lanes)
                    ],
                    axis=1,
                )
                values = jnp.concatenate([values, ones], axis=0)
                piece = jnp.dot(values, waiting[index], preferred_element_type=jnp.float32)
                total = piece if total is None else total + piece
        if waiting is not None:
            at = (block - 1) * width
            if not first:
                total = total + acc_in[:, at : at + width]
            if not last:
                out_refs[0][:, at : at + width] = total
            else:
                turn = out_refs[-1]
                tp, _, per = turn.shape
                tok_count = tp * per
                ready = (total[:HEAD_SIZE] / total[HEAD_SIZE : HEAD_SIZE + 1]).astype(jnp.bfloat16)
                for piece in range(width // per):
                    head, place = divmod(at + piece * per, tok_count)
                    turn[place // per, head * HEAD_SIZE : (head + 1) * HEAD_SIZE, :] = ready[
                        :, piece * per : (piece + 1) * per
                    ]
        waiting = weights
    if staged:
        stage.wait()
    if last:
        me = lax.axis_index("tp")
        turn = out_refs[-1]
        rel = 0
        for out in out_refs[:-1]:
            for j in range(out.shape[0]):
                out[j] = turn[me ^ rel]
                rel += 1


def attend(q_ready, chunks, acc, tp_size=None, staged=None, after=None):
    first, last = acc is None, tp_size is not None
    _, columns = q_ready.shape
    rows = HEAD_SIZE + ONES_ROWS
    key_count = sum(c.shape[0] for c in chunks) * HALF_KEYS
    scratch = []
    if last:
        tok_count = chunks[0].shape[0] * HALF_KEYS * 2
        head_rows = columns // tok_count * HEAD_SIZE
        block = (head_rows, tok_count // tp_size)
        sizes = [1] + [1 << b for b in range(tp_size.bit_length() - 1)]
        shape = [jax.ShapeDtypeStruct((n, *block), jnp.bfloat16) for n in sizes]
        scratch = [pltpu.VMEM((tp_size, *block), jnp.bfloat16)]
    else:
        shape = [jax.ShapeDtypeStruct((rows, columns), jnp.float32)]
    operands = [q_ready, *chunks] + ([] if first else [acc])
    specs = [VMEM] * len(operands)
    aliases = {} if (first or last) else {len(operands) - 1: 0}
    if after is not None:
        operands.append(after)
        specs.append(HBM)
    if staged is not None:
        operands.append(staged)
        specs.append(HBM)
        shape.append(jax.ShapeDtypeStruct(staged.shape, staged.dtype))
        scratch.append(pltpu.SemaphoreType.DMA)
    out = pl.pallas_call(
        functools.partial(
            attend_kernel, len(chunks), first, last, staged is not None, after is not None
        ),
        out_shape=shape,
        in_specs=specs,
        out_specs=[VMEM] * len(shape),
        scratch_shapes=scratch,
        input_output_aliases=aliases,
        cost_estimate=pl.CostEstimate(
            flops=2 * key_count * columns * 512,
            bytes_accessed=key_count * 1024,
            transcendentals=key_count * columns,
        ),
        compiler_params=pltpu.CompilerParams(vmem_limit_bytes=24 * 1024 * 1024),
    )(*operands)
    return out if last or staged is not None else out[0]


def hypercube_exchange(pieces, tp_size):
    held = []
    for bit in reversed(range(tp_size.bit_length() - 1)):
        pairs = [(i, i ^ (1 << bit)) for i in range(tp_size)]
        half = 1 << bit
        moved = [(half, lax.ppermute(pieces[1 + bit], "tp", pairs))]
        kept = []
        for source, block in held:
            moved.append((source ^ half, lax.ppermute(block[half:], "tp", pairs)))
            kept.append((source, block[:half]))
        held = kept + moved
    return [pieces[0]] + [block for _, block in sorted(held, key=lambda item: item[0])]


def out_kernel(tp_size, top_count, *refs):
    blocks = refs[:tp_size]
    w_ref, res_ref, mix_ref, norm_ref, table_ref = refs[tp_size : tp_size + 5]
    stream_ref, normed_ref, out_ref, mixed_ref = refs[tp_size + 5 :]
    me = lax.axis_index("tp")
    _, head_rows, row_count = blocks[0].shape
    width = w_ref.shape[1]
    step = min(512, width)
    turned = [b[0].astype(jnp.float32).T.astype(jnp.bfloat16) for b in blocks]
    power = jnp.zeros((row_count, 1), jnp.float32)
    for at in range(0, width, step):
        mixed = jnp.zeros((row_count, step), jnp.float32)
        for rel in range(tp_size):
            begin = pl.multiple_of((me ^ rel) * head_rows, head_rows)
            mixed = mixed + jnp.dot(
                turned[rel],
                w_ref[pl.ds(begin, head_rows), at : at + step],
                preferred_element_type=jnp.float32,
            )
        mixed_ref[:, at : at + step] = mixed
        power = power + jnp.sum(mixed * mixed, axis=1, keepdims=True)
    scale = lax.rsqrt(power / width + epsilon)
    power = jnp.zeros((row_count, 1), jnp.float32)
    for at in range(0, width, step):
        cols = slice(at, at + step)
        stream = (
            res_ref[:, cols].astype(jnp.float32) + mixed_ref[:, cols] * scale * mix_ref[:, cols]
        ).astype(jnp.bfloat16)
        stream_ref[:, cols] = stream
        wide = stream.astype(jnp.float32)
        power = power + jnp.sum(wide * wide, axis=1, keepdims=True)
    scale = lax.rsqrt(power / width + epsilon)
    for at in range(0, width, step):
        cols = slice(at, at + step)
        wide = stream_ref[:, cols].astype(jnp.float32)
        normed_ref[:, cols] = (wide * scale * norm_ref[:, cols]).astype(jnp.bfloat16)
    fill_slots(top_count, normed_ref, table_ref, out_ref)


def routes_kernel(capacity, expert_ref, weight_ref, out_ref):
    row_count, top_count = expert_ref.shape
    lanes = out_ref.shape[1]
    lane = lax.broadcasted_iota(jnp.int32, (row_count, lanes), 1)
    before = lax.broadcasted_iota(jnp.int32, (row_count, row_count), 0) > (
        lax.broadcasted_iota(jnp.int32, (row_count, row_count), 1)
    )
    before = jnp.where(before, 1.0, 0.0).astype(jnp.bfloat16)
    taken = jnp.zeros((1, lanes), jnp.float32)
    table = jnp.zeros((row_count, lanes), jnp.float32)
    for k in range(top_count):
        expert = expert_ref[:, k : k + 1]
        onehot = jnp.where(lane == expert, 1.0, 0.0)
        earlier = taken + jnp.dot(
            before, onehot.astype(jnp.bfloat16), preferred_element_type=jnp.float32
        )
        rank = jnp.sum(onehot * earlier, axis=1, keepdims=True)
        slot = expert.astype(jnp.float32) * capacity + rank
        taken = taken + jnp.sum(onehot, axis=0, keepdims=True)
        table = jnp.where(lane == k, slot, table)
        table = jnp.where(lane == top_count + k, weight_ref[:, k : k + 1], table)
    out_ref[...] = table.T[: out_ref.shape[0], :row_count]


def fill_slots(top_count, rows_ref, table_ref, *refs):
    out_ref = refs[-1]
    row_count, width = rows_ref.shape
    step = min(512, width)
    slot_count = out_ref.shape[0]
    slots = lax.broadcasted_iota(jnp.int32, (slot_count, row_count), 0)
    slots = (slots + lax.axis_index("hf") * slot_count).astype(jnp.float32)
    hit = slots == table_ref[0:1, :]
    for k in range(1, top_count):
        hit = hit | (slots == table_ref[k : k + 1, :])
    placing = jnp.where(hit, 1.0, 0.0).astype(jnp.bfloat16)
    for at in range(0, width, step):
        cols = slice(at, at + step)
        out_ref[:, cols] = jnp.dot(
            placing, rows_ref[:, cols], preferred_element_type=jnp.float32
        ).astype(jnp.bfloat16)


def gather_kernel(base_count, top_count, *refs):
    bases = refs[:base_count]
    slots_ref, table_ref, out_ref = refs[base_count:]
    row_count, width = out_ref.shape
    slot_count = slots_ref.shape[0]
    step = min(512, width)
    table = table_ref[...].T
    slots = lax.broadcasted_iota(jnp.int32, (row_count, slot_count), 1)
    slots = (slots + lax.axis_index("hf") * slot_count).astype(jnp.float32)
    picks = [
        jnp.where(slots == table[:, k : k + 1], 1.0, 0.0).astype(jnp.bfloat16)
        for k in range(top_count)
    ]
    for at in range(0, width, step):
        cols = slice(at, at + step)
        total = None
        for base in bases:
            piece = base[:, cols].astype(jnp.float32)
            total = piece if total is None else total + piece
        for k in range(top_count):
            row = jnp.dot(picks[k], slots_ref[:, cols], preferred_element_type=jnp.float32)
            row = row * table[:, top_count + k : top_count + k + 1]
            total = row if total is None else total + row
        out_ref[:, cols] = total.astype(out_ref.dtype)


def expert_kernel(first_steps, rows_ref, gate_ref, up_ref, down_ref, *refs):
    out_ref, act_ref = refs[-2:]
    index = pl.program_id(0)
    step = gate_ref.shape[1]

    for i in range(first_steps):

        @pl.when(index == i)
        def _():
            gate = jnp.dot(rows_ref[...], gate_ref[...], preferred_element_type=jnp.float32)
            up = jnp.dot(rows_ref[...], up_ref[...], preferred_element_type=jnp.float32)
            act = gate / (1.0 + jnp.exp(-gate)) * up
            act_ref[:, i * step : (i + 1) * step] = act.astype(jnp.bfloat16)

    @pl.when(index >= first_steps)
    def _():
        out_ref[...] = jnp.dot(
            act_ref[...], down_ref[...], preferred_element_type=jnp.float32
        ).astype(jnp.bfloat16)


def layer(
    sp_size,
    tp_size,
    query_proj,
    projected_keys,
    projected_values,
    residual,
    out_weight,
    mix_gain,
    norm_gain,
    route_expert,
    route_weight,
    expert_gate,
    expert_up,
    expert_down,
):
    tok_count, lanes = projected_keys.shape
    q_heads = query_proj.shape[1] // HEAD_SIZE
    model_width = residual.shape[1]
    grid_rows = tok_count // GRID_W
    cos_table, sin_table = rotation_tables(lax.axis_index(SP) * grid_rows, grid_rows, lanes)
    q_ready, kv_own = pl.pallas_call(
        prepare_kernel,
        out_shape=(
            jax.ShapeDtypeStruct((lanes, q_heads * tok_count), jnp.bfloat16),
            jax.ShapeDtypeStruct((tok_count // HALF_KEYS, 2 * HALF_KEYS, lanes), jnp.bfloat16),
        ),
        in_specs=[HBM] * 3 + [VMEM] * 2,
        out_specs=(VMEM, VMEM),
        scratch_shapes=[
            pltpu.VMEM(query_proj.shape, jnp.bfloat16),
            pltpu.VMEM(projected_keys.shape, jnp.bfloat16),
            pltpu.VMEM(projected_values.shape, jnp.bfloat16),
            pltpu.SemaphoreType.DMA((3,)),
        ],
        cost_estimate=pl.CostEstimate(
            flops=2 * tok_count * 512 * 512, bytes_accessed=1 << 20, transcendentals=0
        ),
    )(query_proj, projected_keys, projected_values, cos_table, sin_table)

    row_count = residual.shape[0]
    top_count = route_expert.shape[1]
    experts = sp_size * tp_size
    capacity = max(2, 2 * top_count * row_count // experts)
    half_slots = experts // 2 * capacity
    mirror = [(0, 1), (1, 0)]
    table = pl.pallas_call(
        functools.partial(routes_kernel, capacity),
        out_shape=jax.ShapeDtypeStruct((8, row_count), jnp.float32),
        in_specs=[VMEM] * 2,
        out_specs=VMEM,
        cost_estimate=pl.CostEstimate(flops=1 << 22, bytes_accessed=1 << 17, transcendentals=0),
        compiler_params=pltpu.CompilerParams(vmem_limit_bytes=8 * 1024 * 1024),
    )(route_expert, route_weight)
    far_table = lax.ppermute(table, "hf", mirror)

    order = list(range(0, sp_size, 2)) + list(range(sp_size - 1, 0, -2))
    ahead = [(order[i], order[(i + 1) % sp_size]) for i in range(sp_size)]
    behind = [(b, a) for a, b in ahead]
    steps = sp_size // 2
    acc = None
    from_left = from_right = kv_own
    held = [kv_own]
    for step in range(steps):
        if step == steps - 1:
            halves = kv_own.shape[0]
            from_left, from_right = from_left[: halves // 2], from_right[halves // 2 :]
        next_left = lax.ppermute(from_left, SP, ahead)
        next_right = lax.ppermute(from_right, SP, behind)
        if step == steps - 1:
            acc, staged_weight = attend(
                q_ready, held, acc, staged=out_weight, after=far_table
            )
        else:
            acc = attend(q_ready, held, acc)
        from_left, from_right = next_left, next_right
        held = [from_left, from_right]
    pieces = attend(q_ready, held, acc, tp_size)
    blocks = hypercube_exchange(pieces, tp_size)

    rows_shape = jax.ShapeDtypeStruct((row_count, model_width), jnp.bfloat16)
    slots_shape = jax.ShapeDtypeStruct((half_slots, model_width), jnp.bfloat16)
    stream, normed, own_out = pl.pallas_call(
        functools.partial(out_kernel, tp_size, top_count),
        out_shape=(rows_shape, rows_shape, slots_shape),
        in_specs=[VMEM] * (tp_size + 5),
        out_specs=(VMEM, VMEM, VMEM),
        scratch_shapes=[pltpu.VMEM((row_count, model_width), jnp.float32)],
        cost_estimate=pl.CostEstimate(
            flops=2 * row_count * model_width * (out_weight.shape[0] + half_slots),
            bytes_accessed=8 << 20,
            transcendentals=0,
        ),
        compiler_params=pltpu.CompilerParams(vmem_limit_bytes=12 * 1024 * 1024),
    )(*blocks, staged_weight, residual, mix_gain[None, :], norm_gain[None, :], table)

    def exchange(slots):
        blocks = slots.reshape(experts // 2, capacity, model_width)
        blocks = lax.all_to_all(blocks, HALF, split_axis=0, concat_axis=0, tiled=True)
        return blocks.reshape(half_slots, model_width)

    def expert(slots, after):
        hidden = expert_gate.shape[2]
        step = min(256, hidden)
        first_steps = hidden // step
        out_step = min(512, model_width)
        return pl.pallas_call(
            functools.partial(expert_kernel, first_steps),
            out_shape=slots_shape,
            grid=(first_steps + model_width // out_step,),
            in_specs=[
                pl.BlockSpec((half_slots, model_width), lambda i: (0, 0)),
                pl.BlockSpec(
                    (None, model_width, step), lambda i: (0, 0, jnp.minimum(i, first_steps - 1))
                ),
                pl.BlockSpec(
                    (None, model_width, step), lambda i: (0, 0, jnp.minimum(i, first_steps - 1))
                ),
                pl.BlockSpec(
                    (None, hidden, out_step), lambda i: (0, 0, jnp.maximum(i - first_steps, 0))
                ),
            ]
            + [HBM] * len(after),
            out_specs=pl.BlockSpec(
                (half_slots, out_step), lambda i: (0, jnp.maximum(i - first_steps, 0))
            ),
            scratch_shapes=[pltpu.VMEM((half_slots, hidden), jnp.bfloat16)],
            cost_estimate=pl.CostEstimate(
                flops=6 * half_slots * model_width * hidden,
                bytes_accessed=14 << 20,
                transcendentals=half_slots * hidden,
            ),
        )(slots, expert_gate, expert_up, expert_down, *after)

    def gather(bases, slots, table):
        return pl.pallas_call(
            functools.partial(gather_kernel, len(bases), top_count),
            out_shape=rows_shape,
            in_specs=[VMEM] * (len(bases) + 2),
            out_specs=VMEM,
            cost_estimate=pl.CostEstimate(
                flops=4 * row_count * half_slots * model_width,
                bytes_accessed=3 << 20,
                transcendentals=0,
            ),
            compiler_params=pltpu.CompilerParams(vmem_limit_bytes=12 * 1024 * 1024),
        )(*bases, slots, table)

    far_rows = lax.ppermute(normed, "hf", mirror)
    own_in = exchange(own_out)
    far_out = pl.pallas_call(
        functools.partial(fill_slots, top_count),
        out_shape=slots_shape,
        in_specs=[VMEM] * 2 + [HBM],
        out_specs=VMEM,
        cost_estimate=pl.CostEstimate(
            flops=2 * row_count * half_slots * model_width,
            bytes_accessed=2 << 20,
            transcendentals=0,
        ),
        compiler_params=pltpu.CompilerParams(vmem_limit_bytes=12 * 1024 * 1024),
    )(far_rows, far_table, own_in)
    far_in = exchange(far_out)
    own_done = expert(own_in, [])
    far_done = expert(far_in, [own_done])
    far_answer = exchange(far_done)
    far_sum = gather([], far_answer, far_table)
    returned = lax.ppermute(far_sum, "hf", mirror)
    own_answer = exchange(own_done)
    return gather([stream, returned], own_answer, table)


def solution(mesh):
    sp_size, tp_size = mesh.shape["sp"], mesh.shape["tp"]
    split = Mesh(mesh.devices.reshape(2, sp_size // 2, tp_size), ALL)
    return jax.shard_map(
        functools.partial(layer, sp_size, tp_size),
        mesh=split,
        in_specs=(
            P(SP, "tp"),
            P(SP, "tp"),
            P(SP, "tp"),
            P(ALL, None),
            P(),
            P(),
            P(),
            P(ALL, None),
            P(ALL, None),
            P(ALL, None, None),
            P(ALL, None, None),
            P(ALL, None, None),
        ),
        out_specs=P(ALL, None),
        check_vma=False,
    )
```

```python
import functools
import math

import jax
import jax.numpy as jnp
from jax import lax
from jax.experimental import pallas as pl
from jax.experimental.pallas import tpu as pltpu
from jax.sharding import PartitionSpec as P

HEAD_SIZE = 64
GRID_W = 64
HALF_KEYS = 256
ONES_ROWS = 16

epsilon = 1e-06
base_theta = 10000.0

VMEM = pl.BlockSpec(memory_space=pltpu.VMEM)
HBM = pl.BlockSpec(memory_space=pltpu.HBM)


def rotation_tables(row_count, lanes):
    quarter = HEAD_SIZE // 4
    lane = jnp.arange(lanes, dtype=jnp.int32) % HEAD_SIZE
    index = jnp.arange(row_count + GRID_W, dtype=jnp.int32)
    place = jnp.where(index < row_count, index, index - row_count)
    frequency = base_theta ** (-(lane % quarter).astype(jnp.float32) / quarter)
    angle = place.astype(jnp.float32)[:, None] * frequency[None, :]
    sign = jnp.where((lane // quarter) % 2 == 0, -1.0, 1.0).astype(jnp.float32)
    return jnp.cos(angle), jnp.sin(angle) * sign[None, :]


def pack_kernel(k_hbm, v_hbm, out_ref, sems):
    halves = out_ref.shape[0]
    copies = [
        pltpu.make_async_copy(
            src.at[pl.ds(half * HALF_KEYS, HALF_KEYS), :], out_ref.at[half, i], sems.at[half, i]
        )
        for half in range(halves)
        for i, src in enumerate((k_hbm, v_hbm))
    ]
    for copy in copies:
        copy.start()
    for copy in copies:
        copy.wait()


class Rotation:
    def __init__(self, cos_ref, sin_ref, lanes):
        rows = lax.broadcasted_iota(jnp.int32, (lanes, lanes), 0)
        cols = lax.broadcasted_iota(jnp.int32, (lanes, lanes), 1)
        same_head = (rows // HEAD_SIZE) == (cols // HEAD_SIZE)
        self.mean_mat = jnp.where(same_head, 1.0 / HEAD_SIZE, 0.0).astype(jnp.bfloat16)
        self.swap_mat = jnp.where((rows ^ (HEAD_SIZE // 4)) == cols, 1.0, 0.0).astype(jnp.bfloat16)
        lane = lax.broadcasted_iota(jnp.int32, (GRID_W, lanes), 1)
        self.by_row = (lane % HEAD_SIZE) < HEAD_SIZE // 2
        self.refs = (cos_ref, sin_ref)

    def table(self, ref, first_row, count):
        total = ref.shape[0] - GRID_W
        cols = ref[total:, :]
        parts = [
            jnp.where(self.by_row, ref[pl.ds(first_row + i, 1), :], cols) for i in range(count)
        ]
        return jnp.concatenate(parts, axis=0)

    def ready(self, raw, first_row, factor):
        count = raw.shape[0] // GRID_W
        cos = self.table(self.refs[0], first_row, count)
        sin = self.table(self.refs[1], first_row, count)
        wide = raw.astype(jnp.float32)
        square = wide * wide
        high = square.astype(jnp.bfloat16)
        low = (square - high.astype(jnp.float32)).astype(jnp.bfloat16)
        mean = jnp.dot(high, self.mean_mat, preferred_element_type=jnp.float32) + jnp.dot(
            low, self.mean_mat, preferred_element_type=jnp.float32
        )
        swapped = jnp.dot(raw, self.swap_mat, preferred_element_type=jnp.float32)
        length = lax.rsqrt(mean + epsilon) * factor
        return (wide * cos + swapped * sin) * length


def ring_place(index, count):
    return jnp.where(index % 2 == 0, index // 2, count - (index + 1) // 2)


def ring_member(place, count):
    place = lax.rem(place + count, count)
    return jnp.where(2 * place < count, 2 * place, 2 * (count - place) - 1)


def attend_kernel(sp_size, pieces, last, raw_queries, after, *refs):
    refs = list(refs)
    first_ref = refs.pop(0)
    cos_ref, sin_ref = refs.pop(0), refs.pop(0)
    chunks = [refs.pop(0) for _ in pieces]
    acc_in = None if raw_queries else refs.pop(0)
    for _ in range(after):
        refs.pop(0)
    outs = [refs.pop(0) for _ in range(2 if raw_queries else 1)] if not last else None
    if last:
        outs, refs = refs[:-3], refs[-3:]
    keys_ref, values_ref = refs[0], refs[1]
    lanes = chunks[0].shape[-1]
    rotation = Rotation(cos_ref, sin_ref, lanes)
    me = lax.axis_index("sp")
    place = ring_place(me, sp_size)
    grid_rows = (cos_ref.shape[0] - GRID_W) // sp_size
    if raw_queries:
        q_ref = outs[0]
        factor = math.log2(math.e) * HEAD_SIZE ** (-0.5)
        tok_count, q_lanes = first_ref.shape
        group = q_lanes // lanes
        q_ref[...] = jnp.zeros_like(q_ref)
        for block in range(group):
            raw = first_ref[:, block * lanes : (block + 1) * lanes]
            turned = rotation.ready(raw, me * grid_rows, factor).T
            for inner in range(lanes // HEAD_SIZE):
                head = block * (lanes // HEAD_SIZE) + inner
                kv_head = head // group
                q_ref[
                    kv_head * HEAD_SIZE : (kv_head + 1) * HEAD_SIZE,
                    head * tok_count : (head + 1) * tok_count,
                ] = turned[inner * HEAD_SIZE : (inner + 1) * HEAD_SIZE].astype(jnp.bfloat16)
    else:
        q_ref = first_ref
    _, columns = q_ref.shape
    width = min(512, columns)
    blocks = columns // width
    kv_heads = lanes // HEAD_SIZE
    ones = jnp.ones((ONES_ROWS, HALF_KEYS), jnp.bfloat16)
    rows = HEAD_SIZE + ONES_ROWS
    halves = 0
    for chunk, (distance, first_half) in zip(chunks, pieces):
        source = ring_member(place + distance, sp_size)
        for half in range(chunk.shape[0]):
            row = source * grid_rows + (first_half + half) * (HALF_KEYS // GRID_W)
            keys_ref[halves] = rotation.ready(chunk[half, 0], row, 1.0).astype(jnp.bfloat16)
            turned = chunk[half, 1].astype(jnp.float32).T.astype(jnp.bfloat16)
            for head in range(kv_heads):
                values_ref[halves, head, :HEAD_SIZE, :] = turned[
                    head * HEAD_SIZE : (head + 1) * HEAD_SIZE
                ]
                values_ref[halves, head, HEAD_SIZE:, :] = ones
            halves += 1
    waiting = None
    for block in range(blocks + 1):
        weights = []
        total = None
        for half in range(halves):
            if block < blocks:
                scores = jnp.dot(
                    keys_ref[half],
                    q_ref[:, block * width : (block + 1) * width],
                    preferred_element_type=jnp.float32,
                )
                weights.append(jnp.exp2(scores).astype(jnp.bfloat16))
            if waiting is not None:
                kv_head = (block - 1) * kv_heads // blocks
                piece = jnp.dot(
                    values_ref[half, kv_head], waiting[half], preferred_element_type=jnp.float32
                )
                total = piece if total is None else total + piece
        if waiting is not None:
            at = (block - 1) * width
            if acc_in is not None:
                total = total + acc_in[:, at : at + width]
            if not last:
                outs[-1][:, at : at + width] = total
            else:
                turn = refs[2]
                tp, head_rows, per = turn.shape
                tok_count = tp * per
                ready = (total[:HEAD_SIZE] / total[HEAD_SIZE : HEAD_SIZE + 1]).astype(jnp.bfloat16)
                for piece in range(width // per):
                    head, spot = divmod(at + piece * per, tok_count)
                    turn[spot // per, head * HEAD_SIZE : (head + 1) * HEAD_SIZE, :] = ready[
                        :, piece * per : (piece + 1) * per
                    ]
        waiting = weights
    if last:
        me = lax.axis_index("tp")
        rel = 0
        for out in outs:
            for j in range(out.shape[0]):
                out[j] = refs[2][me ^ rel]
                rel += 1


def attend(queries, tables, chunks, pieces, acc, sp_size, tp_size, last=False, after=()):
    raw_queries = acc is None
    lanes = chunks[0].shape[-1]
    rows = HEAD_SIZE + ONES_ROWS
    halves = sum(c.shape[0] for c in chunks)
    if raw_queries:
        columns = queries.shape[0] * queries.shape[1] // HEAD_SIZE
        tok_count = queries.shape[0]
    else:
        columns = queries.shape[1]
        tok_count = chunks[0].shape[0] * HALF_KEYS * 2
    scratch = [
        pltpu.VMEM((halves, HALF_KEYS, lanes), jnp.bfloat16),
        pltpu.VMEM((halves, lanes // HEAD_SIZE, rows, HALF_KEYS), jnp.bfloat16),
    ]
    if last:
        head_rows = columns // tok_count * HEAD_SIZE
        block = (head_rows, tok_count // tp_size)
        sizes = [1] + [1 << b for b in range(tp_size.bit_length() - 1)]
        shape = [jax.ShapeDtypeStruct((n, *block), jnp.bfloat16) for n in sizes]
        scratch.append(pltpu.VMEM((tp_size, *block), jnp.bfloat16))
    else:
        shape = [jax.ShapeDtypeStruct((rows, columns), jnp.float32)]
        if raw_queries:
            shape = [jax.ShapeDtypeStruct((lanes, columns), jnp.bfloat16)] + shape
    operands = [queries, *tables, *chunks] + ([] if raw_queries else [acc])
    aliases = {} if (raw_queries or last) else {len(operands) - 1: 0}
    key_count = halves * HALF_KEYS
    return pl.pallas_call(
        functools.partial(attend_kernel, sp_size, pieces, last, raw_queries, len(after)),
        out_shape=shape,
        in_specs=[VMEM] * len(operands) + [HBM] * len(after),
        out_specs=[VMEM] * len(shape),
        scratch_shapes=scratch,
        input_output_aliases=aliases,
        cost_estimate=pl.CostEstimate(
            flops=2 * key_count * columns * 512,
            bytes_accessed=key_count * 1024,
            transcendentals=key_count * columns,
        ),
        compiler_params=pltpu.CompilerParams(vmem_limit_bytes=24 * 1024 * 1024),
    )(*operands, *after)


def hypercube_exchange(pieces, tp_size):
    held = []
    for bit in reversed(range(tp_size.bit_length() - 1)):
        pairs = [(i, i ^ (1 << bit)) for i in range(tp_size)]
        half = 1 << bit
        moved = [(half, lax.ppermute(pieces[1 + bit], "tp", pairs))]
        kept = []
        for source, block in held:
            moved.append((source ^ half, lax.ppermute(block[half:], "tp", pairs)))
            kept.append((source, block[:half]))
        held = kept + moved
    return [pieces[0]] + [block for _, block in sorted(held, key=lambda item: item[0])]


def out_kernel(tp_size, top_count, *refs):
    blocks = refs[:tp_size]
    w_ref, res_ref, mix_ref, norm_ref, table_ref = refs[tp_size : tp_size + 5]
    stream_ref, out_ref, normed_ref, mixed_ref = refs[tp_size + 5 :]
    me = lax.axis_index("tp")
    _, head_rows, row_count = blocks[0].shape
    width = w_ref.shape[1]
    step = min(512, width)
    turned = [b[0].astype(jnp.float32).T.astype(jnp.bfloat16) for b in blocks]
    power = jnp.zeros((row_count, 1), jnp.float32)
    for at in range(0, width, step):
        mixed = jnp.zeros((row_count, step), jnp.float32)
        for rel in range(tp_size):
            begin = pl.multiple_of((me ^ rel) * head_rows, head_rows)
            mixed = mixed + jnp.dot(
                turned[rel],
                w_ref[pl.ds(begin, head_rows), at : at + step],
                preferred_element_type=jnp.float32,
            )
        mixed_ref[:, at : at + step] = mixed
        power = power + jnp.sum(mixed * mixed, axis=1, keepdims=True)
    scale = lax.rsqrt(power / width + epsilon)
    power = jnp.zeros((row_count, 1), jnp.float32)
    for at in range(0, width, step):
        cols = slice(at, at + step)
        stream = (
            res_ref[:, cols].astype(jnp.float32) + mixed_ref[:, cols] * scale * mix_ref[:, cols]
        ).astype(jnp.bfloat16)
        stream_ref[:, cols] = stream
        wide = stream.astype(jnp.float32)
        power = power + jnp.sum(wide * wide, axis=1, keepdims=True)
    scale = lax.rsqrt(power / width + epsilon)
    for at in range(0, width, step):
        cols = slice(at, at + step)
        wide = stream_ref[:, cols].astype(jnp.float32)
        normed_ref[:, cols] = (wide * scale * norm_ref[:, cols]).astype(jnp.bfloat16)
    fill_slots(top_count, normed_ref, table_ref, out_ref)


def routes_kernel(capacity, expert_ref, weight_ref, out_ref):
    row_count, top_count = expert_ref.shape
    lanes = out_ref.shape[1]
    lane = lax.broadcasted_iota(jnp.int32, (row_count, lanes), 1)
    before = lax.broadcasted_iota(jnp.int32, (row_count, row_count), 0) > (
        lax.broadcasted_iota(jnp.int32, (row_count, row_count), 1)
    )
    before = jnp.where(before, 1.0, 0.0).astype(jnp.bfloat16)
    taken = jnp.zeros((1, lanes), jnp.float32)
    table = jnp.zeros((row_count, lanes), jnp.float32)
    for k in range(top_count):
        expert = expert_ref[:, k : k + 1]
        onehot = jnp.where(lane == expert, 1.0, 0.0)
        earlier = taken + jnp.dot(
            before, onehot.astype(jnp.bfloat16), preferred_element_type=jnp.float32
        )
        rank = jnp.sum(onehot * earlier, axis=1, keepdims=True)
        slot = expert.astype(jnp.float32) * capacity + rank
        taken = taken + jnp.sum(onehot, axis=0, keepdims=True)
        table = jnp.where(lane == k, slot, table)
        table = jnp.where(lane == top_count + k, weight_ref[:, k : k + 1], table)
    out_ref[...] = table.T[: out_ref.shape[0], :row_count]


def fill_slots(top_count, rows_ref, table_ref, out_ref):
    row_count, width = rows_ref.shape
    step = min(512, width)
    slot_count = out_ref.shape[0]
    slots = lax.broadcasted_iota(jnp.int32, (slot_count, row_count), 0)
    slots = slots.astype(jnp.float32)
    hit = slots == table_ref[0:1, :]
    for k in range(1, top_count):
        hit = hit | (slots == table_ref[k : k + 1, :])
    placing = jnp.where(hit, 1.0, 0.0).astype(jnp.bfloat16)
    for at in range(0, width, step):
        cols = slice(at, at + step)
        out_ref[:, cols] = jnp.dot(
            placing, rows_ref[:, cols], preferred_element_type=jnp.float32
        ).astype(jnp.bfloat16)


def gather_kernel(base_count, top_count, *refs):
    bases = refs[:base_count]
    slots_ref, table_ref, out_ref = refs[base_count:]
    row_count, width = out_ref.shape
    slot_count = slots_ref.shape[0]
    step = min(512, width)
    table = table_ref[...].T
    slots = lax.broadcasted_iota(jnp.int32, (row_count, slot_count), 1)
    slots = slots.astype(jnp.float32)
    picks = [
        jnp.where(slots == table[:, k : k + 1], 1.0, 0.0).astype(jnp.bfloat16)
        for k in range(top_count)
    ]
    for at in range(0, width, step):
        cols = slice(at, at + step)
        total = None
        for base in bases:
            piece = base[:, cols].astype(jnp.float32)
            total = piece if total is None else total + piece
        for k in range(top_count):
            row = jnp.dot(picks[k], slots_ref[:, cols], preferred_element_type=jnp.float32)
            row = row * table[:, top_count + k : top_count + k + 1]
            total = row if total is None else total + row
        out_ref[:, cols] = total.astype(out_ref.dtype)


def expert_kernel(rows_ref, gate_ref, up_ref, down_ref, out_ref, act_ref):
    hidden = gate_ref.shape[1]
    width = down_ref.shape[1]
    step = min(256, hidden)
    for at in range(0, hidden, step):
        cols = slice(at, at + step)
        gate = jnp.dot(rows_ref[...], gate_ref[:, cols], preferred_element_type=jnp.float32)
        up = jnp.dot(rows_ref[...], up_ref[:, cols], preferred_element_type=jnp.float32)
        act_ref[:, cols] = (gate / (1.0 + jnp.exp(-gate)) * up).astype(jnp.bfloat16)
    step = min(512, width)
    for at in range(0, width, step):
        cols = slice(at, at + step)
        out_ref[:, cols] = jnp.dot(
            act_ref[...], down_ref[:, cols], preferred_element_type=jnp.float32
        ).astype(jnp.bfloat16)


def local(
    sp_size,
    tp_size,
    query_proj,
    projected_keys,
    projected_values,
    residual,
    out_weight,
    mix_gain,
    norm_gain,
    route_expert,
    route_weight,
    expert_gate,
    expert_up,
    expert_down,
):
    tok_count, lanes = projected_keys.shape
    q_heads = query_proj.shape[1] // HEAD_SIZE
    model_width = residual.shape[1]
    halves = tok_count // HALF_KEYS
    tables = rotation_tables(sp_size * tok_count // GRID_W, lanes)
    raw_own = pl.pallas_call(
        pack_kernel,
        out_shape=jax.ShapeDtypeStruct((halves, 2, HALF_KEYS, lanes), jnp.bfloat16),
        in_specs=[HBM, HBM],
        out_specs=VMEM,
        scratch_shapes=[pltpu.SemaphoreType.DMA((halves, 2))],
        cost_estimate=pl.CostEstimate(flops=1 << 20, bytes_accessed=1 << 19, transcendentals=0),
    )(projected_keys, projected_values)

    row_count = residual.shape[0]
    top_count = route_expert.shape[1]
    experts = sp_size * tp_size
    capacity = max(2, 2 * top_count * row_count // experts)
    slots_total = experts * capacity
    table = pl.pallas_call(
        functools.partial(routes_kernel, capacity),
        out_shape=jax.ShapeDtypeStruct((8, row_count), jnp.float32),
        in_specs=[VMEM] * 2,
        out_specs=VMEM,
        cost_estimate=pl.CostEstimate(flops=1 << 22, bytes_accessed=1 << 17, transcendentals=0),
        compiler_params=pltpu.CompilerParams(vmem_limit_bytes=8 * 1024 * 1024),
    )(route_expert, route_weight)

    order = list(range(0, sp_size, 2)) + list(range(sp_size - 1, 0, -2))
    ahead = [(order[i], order[(i + 1) % sp_size]) for i in range(sp_size)]
    behind = [(b, a) for a, b in ahead]
    steps = sp_size // 2
    acc = None
    queries = query_proj
    from_left = from_right = raw_own
    held, pieces = [raw_own], [(0, 0)]
    for step in range(steps):
        if step == steps - 1:
            from_left, from_right = from_left[: halves // 2], from_right[halves // 2 :]
        next_left = lax.ppermute(from_left, "sp", ahead)
        next_right = lax.ppermute(from_right, "sp", behind)
        after = (table,) if step == steps - 1 else ()
        out = attend(queries, tables, held, pieces, acc, sp_size, tp_size, after=after)
        if step == 0:
            queries, acc = out
        else:
            (acc,) = out
        from_left, from_right = next_left, next_right
        held = [from_left, from_right]
        pieces = [(-step - 1, 0), (step + 1, halves // 2 if step == steps - 1 else 0)]
    pieces = attend(queries, tables, held, pieces, acc, sp_size, tp_size, last=True)
    blocks = hypercube_exchange(pieces, tp_size)

    rows_shape = jax.ShapeDtypeStruct((row_count, model_width), jnp.bfloat16)
    slots_shape = jax.ShapeDtypeStruct((slots_total, model_width), jnp.bfloat16)
    stream, outgoing = pl.pallas_call(
        functools.partial(out_kernel, tp_size, top_count),
        out_shape=(rows_shape, slots_shape),
        in_specs=[VMEM] * (tp_size + 5),
        out_specs=(VMEM, VMEM),
        scratch_shapes=[
            pltpu.VMEM((row_count, model_width), jnp.bfloat16),
            pltpu.VMEM((row_count, model_width), jnp.float32),
        ],
        cost_estimate=pl.CostEstimate(
            flops=2 * row_count * model_width * (out_weight.shape[0] + slots_total),
            bytes_accessed=8 << 20,
            transcendentals=0,
        ),
        compiler_params=pltpu.CompilerParams(vmem_limit_bytes=12 * 1024 * 1024),
    )(*blocks, out_weight, residual, mix_gain[None, :], norm_gain[None, :], table)

    def exchange(slots):
        slots = slots.reshape(experts, capacity, model_width)
        slots = lax.all_to_all(slots, ("sp", "tp"), split_axis=0, concat_axis=0, tiled=True)
        return slots.reshape(slots_total, model_width)

    hidden = expert_gate.shape[2]
    done = pl.pallas_call(
        expert_kernel,
        out_shape=slots_shape,
        in_specs=[VMEM] * 4,
        out_specs=VMEM,
        scratch_shapes=[pltpu.VMEM((slots_total, hidden), jnp.bfloat16)],
        cost_estimate=pl.CostEstimate(
            flops=6 * slots_total * model_width * hidden,
            bytes_accessed=16 << 20,
            transcendentals=slots_total * hidden,
        ),
        compiler_params=pltpu.CompilerParams(vmem_limit_bytes=24 * 1024 * 1024),
    )(exchange(outgoing), expert_gate[0], expert_up[0], expert_down[0])
    return pl.pallas_call(
        functools.partial(gather_kernel, 1, top_count),
        out_shape=rows_shape,
        in_specs=[VMEM] * 3,
        out_specs=VMEM,
        cost_estimate=pl.CostEstimate(
            flops=4 * row_count * slots_total * model_width,
            bytes_accessed=3 << 20,
            transcendentals=0,
        ),
        compiler_params=pltpu.CompilerParams(vmem_limit_bytes=12 * 1024 * 1024),
    )(stream, exchange(done), table)


def solution(mesh):
    return jax.shard_map(
        functools.partial(local, mesh.shape["sp"], mesh.shape["tp"]),
        mesh=mesh,
        in_specs=(
            P("sp", "tp"),
            P("sp", "tp"),
            P("sp", "tp"),
            P(("sp", "tp"), None),
            P(),
            P(),
            P(),
            P(("sp", "tp"), None),
            P(("sp", "tp"), None),
            P(("sp", "tp"), None, None),
            P(("sp", "tp"), None, None),
            P(("sp", "tp"), None, None),
        ),
        out_specs=P(("sp", "tp"), None),
        check_vma=False,
    )
```

```python
import functools
import math

import jax
import jax.numpy as jnp
from jax import lax
from jax.experimental import pallas as pl
from jax.experimental.pallas import tpu as pltpu
from jax.sharding import PartitionSpec as P

HEAD_SIZE = 64
GRID_W = 64
HALF_KEYS = 256
ONES_ROWS = 16

epsilon = 1e-06
base_theta = 10000.0

VMEM = pl.BlockSpec(memory_space=pltpu.VMEM)
HBM = pl.BlockSpec(memory_space=pltpu.HBM)


def rotation_tables(row_count, lanes):
    quarter = HEAD_SIZE // 4
    lane = jnp.arange(lanes, dtype=jnp.int32) % HEAD_SIZE
    index = jnp.arange(row_count + GRID_W, dtype=jnp.int32)
    place = jnp.where(index < row_count, index, index - row_count)
    frequency = base_theta ** (-(lane % quarter).astype(jnp.float32) / quarter)
    angle = place.astype(jnp.float32)[:, None] * frequency[None, :]
    sign = jnp.where((lane // quarter) % 2 == 0, -1.0, 1.0).astype(jnp.float32)
    return jnp.cos(angle), jnp.sin(angle) * sign[None, :]


class Rotation:
    def __init__(self, cos_ref, sin_ref, lanes):
        rows = lax.broadcasted_iota(jnp.int32, (lanes, lanes), 0)
        cols = lax.broadcasted_iota(jnp.int32, (lanes, lanes), 1)
        same_head = (rows // HEAD_SIZE) == (cols // HEAD_SIZE)
        self.mean_mat = jnp.where(same_head, 1.0 / HEAD_SIZE, 0.0).astype(jnp.bfloat16)
        self.swap_mat = jnp.where((rows ^ (HEAD_SIZE // 4)) == cols, 1.0, 0.0).astype(jnp.bfloat16)
        lane = lax.broadcasted_iota(jnp.int32, (GRID_W, lanes), 1)
        self.by_row = (lane % HEAD_SIZE) < HEAD_SIZE // 2
        self.refs = (cos_ref, sin_ref)

    def table(self, ref, first_row, count):
        total = ref.shape[0] - GRID_W
        cols = ref[total:, :]
        parts = [
            jnp.where(self.by_row, ref[pl.ds(first_row + i, 1), :], cols) for i in range(count)
        ]
        return jnp.concatenate(parts, axis=0)

    def ready(self, raw, first_row, factor):
        count = raw.shape[0] // GRID_W
        cos = self.table(self.refs[0], first_row, count)
        sin = self.table(self.refs[1], first_row, count)
        wide = raw.astype(jnp.float32)
        square = wide * wide
        high = square.astype(jnp.bfloat16)
        low = (square - high.astype(jnp.float32)).astype(jnp.bfloat16)
        mean = jnp.dot(high, self.mean_mat, preferred_element_type=jnp.float32) + jnp.dot(
            low, self.mean_mat, preferred_element_type=jnp.float32
        )
        swapped = jnp.dot(raw, self.swap_mat, preferred_element_type=jnp.float32)
        length = lax.rsqrt(mean + epsilon) * factor
        return (wide * cos + swapped * sin) * length


def ring_place(index, count):
    return jnp.where(index % 2 == 0, index // 2, count - (index + 1) // 2)


def ring_member(place, count):
    place = lax.rem(place + count, count)
    return jnp.where(2 * place < count, 2 * place, 2 * (count - place) - 1)


def attend_kernel(sp_size, pieces, last, raw_queries, after, *refs):
    refs = list(refs)
    first_ref = refs.pop(0)
    cos_ref, sin_ref = refs.pop(0), refs.pop(0)
    chunks = [refs.pop(0) for _ in pieces]
    acc_in = None if raw_queries else refs.pop(0)
    for _ in range(after):
        refs.pop(0)
    outs = [refs.pop(0) for _ in range(2 if raw_queries else 1)] if not last else None
    if last:
        outs, refs = refs[:-3], refs[-3:]
    keys_ref, values_ref = refs[0], refs[1]
    lanes = chunks[0].shape[-1]
    rotation = Rotation(cos_ref, sin_ref, lanes)
    me = lax.axis_index("sp")
    place = ring_place(me, sp_size)
    grid_rows = (cos_ref.shape[0] - GRID_W) // sp_size
    if raw_queries:
        q_ref = outs[0]
        factor = math.log2(math.e) * HEAD_SIZE ** (-0.5)
        tok_count, q_lanes = first_ref.shape
        group = q_lanes // lanes
        q_ref[...] = jnp.zeros_like(q_ref)
        for block in range(group):
            raw = first_ref[:, block * lanes : (block + 1) * lanes]
            turned = rotation.ready(raw, me * grid_rows, factor).T
            for inner in range(lanes // HEAD_SIZE):
                head = block * (lanes // HEAD_SIZE) + inner
                kv_head = head // group
                q_ref[
                    kv_head * HEAD_SIZE : (kv_head + 1) * HEAD_SIZE,
                    head * tok_count : (head + 1) * tok_count,
                ] = turned[inner * HEAD_SIZE : (inner + 1) * HEAD_SIZE].astype(jnp.bfloat16)
    else:
        q_ref = first_ref
    _, columns = q_ref.shape
    width = min(512, columns)
    blocks = columns // width
    kv_heads = lanes // HEAD_SIZE
    ones = jnp.ones((ONES_ROWS, HALF_KEYS), jnp.bfloat16)
    rows = HEAD_SIZE + ONES_ROWS
    halves = 0
    for chunk, (distance, first_half) in zip(chunks, pieces):
        source = ring_member(place + distance, sp_size)
        for half in range(chunk.shape[0]):
            row = source * grid_rows + (first_half + half) * (HALF_KEYS // GRID_W)
            keys_ref[halves] = rotation.ready(chunk[half, 0], row, 1.0).astype(jnp.bfloat16)
            turned = chunk[half, 1].astype(jnp.float32).T.astype(jnp.bfloat16)
            for head in range(kv_heads):
                values_ref[halves, head, :HEAD_SIZE, :] = turned[
                    head * HEAD_SIZE : (head + 1) * HEAD_SIZE
                ]
                values_ref[halves, head, HEAD_SIZE:, :] = ones
            halves += 1
    waiting = None
    for block in range(blocks + 1):
        weights = []
        total = None
        for half in range(halves):
            if block < blocks:
                scores = jnp.dot(
                    keys_ref[half],
                    q_ref[:, block * width : (block + 1) * width],
                    preferred_element_type=jnp.float32,
                )
                weights.append(jnp.exp2(scores).astype(jnp.bfloat16))
            if waiting is not None:
                kv_head = (block - 1) * kv_heads // blocks
                piece = jnp.dot(
                    values_ref[half, kv_head], waiting[half], preferred_element_type=jnp.float32
                )
                total = piece if total is None else total + piece
        if waiting is not None:
            at = (block - 1) * width
            if acc_in is not None:
                total = total + acc_in[:, at : at + width]
            if not last:
                outs[-1][:, at : at + width] = total
            else:
                turn = refs[2]
                tp, head_rows, per = turn.shape
                tok_count = tp * per
                ready = (total[:HEAD_SIZE] / total[HEAD_SIZE : HEAD_SIZE + 1]).astype(jnp.bfloat16)
                for piece in range(width // per):
                    head, spot = divmod(at + piece * per, tok_count)
                    turn[spot // per, head * HEAD_SIZE : (head + 1) * HEAD_SIZE, :] = ready[
                        :, piece * per : (piece + 1) * per
                    ]
        waiting = weights
    if last:
        me = lax.axis_index("tp")
        for rel, out in enumerate(outs):
            out[...] = refs[2][me ^ rel]


def attend(queries, tables, chunks, pieces, acc, sp_size, tp_size, last=False, after=()):
    raw_queries = acc is None
    lanes = chunks[0].shape[-1]
    rows = HEAD_SIZE + ONES_ROWS
    halves = sum(c.shape[0] for c in chunks)
    if raw_queries:
        columns = queries.shape[0] * queries.shape[1] // HEAD_SIZE
        tok_count = queries.shape[0]
    else:
        columns = queries.shape[1]
        tok_count = chunks[0].shape[0] * HALF_KEYS * 2
    scratch = [
        pltpu.VMEM((halves, HALF_KEYS, lanes), jnp.bfloat16),
        pltpu.VMEM((halves, lanes // HEAD_SIZE, rows, HALF_KEYS), jnp.bfloat16),
    ]
    if last:
        head_rows = columns // tok_count * HEAD_SIZE
        block = (head_rows, tok_count // tp_size)
        shape = [jax.ShapeDtypeStruct(block, jnp.bfloat16)] * tp_size
        scratch.append(pltpu.VMEM((tp_size, *block), jnp.bfloat16))
    else:
        shape = [jax.ShapeDtypeStruct((rows, columns), jnp.float32)]
        if raw_queries:
            shape = [jax.ShapeDtypeStruct((lanes, columns), jnp.bfloat16)] + shape
    operands = [queries, *tables, *chunks] + ([] if raw_queries else [acc])
    aliases = {} if (raw_queries or last) else {len(operands) - 1: 0}
    key_count = halves * HALF_KEYS
    return pl.pallas_call(
        functools.partial(attend_kernel, sp_size, pieces, last, raw_queries, len(after)),
        out_shape=shape,
        in_specs=[VMEM] * len(operands) + [HBM] * len(after),
        out_specs=[VMEM] * len(shape),
        scratch_shapes=scratch,
        input_output_aliases=aliases,
        cost_estimate=pl.CostEstimate(
            flops=2 * key_count * columns * 512,
            bytes_accessed=key_count * 1024,
            transcendentals=key_count * columns,
        ),
        compiler_params=pltpu.CompilerParams(vmem_limit_bytes=24 * 1024 * 1024),
    )(*operands, *after)


def direct_exchange(pieces, tp_size):
    held = {0: pieces[0]}
    for rel in reversed(range(1, tp_size)):
        held[rel] = lax.ppermute(pieces[rel], "tp", [(i, i ^ rel) for i in range(tp_size)])
    return [held[rel] for rel in range(tp_size)]


def out_kernel(tp_size, top_count, *refs):
    blocks = refs[:tp_size]
    w_ref, res_ref, mix_ref, norm_ref, table_ref = refs[tp_size : tp_size + 5]
    stream_ref, out_ref, normed_ref, mixed_ref = refs[tp_size + 5 :]
    me = lax.axis_index("tp")
    head_rows, row_count = blocks[0].shape
    width = w_ref.shape[1]
    step = min(512, width)
    turned = [b[...].astype(jnp.float32).T.astype(jnp.bfloat16) for b in blocks]
    power = jnp.zeros((row_count, 1), jnp.float32)
    for at in range(0, width, step):
        mixed = jnp.zeros((row_count, step), jnp.float32)
        for rel in range(tp_size):
            begin = pl.multiple_of((me ^ rel) * head_rows, head_rows)
            mixed = mixed + jnp.dot(
                turned[rel],
                w_ref[pl.ds(begin, head_rows), at : at + step],
                preferred_element_type=jnp.float32,
            )
        mixed_ref[:, at : at + step] = mixed
        power = power + jnp.sum(mixed * mixed, axis=1, keepdims=True)
    scale = lax.rsqrt(power / width + epsilon)
    power = jnp.zeros((row_count, 1), jnp.float32)
    for at in range(0, width, step):
        cols = slice(at, at + step)
        stream = (
            res_ref[:, cols].astype(jnp.float32) + mixed_ref[:, cols] * scale * mix_ref[:, cols]
        ).astype(jnp.bfloat16)
        stream_ref[:, cols] = stream
        wide = stream.astype(jnp.float32)
        power = power + jnp.sum(wide * wide, axis=1, keepdims=True)
    scale = lax.rsqrt(power / width + epsilon)
    for at in range(0, width, step):
        cols = slice(at, at + step)
        wide = stream_ref[:, cols].astype(jnp.float32)
        normed_ref[:, cols] = (wide * scale * norm_ref[:, cols]).astype(jnp.bfloat16)
    fill_slots(top_count, normed_ref, table_ref, out_ref)


def routes_kernel(capacity, expert_ref, weight_ref, out_ref):
    row_count, top_count = expert_ref.shape
    lanes = out_ref.shape[1]
    lane = lax.broadcasted_iota(jnp.int32, (row_count, lanes), 1)
    before = lax.broadcasted_iota(jnp.int32, (row_count, row_count), 0) > (
        lax.broadcasted_iota(jnp.int32, (row_count, row_count), 1)
    )
    before = jnp.where(before, 1.0, 0.0).astype(jnp.bfloat16)
    taken = jnp.zeros((1, lanes), jnp.float32)
    table = jnp.zeros((row_count, lanes), jnp.float32)
    for k in range(top_count):
        expert = expert_ref[:, k : k + 1]
        onehot = jnp.where(lane == expert, 1.0, 0.0)
        earlier = taken + jnp.dot(
            before, onehot.astype(jnp.bfloat16), preferred_element_type=jnp.float32
        )
        rank = jnp.sum(onehot * earlier, axis=1, keepdims=True)
        slot = expert.astype(jnp.float32) * capacity + rank
        taken = taken + jnp.sum(onehot, axis=0, keepdims=True)
        table = jnp.where(lane == k, slot, table)
        table = jnp.where(lane == top_count + k, weight_ref[:, k : k + 1], table)
    out_ref[...] = table.T[: out_ref.shape[0], :row_count]


def fill_slots(top_count, rows_ref, table_ref, out_ref):
    row_count, width = rows_ref.shape
    step = min(512, width)
    slot_count = out_ref.shape[0]
    slots = lax.broadcasted_iota(jnp.int32, (slot_count, row_count), 0)
    slots = slots.astype(jnp.float32)
    hit = slots == table_ref[0:1, :]
    for k in range(1, top_count):
        hit = hit | (slots == table_ref[k : k + 1, :])
    placing = jnp.where(hit, 1.0, 0.0).astype(jnp.bfloat16)
    for at in range(0, width, step):
        cols = slice(at, at + step)
        out_ref[:, cols] = jnp.dot(
            placing, rows_ref[:, cols], preferred_element_type=jnp.float32
        ).astype(jnp.bfloat16)


def gather_kernel(top_count, base_ref, slots_ref, table_ref, out_hbm, out_ref, sems):
    row_count, width = base_ref.shape
    step = width // sems.shape[0]
    table = table_ref[...].T
    slots = lax.broadcasted_iota(jnp.int32, (row_count, slots_ref.shape[0]), 1)
    slots = slots.astype(jnp.float32)
    picks = [
        jnp.where(slots == table[:, k : k + 1], 1.0, 0.0).astype(jnp.bfloat16)
        for k in range(top_count)
    ]
    picks = jnp.concatenate(picks, axis=0)
    copies = []
    for i in range(sems.shape[0]):
        cols = pl.ds(i * step, step)
        rows = jnp.dot(picks, slots_ref[:, cols], preferred_element_type=jnp.float32)
        total = None
        for k in range(top_count):
            row = rows[k * row_count : (k + 1) * row_count]
            row = row * table[:, top_count + k : top_count + k + 1]
            total = row if total is None else total + row
        out_ref[:, cols] = (base_ref[:, cols].astype(jnp.float32) + total).astype(out_ref.dtype)
        copies.append(
            pltpu.make_async_copy(out_ref.at[:, cols], out_hbm.at[:, cols], sems.at[i])
        )
        copies[-1].start()
    for copy in copies:
        copy.wait()


def expert_kernel(rows_ref, gate_ref, up_ref, down_ref, out_ref, act_ref):
    hidden = gate_ref.shape[1]
    width = down_ref.shape[1]
    step = min(256, hidden)
    for at in range(0, hidden, step):
        cols = slice(at, at + step)
        gate = jnp.dot(rows_ref[...], gate_ref[:, cols], preferred_element_type=jnp.float32)
        up = jnp.dot(rows_ref[...], up_ref[:, cols], preferred_element_type=jnp.float32)
        act_ref[:, cols] = (gate / (1.0 + jnp.exp(-gate)) * up).astype(jnp.bfloat16)
    step = min(512, width)
    for at in range(0, width, step):
        cols = slice(at, at + step)
        out_ref[:, cols] = jnp.dot(
            act_ref[...], down_ref[:, cols], preferred_element_type=jnp.float32
        ).astype(jnp.bfloat16)


def local(
    sp_size,
    tp_size,
    query_proj,
    projected_keys,
    projected_values,
    residual,
    out_weight,
    mix_gain,
    norm_gain,
    route_expert,
    route_weight,
    expert_gate,
    expert_up,
    expert_down,
):
    tok_count, lanes = projected_keys.shape
    q_heads = query_proj.shape[1] // HEAD_SIZE
    model_width = residual.shape[1]
    halves = tok_count // HALF_KEYS
    tables = rotation_tables(sp_size * tok_count // GRID_W, lanes)
    raw_own = jnp.stack(
        [part.reshape(halves, HALF_KEYS, lanes) for part in (projected_keys, projected_values)],
        axis=1,
    )

    row_count = residual.shape[0]
    top_count = route_expert.shape[1]
    experts = sp_size * tp_size
    capacity = max(2, 2 * top_count * row_count // experts)
    slots_total = experts * capacity
    table = pl.pallas_call(
        functools.partial(routes_kernel, capacity),
        out_shape=jax.ShapeDtypeStruct((8, row_count), jnp.float32),
        in_specs=[VMEM] * 2,
        out_specs=VMEM,
        cost_estimate=pl.CostEstimate(flops=1 << 22, bytes_accessed=1 << 17, transcendentals=0),
        compiler_params=pltpu.CompilerParams(vmem_limit_bytes=8 * 1024 * 1024),
    )(route_expert, route_weight)

    order = list(range(0, sp_size, 2)) + list(range(sp_size - 1, 0, -2))
    ahead = [(order[i], order[(i + 1) % sp_size]) for i in range(sp_size)]
    behind = [(b, a) for a, b in ahead]
    steps = sp_size // 2
    acc = None
    queries = query_proj
    from_left = from_right = raw_own
    held, pieces = [raw_own], [(0, 0)]
    for step in range(steps):
        if step == steps - 1:
            from_left, from_right = from_left[: halves // 2], from_right[halves // 2 :]
        next_left = lax.ppermute(from_left, "sp", ahead)
        next_right = lax.ppermute(from_right, "sp", behind)
        after = (table,) if step == steps - 1 else ()
        out = attend(queries, tables, held, pieces, acc, sp_size, tp_size, after=after)
        if step == 0:
            queries, acc = out
        else:
            (acc,) = out
        from_left, from_right = next_left, next_right
        held = [from_left, from_right]
        pieces = [(-step - 1, 0), (step + 1, halves // 2 if step == steps - 1 else 0)]
    pieces = attend(queries, tables, held, pieces, acc, sp_size, tp_size, last=True)
    blocks = direct_exchange(pieces, tp_size)

    rows_shape = jax.ShapeDtypeStruct((row_count, model_width), jnp.bfloat16)
    slots_shape = jax.ShapeDtypeStruct((slots_total, model_width), jnp.bfloat16)
    stream, outgoing = pl.pallas_call(
        functools.partial(out_kernel, tp_size, top_count),
        out_shape=(rows_shape, slots_shape),
        in_specs=[VMEM] * (tp_size + 5),
        out_specs=(VMEM, VMEM),
        scratch_shapes=[
            pltpu.VMEM((row_count, model_width), jnp.bfloat16),
            pltpu.VMEM((row_count, model_width), jnp.float32),
        ],
        cost_estimate=pl.CostEstimate(
            flops=2 * row_count * model_width * (out_weight.shape[0] + slots_total),
            bytes_accessed=8 << 20,
            transcendentals=0,
        ),
        compiler_params=pltpu.CompilerParams(vmem_limit_bytes=12 * 1024 * 1024),
    )(*blocks, out_weight, residual, mix_gain[None, :], norm_gain[None, :], table)

    def exchange(slots):
        slots = slots.reshape(experts, capacity, model_width)
        slots = lax.all_to_all(slots, ("sp", "tp"), split_axis=0, concat_axis=0, tiled=True)
        return slots.reshape(slots_total, model_width)

    hidden = expert_gate.shape[2]
    done = pl.pallas_call(
        expert_kernel,
        out_shape=slots_shape,
        in_specs=[VMEM] * 4,
        out_specs=VMEM,
        scratch_shapes=[pltpu.VMEM((slots_total, hidden), jnp.bfloat16)],
        cost_estimate=pl.CostEstimate(
            flops=6 * slots_total * model_width * hidden,
            bytes_accessed=16 << 20,
            transcendentals=slots_total * hidden,
        ),
        compiler_params=pltpu.CompilerParams(vmem_limit_bytes=24 * 1024 * 1024),
    )(exchange(outgoing), expert_gate[0], expert_up[0], expert_down[0])
    return pl.pallas_call(
        functools.partial(gather_kernel, top_count),
        out_shape=rows_shape,
        in_specs=[VMEM] * 3,
        out_specs=HBM,
        scratch_shapes=[
            pltpu.VMEM((row_count, model_width), jnp.bfloat16),
            pltpu.SemaphoreType.DMA((4,)),
        ],
        cost_estimate=pl.CostEstimate(
            flops=4 * row_count * slots_total * model_width,
            bytes_accessed=3 << 20,
            transcendentals=0,
        ),
        compiler_params=pltpu.CompilerParams(vmem_limit_bytes=12 * 1024 * 1024),
    )(stream, exchange(done), table)


def solution(mesh):
    return jax.shard_map(
        functools.partial(local, mesh.shape["sp"], mesh.shape["tp"]),
        mesh=mesh,
        in_specs=(
            P("sp", "tp"),
            P("sp", "tp"),
            P("sp", "tp"),
            P(("sp", "tp"), None),
            P(),
            P(),
            P(),
            P(("sp", "tp"), None),
            P(("sp", "tp"), None),
            P(("sp", "tp"), None, None),
            P(("sp", "tp"), None, None),
            P(("sp", "tp"), None, None),
        ),
        out_specs=P(("sp", "tp"), None),
        check_vma=False,
    )
```

```python
import functools
import math

import jax
import jax.numpy as jnp
from jax import lax
from jax.experimental import pallas as pl
from jax.experimental.pallas import tpu as pltpu
from jax.sharding import PartitionSpec as P

HEAD_SIZE = 64
GRID_W = 64
HALF_KEYS = 256
ONES_ROWS = 16

epsilon = 1e-06
base_theta = 10000.0

VMEM = pl.BlockSpec(memory_space=pltpu.VMEM)
HBM = pl.BlockSpec(memory_space=pltpu.HBM)


def rotation_tables(row_count, lanes):
    quarter = HEAD_SIZE // 4
    lane = jnp.arange(lanes, dtype=jnp.int32) % HEAD_SIZE
    index = jnp.arange(row_count + GRID_W, dtype=jnp.int32)
    place = jnp.where(index < row_count, index, index - row_count)
    frequency = base_theta ** (-(lane % quarter).astype(jnp.float32) / quarter)
    angle = place.astype(jnp.float32)[:, None] * frequency[None, :]
    sign = jnp.where((lane // quarter) % 2 == 0, -1.0, 1.0).astype(jnp.float32)
    return jnp.cos(angle), jnp.sin(angle) * sign[None, :]


class Rotation:
    def __init__(self, cos_ref, sin_ref, lanes):
        rows = lax.broadcasted_iota(jnp.int32, (lanes, lanes), 0)
        cols = lax.broadcasted_iota(jnp.int32, (lanes, lanes), 1)
        same_head = (rows // HEAD_SIZE) == (cols // HEAD_SIZE)
        self.mean_mat = jnp.where(same_head, 1.0 / HEAD_SIZE, 0.0).astype(jnp.bfloat16)
        self.swap_mat = jnp.where((rows ^ (HEAD_SIZE // 4)) == cols, 1.0, 0.0).astype(jnp.bfloat16)
        lane = lax.broadcasted_iota(jnp.int32, (GRID_W, lanes), 1)
        self.by_row = (lane % HEAD_SIZE) < HEAD_SIZE // 2
        self.refs = (cos_ref, sin_ref)

    def table(self, ref, first_row, count):
        total = ref.shape[0] - GRID_W
        cols = ref[total:, :]
        parts = [
            jnp.where(self.by_row, ref[pl.ds(first_row + i, 1), :], cols) for i in range(count)
        ]
        return jnp.concatenate(parts, axis=0)

    def ready(self, raw, first_row, factor):
        count = raw.shape[0] // GRID_W
        cos = self.table(self.refs[0], first_row, count)
        sin = self.table(self.refs[1], first_row, count)
        wide = raw.astype(jnp.float32)
        square = wide * wide
        high = square.astype(jnp.bfloat16)
        low = (square - high.astype(jnp.float32)).astype(jnp.bfloat16)
        mean = jnp.dot(high, self.mean_mat, preferred_element_type=jnp.float32) + jnp.dot(
            low, self.mean_mat, preferred_element_type=jnp.float32
        )
        swapped = jnp.dot(raw, self.swap_mat, preferred_element_type=jnp.float32)
        length = lax.rsqrt(mean + epsilon) * factor
        return (wide * cos + swapped * sin) * length


def ring_place(index, count):
    return jnp.where(index % 2 == 0, index // 2, count - (index + 1) // 2)


def ring_member(place, count):
    place = lax.rem(place + count, count)
    return jnp.where(2 * place < count, 2 * place, 2 * (count - place) - 1)


def attend_kernel(sp_size, pieces, last, raw_queries, after, *refs):
    refs = list(refs)
    first_ref = refs.pop(0)
    cos_ref, sin_ref = refs.pop(0), refs.pop(0)
    chunks = [(refs.pop(0), refs.pop(0)) for _ in pieces]
    acc_in = None if raw_queries else refs.pop(0)
    for _ in range(after):
        refs.pop(0)
    outs = [refs.pop(0) for _ in range(2 if raw_queries else 1)] if not last else None
    if last:
        outs, refs = refs[:-3], refs[-3:]
    keys_ref, values_ref = refs[0], refs[1]
    lanes = chunks[0][0].shape[-1]
    rotation = Rotation(cos_ref, sin_ref, lanes)
    me = lax.axis_index("sp")
    place = ring_place(me, sp_size)
    grid_rows = (cos_ref.shape[0] - GRID_W) // sp_size
    if raw_queries:
        q_ref = outs[0]
        factor = math.log2(math.e) * HEAD_SIZE ** (-0.5)
        tok_count, q_lanes = first_ref.shape
        group = q_lanes // lanes
        q_ref[...] = jnp.zeros_like(q_ref)
        for block in range(group):
            raw = first_ref[:, block * lanes : (block + 1) * lanes]
            turned = rotation.ready(raw, me * grid_rows, factor).T
            for inner in range(lanes // HEAD_SIZE):
                head = block * (lanes // HEAD_SIZE) + inner
                kv_head = head // group
                q_ref[
                    kv_head * HEAD_SIZE : (kv_head + 1) * HEAD_SIZE,
                    head * tok_count : (head + 1) * tok_count,
                ] = turned[inner * HEAD_SIZE : (inner + 1) * HEAD_SIZE].astype(jnp.bfloat16)
    else:
        q_ref = first_ref
    _, columns = q_ref.shape
    width = min(512, columns)
    blocks = columns // width
    kv_heads = lanes // HEAD_SIZE
    ones = jnp.ones((ONES_ROWS, HALF_KEYS), jnp.bfloat16)
    rows = HEAD_SIZE + ONES_ROWS
    halves = 0
    for (k_ref, v_ref), (distance, first_half) in zip(chunks, pieces):
        source = ring_member(place + distance, sp_size)
        for half in range(k_ref.shape[0] // HALF_KEYS):
            span = slice(half * HALF_KEYS, (half + 1) * HALF_KEYS)
            row = source * grid_rows + (first_half + half) * (HALF_KEYS // GRID_W)
            keys_ref[halves] = rotation.ready(k_ref[span, :], row, 1.0).astype(jnp.bfloat16)
            turned = v_ref[span, :].astype(jnp.float32).T.astype(jnp.bfloat16)
            for head in range(kv_heads):
                values_ref[halves, head, :HEAD_SIZE, :] = turned[
                    head * HEAD_SIZE : (head + 1) * HEAD_SIZE
                ]
                values_ref[halves, head, HEAD_SIZE:, :] = ones
            halves += 1
    waiting = None
    for block in range(blocks + 1):
        weights = []
        total = None
        for half in range(halves):
            if block < blocks:
                scores = jnp.dot(
                    keys_ref[half],
                    q_ref[:, block * width : (block + 1) * width],
                    preferred_element_type=jnp.float32,
                )
                weights.append(jnp.exp2(scores).astype(jnp.bfloat16))
            if waiting is not None:
                kv_head = (block - 1) * kv_heads // blocks
                piece = jnp.dot(
                    values_ref[half, kv_head], waiting[half], preferred_element_type=jnp.float32
                )
                total = piece if total is None else total + piece
        if waiting is not None:
            at = (block - 1) * width
            if acc_in is not None:
                total = total + acc_in[:, at : at + width]
            if not last:
                outs[-1][:, at : at + width] = total
            else:
                turn = refs[2]
                tp, head_rows, per = turn.shape
                tok_count = tp * per
                ready = (total[:HEAD_SIZE] / total[HEAD_SIZE : HEAD_SIZE + 1]).astype(jnp.bfloat16)
                for piece in range(width // per):
                    head, spot = divmod(at + piece * per, tok_count)
                    turn[spot // per, head * HEAD_SIZE : (head + 1) * HEAD_SIZE, :] = ready[
                        :, piece * per : (piece + 1) * per
                    ]
        waiting = weights
    if last:
        me = lax.axis_index("tp")
        for rel, out in enumerate(outs):
            out[...] = refs[2][me ^ rel]


def attend(queries, tables, chunks, pieces, acc, sp_size, tp_size, last=False, after=()):
    raw_queries = acc is None
    lanes = chunks[0][0].shape[-1]
    rows = HEAD_SIZE + ONES_ROWS
    halves = sum(k.shape[0] for k, _ in chunks) // HALF_KEYS
    if raw_queries:
        columns = queries.shape[0] * queries.shape[1] // HEAD_SIZE
        tok_count = queries.shape[0]
    else:
        columns = queries.shape[1]
        tok_count = chunks[0][0].shape[0] * 2
    scratch = [
        pltpu.VMEM((halves, HALF_KEYS, lanes), jnp.bfloat16),
        pltpu.VMEM((halves, lanes // HEAD_SIZE, rows, HALF_KEYS), jnp.bfloat16),
    ]
    if last:
        head_rows = columns // tok_count * HEAD_SIZE
        block = (head_rows, tok_count // tp_size)
        shape = [jax.ShapeDtypeStruct(block, jnp.bfloat16)] * tp_size
        scratch.append(pltpu.VMEM((tp_size, *block), jnp.bfloat16))
    else:
        shape = [jax.ShapeDtypeStruct((rows, columns), jnp.float32)]
        if raw_queries:
            shape = [jax.ShapeDtypeStruct((lanes, columns), jnp.bfloat16)] + shape
    operands = [queries, *tables, *(part for chunk in chunks for part in chunk)]
    operands += [] if raw_queries else [acc]
    aliases = {} if (raw_queries or last) else {len(operands) - 1: 0}
    key_count = halves * HALF_KEYS
    return pl.pallas_call(
        functools.partial(attend_kernel, sp_size, pieces, last, raw_queries, len(after)),
        out_shape=shape,
        in_specs=[VMEM] * len(operands) + [HBM] * len(after),
        out_specs=[VMEM] * len(shape),
        scratch_shapes=scratch,
        input_output_aliases=aliases,
        cost_estimate=pl.CostEstimate(
            flops=2 * key_count * columns * 512,
            bytes_accessed=key_count * 1024,
            transcendentals=key_count * columns,
        ),
        compiler_params=pltpu.CompilerParams(vmem_limit_bytes=24 * 1024 * 1024),
    )(*operands, *after)


def direct_exchange(pieces, tp_size):
    held = {0: pieces[0]}
    for rel in reversed(range(1, tp_size)):
        held[rel] = lax.ppermute(pieces[rel], "tp", [(i, i ^ rel) for i in range(tp_size)])
    return [held[rel] for rel in range(tp_size)]


def out_kernel(tp_size, top_count, *refs):
    blocks = refs[:tp_size]
    w_ref, res_ref, mix_ref, norm_ref, table_ref = refs[tp_size : tp_size + 5]
    stream_ref, out_ref, normed_ref, mixed_ref = refs[tp_size + 5 :]
    me = lax.axis_index("tp")
    head_rows, row_count = blocks[0].shape
    width = w_ref.shape[1]
    step = min(512, width)
    turned = [b[...].astype(jnp.float32).T.astype(jnp.bfloat16) for b in blocks]
    power = jnp.zeros((row_count, 1), jnp.float32)
    for at in range(0, width, step):
        mixed = jnp.zeros((row_count, step), jnp.float32)
        for rel in range(tp_size):
            begin = pl.multiple_of((me ^ rel) * head_rows, head_rows)
            mixed = mixed + jnp.dot(
                turned[rel],
                w_ref[pl.ds(begin, head_rows), at : at + step],
                preferred_element_type=jnp.float32,
            )
        mixed_ref[:, at : at + step] = mixed
        power = power + jnp.sum(mixed * mixed, axis=1, keepdims=True)
    scale = lax.rsqrt(power / width + epsilon)
    power = jnp.zeros((row_count, 1), jnp.float32)
    for at in range(0, width, step):
        cols = slice(at, at + step)
        stream = (
            res_ref[:, cols].astype(jnp.float32) + mixed_ref[:, cols] * scale * mix_ref[:, cols]
        ).astype(jnp.bfloat16)
        stream_ref[:, cols] = stream
        wide = stream.astype(jnp.float32)
        power = power + jnp.sum(wide * wide, axis=1, keepdims=True)
    scale = lax.rsqrt(power / width + epsilon)
    for at in range(0, width, step):
        cols = slice(at, at + step)
        wide = stream_ref[:, cols].astype(jnp.float32)
        normed_ref[:, cols] = (wide * scale * norm_ref[:, cols]).astype(jnp.bfloat16)
    fill_slots(top_count, normed_ref, table_ref, out_ref)


def routes_kernel(capacity, expert_ref, weight_ref, out_ref):
    row_count, top_count = expert_ref.shape
    lanes = out_ref.shape[1]
    lane = lax.broadcasted_iota(jnp.int32, (row_count, lanes), 1)
    before = lax.broadcasted_iota(jnp.int32, (row_count, row_count), 0) > (
        lax.broadcasted_iota(jnp.int32, (row_count, row_count), 1)
    )
    before = jnp.where(before, 1.0, 0.0).astype(jnp.bfloat16)
    taken = jnp.zeros((1, lanes), jnp.float32)
    table = jnp.zeros((row_count, lanes), jnp.float32)
    for k in range(top_count):
        expert = expert_ref[:, k : k + 1]
        onehot = jnp.where(lane == expert, 1.0, 0.0)
        earlier = taken + jnp.dot(
            before, onehot.astype(jnp.bfloat16), preferred_element_type=jnp.float32
        )
        rank = jnp.sum(onehot * earlier, axis=1, keepdims=True)
        slot = expert.astype(jnp.float32) * capacity + rank
        taken = taken + jnp.sum(onehot, axis=0, keepdims=True)
        table = jnp.where(lane == k, slot, table)
        table = jnp.where(lane == top_count + k, weight_ref[:, k : k + 1], table)
    out_ref[...] = table.T[: out_ref.shape[0], :row_count]


def fill_slots(top_count, rows_ref, table_ref, out_ref):
    row_count, width = rows_ref.shape
    step = min(512, width)
    slot_count = out_ref.shape[0]
    slots = lax.broadcasted_iota(jnp.int32, (slot_count, row_count), 0)
    slots = slots.astype(jnp.float32)
    hit = slots == table_ref[0:1, :]
    for k in range(1, top_count):
        hit = hit | (slots == table_ref[k : k + 1, :])
    placing = jnp.where(hit, 1.0, 0.0).astype(jnp.bfloat16)
    for at in range(0, width, step):
        cols = slice(at, at + step)
        out_ref[:, cols] = jnp.dot(
            placing, rows_ref[:, cols], preferred_element_type=jnp.float32
        ).astype(jnp.bfloat16)


def gather_kernel(top_count, base_ref, slots_ref, table_ref, out_hbm, out_ref, sems):
    row_count, width = base_ref.shape
    step = width // sems.shape[0]
    table = table_ref[...].T
    slots = lax.broadcasted_iota(jnp.int32, (row_count, slots_ref.shape[0]), 1)
    slots = slots.astype(jnp.float32)
    picks = [
        jnp.where(slots == table[:, k : k + 1], 1.0, 0.0).astype(jnp.bfloat16)
        for k in range(top_count)
    ]
    picks = jnp.concatenate(picks, axis=0)
    copies = []
    for i in range(sems.shape[0]):
        cols = pl.ds(i * step, step)
        rows = jnp.dot(picks, slots_ref[:, cols], preferred_element_type=jnp.float32)
        total = None
        for k in range(top_count):
            row = rows[k * row_count : (k + 1) * row_count]
            row = row * table[:, top_count + k : top_count + k + 1]
            total = row if total is None else total + row
        out_ref[:, cols] = (base_ref[:, cols].astype(jnp.float32) + total).astype(out_ref.dtype)
        copies.append(
            pltpu.make_async_copy(out_ref.at[:, cols], out_hbm.at[:, cols], sems.at[i])
        )
        copies[-1].start()
    for copy in copies:
        copy.wait()


def expert_kernel(rows_ref, gate_ref, up_ref, down_ref, out_ref, act_ref):
    hidden = gate_ref.shape[1]
    width = down_ref.shape[1]
    step = min(256, hidden)
    for at in range(0, hidden, step):
        cols = slice(at, at + step)
        gate = jnp.dot(rows_ref[...], gate_ref[:, cols], preferred_element_type=jnp.float32)
        up = jnp.dot(rows_ref[...], up_ref[:, cols], preferred_element_type=jnp.float32)
        act_ref[:, cols] = (gate / (1.0 + jnp.exp(-gate)) * up).astype(jnp.bfloat16)
    step = min(512, width)
    for at in range(0, width, step):
        cols = slice(at, at + step)
        out_ref[:, cols] = jnp.dot(
            act_ref[...], down_ref[:, cols], preferred_element_type=jnp.float32
        ).astype(jnp.bfloat16)


def local(
    sp_size,
    tp_size,
    query_proj,
    projected_keys,
    projected_values,
    residual,
    out_weight,
    mix_gain,
    norm_gain,
    route_expert,
    route_weight,
    expert_gate,
    expert_up,
    expert_down,
):
    tok_count, lanes = projected_keys.shape
    q_heads = query_proj.shape[1] // HEAD_SIZE
    model_width = residual.shape[1]
    halves = tok_count // HALF_KEYS
    tables = rotation_tables(sp_size * tok_count // GRID_W, lanes)
    raw_own = (projected_keys, projected_values)
    row_count = residual.shape[0]
    top_count = route_expert.shape[1]
    experts = sp_size * tp_size
    capacity = max(2, 2 * top_count * row_count // experts)
    slots_total = experts * capacity
    table = pl.pallas_call(
        functools.partial(routes_kernel, capacity),
        out_shape=jax.ShapeDtypeStruct((8, row_count), jnp.float32),
        in_specs=[VMEM] * 2,
        out_specs=VMEM,
        cost_estimate=pl.CostEstimate(flops=1 << 22, bytes_accessed=1 << 17, transcendentals=0),
        compiler_params=pltpu.CompilerParams(vmem_limit_bytes=8 * 1024 * 1024),
    )(route_expert, route_weight)

    order = list(range(0, sp_size, 2)) + list(range(sp_size - 1, 0, -2))
    ahead = [(order[i], order[(i + 1) % sp_size]) for i in range(sp_size)]
    behind = [(b, a) for a, b in ahead]
    steps = sp_size // 2
    acc = None
    queries = query_proj
    from_left = from_right = raw_own
    held, pieces = [raw_own], [(0, 0)]
    for step in range(steps):
        if step == steps - 1:
            from_left = [part[: tok_count // 2] for part in from_left]
            from_right = [part[tok_count // 2 :] for part in from_right]
        next_left, next_right = [], []
        for left, right in zip(from_left, from_right):
            next_left.append(lax.ppermute(left, "sp", ahead))
            next_right.append(lax.ppermute(right, "sp", behind))
        after = (table,) if step == steps - 1 else ()
        out = attend(queries, tables, held, pieces, acc, sp_size, tp_size, after=after)
        if step == 0:
            queries, acc = out
        else:
            (acc,) = out
        from_left, from_right = next_left, next_right
        held = [from_left, from_right]
        pieces = [(-step - 1, 0), (step + 1, halves // 2 if step == steps - 1 else 0)]
    pieces = attend(queries, tables, held, pieces, acc, sp_size, tp_size, last=True)
    blocks = direct_exchange(pieces, tp_size)

    rows_shape = jax.ShapeDtypeStruct((row_count, model_width), jnp.bfloat16)
    slots_shape = jax.ShapeDtypeStruct((slots_total, model_width), jnp.bfloat16)
    stream, outgoing = pl.pallas_call(
        functools.partial(out_kernel, tp_size, top_count),
        out_shape=(rows_shape, slots_shape),
        in_specs=[VMEM] * (tp_size + 5),
        out_specs=(VMEM, VMEM),
        scratch_shapes=[
            pltpu.VMEM((row_count, model_width), jnp.bfloat16),
            pltpu.VMEM((row_count, model_width), jnp.float32),
        ],
        cost_estimate=pl.CostEstimate(
            flops=2 * row_count * model_width * (out_weight.shape[0] + slots_total),
            bytes_accessed=8 << 20,
            transcendentals=0,
        ),
        compiler_params=pltpu.CompilerParams(vmem_limit_bytes=12 * 1024 * 1024),
    )(*blocks, out_weight, residual, mix_gain[None, :], norm_gain[None, :], table)

    def exchange(slots):
        slots = slots.reshape(experts, capacity, model_width)
        slots = lax.all_to_all(slots, ("sp", "tp"), split_axis=0, concat_axis=0, tiled=True)
        return slots.reshape(slots_total, model_width)

    hidden = expert_gate.shape[2]
    done = pl.pallas_call(
        expert_kernel,
        out_shape=slots_shape,
        in_specs=[VMEM] * 4,
        out_specs=VMEM,
        scratch_shapes=[pltpu.VMEM((slots_total, hidden), jnp.bfloat16)],
        cost_estimate=pl.CostEstimate(
            flops=6 * slots_total * model_width * hidden,
            bytes_accessed=16 << 20,
            transcendentals=slots_total * hidden,
        ),
        compiler_params=pltpu.CompilerParams(vmem_limit_bytes=24 * 1024 * 1024),
    )(exchange(outgoing), expert_gate[0], expert_up[0], expert_down[0])
    return pl.pallas_call(
        functools.partial(gather_kernel, top_count),
        out_shape=rows_shape,
        in_specs=[VMEM] * 3,
        out_specs=HBM,
        scratch_shapes=[
            pltpu.VMEM((row_count, model_width), jnp.bfloat16),
            pltpu.SemaphoreType.DMA((4,)),
        ],
        cost_estimate=pl.CostEstimate(
            flops=4 * row_count * slots_total * model_width,
            bytes_accessed=3 << 20,
            transcendentals=0,
        ),
        compiler_params=pltpu.CompilerParams(vmem_limit_bytes=12 * 1024 * 1024),
    )(stream, exchange(done), table)


def solution(mesh):
    return jax.shard_map(
        functools.partial(local, mesh.shape["sp"], mesh.shape["tp"]),
        mesh=mesh,
        in_specs=(
            P("sp", "tp"),
            P("sp", "tp"),
            P("sp", "tp"),
            P(("sp", "tp"), None),
            P(),
            P(),
            P(),
            P(("sp", "tp"), None),
            P(("sp", "tp"), None),
            P(("sp", "tp"), None, None),
            P(("sp", "tp"), None, None),
            P(("sp", "tp"), None, None),
        ),
        out_specs=P(("sp", "tp"), None),
        check_vma=False,
    )
```

```python
import functools
import math

import jax
import jax.numpy as jnp
from jax import lax
from jax.experimental import pallas as pl
from jax.experimental.pallas import tpu as pltpu
from jax.sharding import PartitionSpec as P

HEAD_SIZE = 64
GRID_W = 64
HALF_KEYS = 256
ONES_ROWS = 16

epsilon = 1e-06
base_theta = 10000.0

VMEM = pl.BlockSpec(memory_space=pltpu.VMEM)
HBM = pl.BlockSpec(memory_space=pltpu.HBM)


def rotation_tables(row_count, lanes):
    quarter = HEAD_SIZE // 4
    lane = jnp.arange(lanes, dtype=jnp.int32) % HEAD_SIZE
    index = jnp.arange(row_count + GRID_W, dtype=jnp.int32)
    place = jnp.where(index < row_count, index, index - row_count)
    frequency = base_theta ** (-(lane % quarter).astype(jnp.float32) / quarter)
    angle = place.astype(jnp.float32)[:, None] * frequency[None, :]
    sign = jnp.where((lane // quarter) % 2 == 0, -1.0, 1.0).astype(jnp.float32)
    return jnp.cos(angle), jnp.sin(angle) * sign[None, :]


class Rotation:
    def __init__(self, cos_ref, sin_ref, lanes):
        rows = lax.broadcasted_iota(jnp.int32, (lanes, lanes), 0)
        cols = lax.broadcasted_iota(jnp.int32, (lanes, lanes), 1)
        same_head = (rows // HEAD_SIZE) == (cols // HEAD_SIZE)
        self.mean_mat = jnp.where(same_head, 1.0 / HEAD_SIZE, 0.0).astype(jnp.bfloat16)
        self.swap_mat = jnp.where((rows ^ (HEAD_SIZE // 4)) == cols, 1.0, 0.0).astype(jnp.bfloat16)
        lane = lax.broadcasted_iota(jnp.int32, (GRID_W, lanes), 1)
        self.by_row = (lane % HEAD_SIZE) < HEAD_SIZE // 2
        self.refs = (cos_ref, sin_ref)

    def table(self, ref, first_row, count):
        total = ref.shape[0] - GRID_W
        cols = ref[total:, :]
        parts = [
            jnp.where(self.by_row, ref[pl.ds(first_row + i, 1), :], cols) for i in range(count)
        ]
        return jnp.concatenate(parts, axis=0)

    def ready(self, raw, first_row, factor):
        count = raw.shape[0] // GRID_W
        cos = self.table(self.refs[0], first_row, count)
        sin = self.table(self.refs[1], first_row, count)
        wide = raw.astype(jnp.float32)
        square = wide * wide
        high = square.astype(jnp.bfloat16)
        low = (square - high.astype(jnp.float32)).astype(jnp.bfloat16)
        mean = jnp.dot(high, self.mean_mat, preferred_element_type=jnp.float32) + jnp.dot(
            low, self.mean_mat, preferred_element_type=jnp.float32
        )
        swapped = jnp.dot(raw, self.swap_mat, preferred_element_type=jnp.float32)
        length = lax.rsqrt(mean + epsilon) * factor
        return (wide * cos + swapped * sin) * length


def ring_place(index, count):
    return jnp.where(index % 2 == 0, index // 2, count - (index + 1) // 2)


def ring_member(place, count):
    place = lax.rem(place + count, count)
    return jnp.where(2 * place < count, 2 * place, 2 * (count - place) - 1)


def attend_kernel(sp_size, pieces, last, raw_queries, after, *refs):
    refs = list(refs)
    first_ref = refs.pop(0)
    cos_ref, sin_ref = refs.pop(0), refs.pop(0)
    chunks = [refs.pop(0) for _ in pieces]
    acc_in = None if raw_queries else refs.pop(0)
    for _ in range(after):
        refs.pop(0)
    outs = [refs.pop(0) for _ in range(2 if raw_queries else 1)] if not last else None
    if last:
        outs, refs = refs[:-3], refs[-3:]
    keys_ref, values_ref = refs[0], refs[1]
    lanes = chunks[0].shape[-1]
    rotation = Rotation(cos_ref, sin_ref, lanes)
    me = lax.axis_index("sp")
    place = ring_place(me, sp_size)
    grid_rows = (cos_ref.shape[0] - GRID_W) // sp_size
    if raw_queries:
        q_ref = outs[0]
        factor = math.log2(math.e) * HEAD_SIZE ** (-0.5)
        tok_count, q_lanes = first_ref.shape
        group = q_lanes // lanes
        q_ref[...] = jnp.zeros_like(q_ref)
        for block in range(group):
            raw = first_ref[:, block * lanes : (block + 1) * lanes]
            turned = rotation.ready(raw, me * grid_rows, factor).T
            for inner in range(lanes // HEAD_SIZE):
                head = block * (lanes // HEAD_SIZE) + inner
                kv_head = head // group
                q_ref[
                    kv_head * HEAD_SIZE : (kv_head + 1) * HEAD_SIZE,
                    head * tok_count : (head + 1) * tok_count,
                ] = turned[inner * HEAD_SIZE : (inner + 1) * HEAD_SIZE].astype(jnp.bfloat16)
    else:
        q_ref = first_ref
    _, columns = q_ref.shape
    width = min(512, columns)
    blocks = columns // width
    kv_heads = lanes // HEAD_SIZE
    ones = jnp.ones((ONES_ROWS, HALF_KEYS), jnp.bfloat16)
    rows = HEAD_SIZE + ONES_ROWS
    halves = 0
    for chunk, (distance, first_half) in zip(chunks, pieces):
        source = ring_member(place + distance, sp_size)
        for half in range(chunk.shape[0]):
            row = source * grid_rows + (first_half + half) * (HALF_KEYS // GRID_W)
            keys_ref[halves] = rotation.ready(chunk[half, 0], row, 1.0).astype(jnp.bfloat16)
            turned = chunk[half, 1].astype(jnp.float32).T.astype(jnp.bfloat16)
            for head in range(kv_heads):
                values_ref[halves, head, :HEAD_SIZE, :] = turned[
                    head * HEAD_SIZE : (head + 1) * HEAD_SIZE
                ]
                values_ref[halves, head, HEAD_SIZE:, :] = ones
            halves += 1
    waiting = None
    for block in range(blocks + 1):
        weights = []
        total = None
        for half in range(halves):
            if block < blocks:
                scores = jnp.dot(
                    keys_ref[half],
                    q_ref[:, block * width : (block + 1) * width],
                    preferred_element_type=jnp.float32,
                )
                weights.append(jnp.exp2(scores).astype(jnp.bfloat16))
            if waiting is not None:
                kv_head = (block - 1) * kv_heads // blocks
                piece = jnp.dot(
                    values_ref[half, kv_head], waiting[half], preferred_element_type=jnp.float32
                )
                total = piece if total is None else total + piece
        if waiting is not None:
            at = (block - 1) * width
            if acc_in is not None:
                total = total + acc_in[:, at : at + width]
            if not last:
                outs[-1][:, at : at + width] = total
            else:
                turn = refs[2]
                tp, head_rows, per = turn.shape
                tok_count = tp * per
                ready = (total[:HEAD_SIZE] / total[HEAD_SIZE : HEAD_SIZE + 1]).astype(jnp.bfloat16)
                for piece in range(width // per):
                    head, spot = divmod(at + piece * per, tok_count)
                    turn[spot // per, head * HEAD_SIZE : (head + 1) * HEAD_SIZE, :] = ready[
                        :, piece * per : (piece + 1) * per
                    ]
        waiting = weights
    if last:
        me = lax.axis_index("tp")
        for rel, out in enumerate(outs):
            out[...] = refs[2][me ^ rel]


def attend(queries, tables, chunks, pieces, acc, sp_size, tp_size, last=False, after=()):
    raw_queries = acc is None
    lanes = chunks[0].shape[-1]
    rows = HEAD_SIZE + ONES_ROWS
    halves = sum(c.shape[0] for c in chunks)
    if raw_queries:
        columns = queries.shape[0] * queries.shape[1] // HEAD_SIZE
        tok_count = queries.shape[0]
    else:
        columns = queries.shape[1]
        tok_count = chunks[0].shape[0] * HALF_KEYS * 2
    scratch = [
        pltpu.VMEM((halves, HALF_KEYS, lanes), jnp.bfloat16),
        pltpu.VMEM((halves, lanes // HEAD_SIZE, rows, HALF_KEYS), jnp.bfloat16),
    ]
    if last:
        head_rows = columns // tok_count * HEAD_SIZE
        block = (head_rows, tok_count // tp_size)
        shape = [jax.ShapeDtypeStruct(block, jnp.bfloat16)] * tp_size
        scratch.append(pltpu.VMEM((tp_size, *block), jnp.bfloat16))
    else:
        shape = [jax.ShapeDtypeStruct((rows, columns), jnp.float32)]
        if raw_queries:
            shape = [jax.ShapeDtypeStruct((lanes, columns), jnp.bfloat16)] + shape
    operands = [queries, *tables, *chunks] + ([] if raw_queries else [acc])
    aliases = {} if (raw_queries or last) else {len(operands) - 1: 0}
    key_count = halves * HALF_KEYS
    return pl.pallas_call(
        functools.partial(attend_kernel, sp_size, pieces, last, raw_queries, len(after)),
        out_shape=shape,
        in_specs=[VMEM] * len(operands) + [HBM] * len(after),
        out_specs=[VMEM] * len(shape),
        scratch_shapes=scratch,
        input_output_aliases=aliases,
        cost_estimate=pl.CostEstimate(
            flops=2 * key_count * columns * 512,
            bytes_accessed=key_count * 1024,
            transcendentals=key_count * columns,
        ),
        compiler_params=pltpu.CompilerParams(vmem_limit_bytes=24 * 1024 * 1024),
    )(*operands, *after)


def direct_exchange(pieces, tp_size):
    held = {0: pieces[0]}
    for rel in reversed(range(1, tp_size)):
        held[rel] = lax.ppermute(pieces[rel], "tp", [(i, i ^ rel) for i in range(tp_size)])
    return [held[rel] for rel in range(tp_size)]


def out_kernel(tp_size, top_count, *refs):
    blocks = refs[:tp_size]
    w_ref, res_ref, mix_ref, norm_ref, table_ref = refs[tp_size : tp_size + 5]
    stream_ref, out_ref, normed_ref, mixed_ref = refs[tp_size + 5 :]
    me = lax.axis_index("tp")
    head_rows, row_count = blocks[0].shape
    width = w_ref.shape[1]
    step = min(512, width)
    turned = [b[...].astype(jnp.float32).T.astype(jnp.bfloat16) for b in blocks]
    power = jnp.zeros((row_count, 1), jnp.float32)
    for at in range(0, width, step):
        mixed = jnp.zeros((row_count, step), jnp.float32)
        for rel in range(tp_size):
            begin = pl.multiple_of((me ^ rel) * head_rows, head_rows)
            mixed = mixed + jnp.dot(
                turned[rel],
                w_ref[pl.ds(begin, head_rows), at : at + step],
                preferred_element_type=jnp.float32,
            )
        mixed_ref[:, at : at + step] = mixed
        power = power + jnp.sum(mixed * mixed, axis=1, keepdims=True)
    scale = lax.rsqrt(power / width + epsilon)
    power = jnp.zeros((row_count, 1), jnp.float32)
    for at in range(0, width, step):
        cols = slice(at, at + step)
        stream = (
            res_ref[:, cols].astype(jnp.float32) + mixed_ref[:, cols] * scale * mix_ref[:, cols]
        ).astype(jnp.bfloat16)
        stream_ref[:, cols] = stream
        wide = stream.astype(jnp.float32)
        power = power + jnp.sum(wide * wide, axis=1, keepdims=True)
    scale = lax.rsqrt(power / width + epsilon)
    for at in range(0, width, step):
        cols = slice(at, at + step)
        wide = stream_ref[:, cols].astype(jnp.float32)
        normed_ref[:, cols] = (wide * scale * norm_ref[:, cols]).astype(jnp.bfloat16)
    fill_slots(top_count, normed_ref, table_ref, out_ref)


def routes_kernel(capacity, expert_ref, weight_ref, out_ref):
    row_count, top_count = expert_ref.shape
    lanes = out_ref.shape[1]
    lane = lax.broadcasted_iota(jnp.int32, (row_count, lanes), 1)
    before = lax.broadcasted_iota(jnp.int32, (row_count, row_count), 0) > (
        lax.broadcasted_iota(jnp.int32, (row_count, row_count), 1)
    )
    before = jnp.where(before, 1.0, 0.0).astype(jnp.bfloat16)
    taken = jnp.zeros((1, lanes), jnp.float32)
    table = jnp.zeros((row_count, lanes), jnp.float32)
    for k in range(top_count):
        expert = expert_ref[:, k : k + 1]
        onehot = jnp.where(lane == expert, 1.0, 0.0)
        earlier = taken + jnp.dot(
            before, onehot.astype(jnp.bfloat16), preferred_element_type=jnp.float32
        )
        rank = jnp.sum(onehot * earlier, axis=1, keepdims=True)
        slot = expert.astype(jnp.float32) * capacity + rank
        taken = taken + jnp.sum(onehot, axis=0, keepdims=True)
        table = jnp.where(lane == k, slot, table)
        table = jnp.where(lane == top_count + k, weight_ref[:, k : k + 1], table)
    out_ref[...] = table.T[: out_ref.shape[0], :row_count]


def fill_slots(top_count, rows_ref, table_ref, out_ref):
    row_count, width = rows_ref.shape
    step = min(512, width)
    slot_count = out_ref.shape[0]
    slots = lax.broadcasted_iota(jnp.int32, (slot_count, row_count), 0)
    slots = slots.astype(jnp.float32)
    hit = slots == table_ref[0:1, :]
    for k in range(1, top_count):
        hit = hit | (slots == table_ref[k : k + 1, :])
    placing = jnp.where(hit, 1.0, 0.0).astype(jnp.bfloat16)
    for at in range(0, width, step):
        cols = slice(at, at + step)
        out_ref[:, cols] = jnp.dot(
            placing, rows_ref[:, cols], preferred_element_type=jnp.float32
        ).astype(jnp.bfloat16)


def gather_kernel(top_count, base_ref, slots_ref, table_ref, out_hbm, out_ref, sems):
    row_count, width = base_ref.shape
    step = width // sems.shape[0]
    table = table_ref[...].T
    slots = lax.broadcasted_iota(jnp.int32, (row_count, slots_ref.shape[0]), 1)
    slots = slots.astype(jnp.float32)
    picks = [
        jnp.where(slots == table[:, k : k + 1], 1.0, 0.0).astype(jnp.bfloat16)
        for k in range(top_count)
    ]
    picks = jnp.concatenate(picks, axis=0)
    copies = []
    for i in range(sems.shape[0]):
        cols = pl.ds(i * step, step)
        rows = jnp.dot(picks, slots_ref[:, cols], preferred_element_type=jnp.float32)
        total = None
        for k in range(top_count):
            row = rows[k * row_count : (k + 1) * row_count]
            row = row * table[:, top_count + k : top_count + k + 1]
            total = row if total is None else total + row
        out_ref[:, cols] = (base_ref[:, cols].astype(jnp.float32) + total).astype(out_ref.dtype)
        copies.append(
            pltpu.make_async_copy(out_ref.at[:, cols], out_hbm.at[:, cols], sems.at[i])
        )
        copies[-1].start()
    for copy in copies:
        copy.wait()


def expert_kernel(rows_ref, gate_ref, up_ref, down_ref, out_ref, act_ref):
    hidden = gate_ref.shape[1]
    width = down_ref.shape[1]
    step = min(256, hidden)
    for at in range(0, hidden, step):
        cols = slice(at, at + step)
        gate = jnp.dot(rows_ref[...], gate_ref[:, cols], preferred_element_type=jnp.float32)
        up = jnp.dot(rows_ref[...], up_ref[:, cols], preferred_element_type=jnp.float32)
        act_ref[:, cols] = (gate / (1.0 + jnp.exp(-gate)) * up).astype(jnp.bfloat16)
    step = min(512, width)
    for at in range(0, width, step):
        cols = slice(at, at + step)
        out_ref[:, cols] = jnp.dot(
            act_ref[...], down_ref[:, cols], preferred_element_type=jnp.float32
        ).astype(jnp.bfloat16)


def local(
    sp_size,
    tp_size,
    query_proj,
    projected_keys,
    projected_values,
    residual,
    out_weight,
    mix_gain,
    norm_gain,
    route_expert,
    route_weight,
    expert_gate,
    expert_up,
    expert_down,
):
    tok_count, lanes = projected_keys.shape
    q_heads = query_proj.shape[1] // HEAD_SIZE
    model_width = residual.shape[1]
    halves = tok_count // HALF_KEYS
    tables = rotation_tables(sp_size * tok_count // GRID_W, lanes)
    raw_own = jnp.stack(
        [part.reshape(halves, HALF_KEYS, lanes) for part in (projected_keys, projected_values)],
        axis=1,
    )

    row_count = residual.shape[0]
    top_count = route_expert.shape[1]
    experts = sp_size * tp_size
    capacity = max(2, 2 * top_count * row_count // experts)
    slots_total = experts * capacity
    table = pl.pallas_call(
        functools.partial(routes_kernel, capacity),
        out_shape=jax.ShapeDtypeStruct((8, row_count), jnp.float32),
        in_specs=[VMEM] * 2,
        out_specs=VMEM,
        cost_estimate=pl.CostEstimate(flops=1 << 22, bytes_accessed=1 << 17, transcendentals=0),
        compiler_params=pltpu.CompilerParams(vmem_limit_bytes=8 * 1024 * 1024),
    )(route_expert, route_weight)

    order = list(range(0, sp_size, 2)) + list(range(sp_size - 1, 0, -2))
    ahead = [(order[i], order[(i + 1) % sp_size]) for i in range(sp_size)]
    behind = [(b, a) for a, b in ahead]
    steps = sp_size // 2
    acc = None
    queries = query_proj
    from_left = from_right = raw_own
    held, pieces = [raw_own], [(0, 0)]
    for step in range(steps):
        if step == steps - 1:
            from_left, from_right = from_left[: halves // 2], from_right[halves // 2 :]
        next_left = lax.ppermute(from_left, "sp", ahead)
        next_right = lax.ppermute(from_right, "sp", behind)
        after = (table,) if step == steps - 1 else ()
        out = attend(queries, tables, held, pieces, acc, sp_size, tp_size, after=after)
        if step == 0:
            queries, acc = out
        else:
            (acc,) = out
        from_left, from_right = next_left, next_right
        held = [from_left, from_right]
        pieces = [(-step - 1, 0), (step + 1, halves // 2 if step == steps - 1 else 0)]
    (acc,) = attend(queries, tables, held[1:], pieces[1:], acc, sp_size, tp_size)
    pieces = attend(queries, tables, held[:1], pieces[:1], acc, sp_size, tp_size, last=True)
    blocks = direct_exchange(pieces, tp_size)

    rows_shape = jax.ShapeDtypeStruct((row_count, model_width), jnp.bfloat16)
    slots_shape = jax.ShapeDtypeStruct((slots_total, model_width), jnp.bfloat16)
    stream, outgoing = pl.pallas_call(
        functools.partial(out_kernel, tp_size, top_count),
        out_shape=(rows_shape, slots_shape),
        in_specs=[VMEM] * (tp_size + 5),
        out_specs=(VMEM, VMEM),
        scratch_shapes=[
            pltpu.VMEM((row_count, model_width), jnp.bfloat16),
            pltpu.VMEM((row_count, model_width), jnp.float32),
        ],
        cost_estimate=pl.CostEstimate(
            flops=2 * row_count * model_width * (out_weight.shape[0] + slots_total),
            bytes_accessed=8 << 20,
            transcendentals=0,
        ),
        compiler_params=pltpu.CompilerParams(vmem_limit_bytes=12 * 1024 * 1024),
    )(*blocks, out_weight, residual, mix_gain[None, :], norm_gain[None, :], table)

    def exchange(slots):
        slots = slots.reshape(experts, capacity, model_width)
        slots = lax.all_to_all(slots, ("sp", "tp"), split_axis=0, concat_axis=0, tiled=True)
        return slots.reshape(slots_total, model_width)

    hidden = expert_gate.shape[2]
    done = pl.pallas_call(
        expert_kernel,
        out_shape=slots_shape,
        in_specs=[VMEM] * 4,
        out_specs=VMEM,
        scratch_shapes=[pltpu.VMEM((slots_total, hidden), jnp.bfloat16)],
        cost_estimate=pl.CostEstimate(
            flops=6 * slots_total * model_width * hidden,
            bytes_accessed=16 << 20,
            transcendentals=slots_total * hidden,
        ),
        compiler_params=pltpu.CompilerParams(vmem_limit_bytes=24 * 1024 * 1024),
    )(exchange(outgoing), expert_gate[0], expert_up[0], expert_down[0])
    return pl.pallas_call(
        functools.partial(gather_kernel, top_count),
        out_shape=rows_shape,
        in_specs=[VMEM] * 3,
        out_specs=HBM,
        scratch_shapes=[
            pltpu.VMEM((row_count, model_width), jnp.bfloat16),
            pltpu.SemaphoreType.DMA((4,)),
        ],
        cost_estimate=pl.CostEstimate(
            flops=4 * row_count * slots_total * model_width,
            bytes_accessed=3 << 20,
            transcendentals=0,
        ),
        compiler_params=pltpu.CompilerParams(vmem_limit_bytes=12 * 1024 * 1024),
    )(stream, exchange(done), table)


def solution(mesh):
    return jax.shard_map(
        functools.partial(local, mesh.shape["sp"], mesh.shape["tp"]),
        mesh=mesh,
        in_specs=(
            P("sp", "tp"),
            P("sp", "tp"),
            P("sp", "tp"),
            P(("sp", "tp"), None),
            P(),
            P(),
            P(),
            P(("sp", "tp"), None),
            P(("sp", "tp"), None),
            P(("sp", "tp"), None, None),
            P(("sp", "tp"), None, None),
            P(("sp", "tp"), None, None),
        ),
        out_specs=P(("sp", "tp"), None),
        check_vma=False,
    )
```

```python
import functools
import math

import jax
import jax.numpy as jnp
from jax import lax
from jax.experimental import pallas as pl
from jax.experimental.pallas import tpu as pltpu
from jax.sharding import PartitionSpec as P


HEAD_SIZE = 64
GRID_W = 64
HALF_KEYS = 256
ONES_ROWS = 16

epsilon = 1e-06
base_theta = 10000.0

VMEM = pl.BlockSpec(memory_space=pltpu.VMEM)
HBM = pl.BlockSpec(memory_space=pltpu.HBM)


def rotation_tables(row_count, lanes):
    quarter = HEAD_SIZE // 4
    lane = jnp.arange(lanes, dtype=jnp.int32) % HEAD_SIZE
    index = jnp.arange(row_count + GRID_W, dtype=jnp.int32)
    place = jnp.where(index < row_count, index, index - row_count)
    frequency = base_theta ** (-(lane % quarter).astype(jnp.float32) / quarter)
    angle = place.astype(jnp.float32)[:, None] * frequency[None, :]
    sign = jnp.where((lane // quarter) % 2 == 0, -1.0, 1.0).astype(jnp.float32)
    return jnp.cos(angle), jnp.sin(angle) * sign[None, :]


class Rotation:
    def __init__(self, cos_ref, sin_ref, lanes):
        rows = lax.broadcasted_iota(jnp.int32, (lanes, lanes), 0)
        cols = lax.broadcasted_iota(jnp.int32, (lanes, lanes), 1)
        same_head = (rows // HEAD_SIZE) == (cols // HEAD_SIZE)
        self.mean_mat = jnp.where(same_head, 1.0 / HEAD_SIZE, 0.0).astype(jnp.bfloat16)
        self.swap_mat = jnp.where((rows ^ (HEAD_SIZE // 4)) == cols, 1.0, 0.0).astype(jnp.bfloat16)
        lane = lax.broadcasted_iota(jnp.int32, (GRID_W, lanes), 1)
        self.by_row = (lane % HEAD_SIZE) < HEAD_SIZE // 2
        self.refs = (cos_ref, sin_ref)

    def table(self, ref, first_row, count):
        total = ref.shape[0] - GRID_W
        cols = ref[total:, :]
        parts = [
            jnp.where(self.by_row, ref[pl.ds(first_row + i, 1), :], cols) for i in range(count)
        ]
        return jnp.concatenate(parts, axis=0)

    def ready(self, raw, first_row, factor):
        count = raw.shape[0] // GRID_W
        cos = self.table(self.refs[0], first_row, count)
        sin = self.table(self.refs[1], first_row, count)
        wide = raw.astype(jnp.float32)
        square = wide * wide
        high = square.astype(jnp.bfloat16)
        low = (square - high.astype(jnp.float32)).astype(jnp.bfloat16)
        mean = jnp.dot(high, self.mean_mat, preferred_element_type=jnp.float32) + jnp.dot(
            low, self.mean_mat, preferred_element_type=jnp.float32
        )
        swapped = jnp.dot(raw, self.swap_mat, preferred_element_type=jnp.float32)
        length = lax.rsqrt(mean + epsilon) * factor
        return (wide * cos + swapped * sin) * length


def ring_place(index, count):
    return jnp.where(index % 2 == 0, index // 2, count - (index + 1) // 2)


def ring_member(place, count):
    place = lax.rem(place + count, count)
    return jnp.where(2 * place < count, 2 * place, 2 * (count - place) - 1)


def attend_kernel(sp_size, pieces, last, raw_queries, after, *refs):
    refs = list(refs)
    first_ref = refs.pop(0)
    cos_ref, sin_ref = refs.pop(0), refs.pop(0)
    chunks = [refs.pop(0) for _ in pieces]
    acc_in = None if raw_queries else refs.pop(0)
    for _ in range(after):
        refs.pop(0)
    outs = [refs.pop(0) for _ in range(2 if raw_queries else 1)] if not last else None
    if last:
        outs, refs = refs[:-3], refs[-3:]
    keys_ref, values_ref = refs[0], refs[1]
    lanes = chunks[0].shape[-1]
    rotation = Rotation(cos_ref, sin_ref, lanes)
    me = lax.axis_index("sp")
    place = ring_place(me, sp_size)
    grid_rows = (cos_ref.shape[0] - GRID_W) // sp_size
    if raw_queries:
        q_ref = outs[0]
        factor = math.log2(math.e) * HEAD_SIZE ** (-0.5)
        tok_count, q_lanes = first_ref.shape
        group = q_lanes // lanes
        q_ref[...] = jnp.zeros_like(q_ref)
        for block in range(group):
            raw = first_ref[:, block * lanes : (block + 1) * lanes]
            turned = rotation.ready(raw, me * grid_rows, factor).T
            for inner in range(lanes // HEAD_SIZE):
                head = block * (lanes // HEAD_SIZE) + inner
                kv_head = head // group
                q_ref[
                    kv_head * HEAD_SIZE : (kv_head + 1) * HEAD_SIZE,
                    head * tok_count : (head + 1) * tok_count,
                ] = turned[inner * HEAD_SIZE : (inner + 1) * HEAD_SIZE].astype(jnp.bfloat16)
    else:
        q_ref = first_ref
    _, columns = q_ref.shape
    width = min(512, columns)
    blocks = columns // width
    kv_heads = lanes // HEAD_SIZE
    ones = jnp.ones((ONES_ROWS, HALF_KEYS), jnp.bfloat16)
    halves = 0
    for chunk, (distance, first_half) in zip(chunks, pieces):
        source = ring_member(place + distance, sp_size)
        for half in range(chunk.shape[0]):
            row = source * grid_rows + (first_half + half) * (HALF_KEYS // GRID_W)
            keys_ref[halves] = rotation.ready(chunk[half, 0], row, 1.0).astype(jnp.bfloat16)
            turned = chunk[half, 1].astype(jnp.float32).T.astype(jnp.bfloat16)
            for head in range(kv_heads):
                values_ref[halves, head, :HEAD_SIZE, :] = turned[
                    head * HEAD_SIZE : (head + 1) * HEAD_SIZE
                ]
                values_ref[halves, head, HEAD_SIZE:, :] = ones
            halves += 1
    waiting = None
    for block in range(blocks + 1):
        weights = []
        total = None
        for half in range(halves):
            if block < blocks:
                scores = jnp.dot(
                    keys_ref[half],
                    q_ref[:, block * width : (block + 1) * width],
                    preferred_element_type=jnp.float32,
                )
                weights.append(jnp.exp2(scores).astype(jnp.bfloat16))
            if waiting is not None:
                kv_head = (block - 1) * kv_heads // blocks
                piece = jnp.dot(
                    values_ref[half, kv_head], waiting[half], preferred_element_type=jnp.float32
                )
                total = piece if total is None else total + piece
        if waiting is not None:
            at = (block - 1) * width
            if acc_in is not None:
                total = total + acc_in[:, at : at + width]
            if not last:
                outs[-1][:, at : at + width] = total
            else:
                turn = refs[2]
                tp, _, per = turn.shape
                tok_count = tp * per
                ready = (total[:HEAD_SIZE] / total[HEAD_SIZE : HEAD_SIZE + 1]).astype(jnp.bfloat16)
                for piece in range(width // per):
                    head, spot = divmod(at + piece * per, tok_count)
                    turn[spot // per, head * HEAD_SIZE : (head + 1) * HEAD_SIZE, :] = ready[
                        :, piece * per : (piece + 1) * per
                    ]
        waiting = weights
    if last:
        me = lax.axis_index("tp")
        for rel, out in enumerate(outs):
            out[...] = refs[2][me ^ rel]


def attend(queries, tables, chunks, pieces, acc, sp_size, tp_size, last=False, after=()):
    raw_queries = acc is None
    lanes = chunks[0].shape[-1]
    rows = HEAD_SIZE + ONES_ROWS
    halves = sum(c.shape[0] for c in chunks)
    if raw_queries:
        columns = queries.shape[0] * queries.shape[1] // HEAD_SIZE
        tok_count = queries.shape[0]
    else:
        columns = queries.shape[1]
        tok_count = chunks[0].shape[0] * HALF_KEYS * 2
    scratch = [
        pltpu.VMEM((halves, HALF_KEYS, lanes), jnp.bfloat16),
        pltpu.VMEM((halves, lanes // HEAD_SIZE, rows, HALF_KEYS), jnp.bfloat16),
    ]
    if last:
        head_rows = columns // tok_count * HEAD_SIZE
        block = (head_rows, tok_count // tp_size)
        shape = [jax.ShapeDtypeStruct(block, jnp.bfloat16)] * tp_size
        scratch.append(pltpu.VMEM((tp_size, *block), jnp.bfloat16))
    else:
        shape = [jax.ShapeDtypeStruct((rows, columns), jnp.float32)]
        if raw_queries:
            shape = [jax.ShapeDtypeStruct((lanes, columns), jnp.bfloat16)] + shape
    operands = [queries, *tables, *chunks] + ([] if raw_queries else [acc])
    aliases = {} if (raw_queries or last) else {len(operands) - 1: 0}
    key_count = halves * HALF_KEYS
    return pl.pallas_call(
        functools.partial(attend_kernel, sp_size, pieces, last, raw_queries, len(after)),
        out_shape=shape,
        in_specs=[VMEM] * len(operands) + [HBM] * len(after),
        out_specs=[VMEM] * len(shape),
        scratch_shapes=scratch,
        input_output_aliases=aliases,
        cost_estimate=pl.CostEstimate(
            flops=2 * key_count * columns * 512,
            bytes_accessed=key_count * 1024,
            transcendentals=key_count * columns,
        ),
        compiler_params=pltpu.CompilerParams(vmem_limit_bytes=24 * 1024 * 1024),
    )(*operands, *after)


def direct_exchange(pieces, tp_size):
    held = {0: pieces[0]}
    for rel in reversed(range(1, tp_size)):
        held[rel] = lax.ppermute(pieces[rel], "tp", [(i, i ^ rel) for i in range(tp_size)])
    return [held[rel] for rel in range(tp_size)]


def out_kernel(tp_size, top_count, *refs):
    blocks = refs[:tp_size]
    w_ref, res_ref, mix_ref, norm_ref, table_ref = refs[tp_size : tp_size + 5]
    stream_ref, out_ref, normed_ref, mixed_ref = refs[tp_size + 5 :]
    me = lax.axis_index("tp")
    head_rows, row_count = blocks[0].shape
    width = w_ref.shape[1]
    step = min(512, width)
    turned = [b[...].astype(jnp.float32).T.astype(jnp.bfloat16) for b in blocks]
    power = jnp.zeros((row_count, 1), jnp.float32)
    for at in range(0, width, step):
        mixed = jnp.zeros((row_count, step), jnp.float32)
        for rel in range(tp_size):
            begin = pl.multiple_of((me ^ rel) * head_rows, head_rows)
            mixed = mixed + jnp.dot(
                turned[rel],
                w_ref[pl.ds(begin, head_rows), at : at + step],
                preferred_element_type=jnp.float32,
            )
        mixed_ref[:, at : at + step] = mixed
        power = power + jnp.sum(mixed * mixed, axis=1, keepdims=True)
    scale = lax.rsqrt(power / width + epsilon)
    power = jnp.zeros((row_count, 1), jnp.float32)
    for at in range(0, width, step):
        cols = slice(at, at + step)
        stream = (
            res_ref[:, cols].astype(jnp.float32) + mixed_ref[:, cols] * scale * mix_ref[:, cols]
        ).astype(jnp.bfloat16)
        stream_ref[:, cols] = stream
        wide = stream.astype(jnp.float32)
        power = power + jnp.sum(wide * wide, axis=1, keepdims=True)
    scale = lax.rsqrt(power / width + epsilon)
    for at in range(0, width, step):
        cols = slice(at, at + step)
        wide = stream_ref[:, cols].astype(jnp.float32)
        normed_ref[:, cols] = (wide * scale * norm_ref[:, cols]).astype(jnp.bfloat16)
    fill_slots(top_count, normed_ref, table_ref, out_ref)


def routes_kernel(capacity, expert_ref, weight_ref, out_ref):
    row_count, top_count = expert_ref.shape
    lanes = out_ref.shape[1]
    lane = lax.broadcasted_iota(jnp.int32, (row_count, lanes), 1)
    before = lax.broadcasted_iota(jnp.int32, (row_count, row_count), 0) > (
        lax.broadcasted_iota(jnp.int32, (row_count, row_count), 1)
    )
    before = jnp.where(before, 1.0, 0.0).astype(jnp.bfloat16)
    taken = jnp.zeros((1, lanes), jnp.float32)
    table = jnp.zeros((row_count, lanes), jnp.float32)
    for k in range(top_count):
        expert = expert_ref[:, k : k + 1]
        onehot = jnp.where(lane == expert, 1.0, 0.0)
        earlier = taken + jnp.dot(
            before, onehot.astype(jnp.bfloat16), preferred_element_type=jnp.float32
        )
        rank = jnp.sum(onehot * earlier, axis=1, keepdims=True)
        slot = expert.astype(jnp.float32) * capacity + rank
        taken = taken + jnp.sum(onehot, axis=0, keepdims=True)
        table = jnp.where(lane == k, slot, table)
        table = jnp.where(lane == top_count + k, weight_ref[:, k : k + 1], table)
    out_ref[...] = table.T[: out_ref.shape[0], :row_count]


def fill_slots(top_count, rows_ref, table_ref, out_ref):
    row_count, width = rows_ref.shape
    step = min(512, width)
    slot_count = out_ref.shape[0]
    slots = lax.broadcasted_iota(jnp.int32, (slot_count, row_count), 0)
    slots = slots.astype(jnp.float32)
    hit = slots == table_ref[0:1, :]
    for k in range(1, top_count):
        hit = hit | (slots == table_ref[k : k + 1, :])
    placing = jnp.where(hit, 1.0, 0.0).astype(jnp.bfloat16)
    for at in range(0, width, step):
        cols = slice(at, at + step)
        out_ref[:, cols] = jnp.dot(
            placing, rows_ref[:, cols], preferred_element_type=jnp.float32
        ).astype(jnp.bfloat16)


def gather_kernel(top_count, base_ref, slots_ref, table_ref, out_hbm, out_ref, sems):
    row_count, width = base_ref.shape
    step = width // sems.shape[0]
    table = table_ref[...].T
    slots = lax.broadcasted_iota(jnp.int32, (row_count, slots_ref.shape[0]), 1)
    slots = slots.astype(jnp.float32)
    picks = [
        jnp.where(slots == table[:, k : k + 1], 1.0, 0.0).astype(jnp.bfloat16)
        for k in range(top_count)
    ]
    picks = jnp.concatenate(picks, axis=0)
    copies = []
    for i in range(sems.shape[0]):
        cols = pl.ds(i * step, step)
        rows = jnp.dot(picks, slots_ref[:, cols], preferred_element_type=jnp.float32)
        total = None
        for k in range(top_count):
            row = rows[k * row_count : (k + 1) * row_count]
            row = row * table[:, top_count + k : top_count + k + 1]
            total = row if total is None else total + row
        out_ref[:, cols] = (base_ref[:, cols].astype(jnp.float32) + total).astype(out_ref.dtype)
        copies.append(
            pltpu.make_async_copy(out_ref.at[:, cols], out_hbm.at[:, cols], sems.at[i])
        )
        copies[-1].start()
    for copy in copies:
        copy.wait()


def expert_kernel(rows_ref, gate_ref, up_ref, down_ref, out_ref, act_ref):
    hidden = gate_ref.shape[1]
    width = down_ref.shape[1]
    step = min(256, hidden)
    for at in range(0, hidden, step):
        cols = slice(at, at + step)
        gate = jnp.dot(rows_ref[...], gate_ref[:, cols], preferred_element_type=jnp.float32)
        up = jnp.dot(rows_ref[...], up_ref[:, cols], preferred_element_type=jnp.float32)
        act_ref[:, cols] = (gate / (1.0 + jnp.exp(-gate)) * up).astype(jnp.bfloat16)
    step = min(512, width)
    for at in range(0, width, step):
        cols = slice(at, at + step)
        out_ref[:, cols] = jnp.dot(
            act_ref[...], down_ref[:, cols], preferred_element_type=jnp.float32
        ).astype(jnp.bfloat16)


def layer(
    sp_size,
    tp_size,
    query_proj,
    projected_keys,
    projected_values,
    residual,
    out_weight,
    mix_gain,
    norm_gain,
    route_expert,
    route_weight,
    expert_gate,
    expert_up,
    expert_down,
):
    tok_count, lanes = projected_keys.shape
    model_width = residual.shape[1]
    halves = tok_count // HALF_KEYS
    tables = rotation_tables(sp_size * tok_count // GRID_W, lanes)
    raw_own = jnp.stack(
        [part.reshape(halves, HALF_KEYS, lanes) for part in (projected_keys, projected_values)],
        axis=1,
    )

    row_count = residual.shape[0]
    top_count = route_expert.shape[1]
    experts = sp_size * tp_size
    capacity = max(2, 2 * top_count * row_count // experts)
    slots_total = experts * capacity
    table = pl.pallas_call(
        functools.partial(routes_kernel, capacity),
        out_shape=jax.ShapeDtypeStruct((8, row_count), jnp.float32),
        in_specs=[VMEM] * 2,
        out_specs=VMEM,
        cost_estimate=pl.CostEstimate(flops=1 << 22, bytes_accessed=1 << 17, transcendentals=0),
        compiler_params=pltpu.CompilerParams(vmem_limit_bytes=8 * 1024 * 1024),
    )(route_expert, route_weight)

    order = list(range(0, sp_size, 2)) + list(range(sp_size - 1, 0, -2))
    ahead = [(order[i], order[(i + 1) % sp_size]) for i in range(sp_size)]
    behind = [(b, a) for a, b in ahead]
    steps = sp_size // 2
    acc = None
    queries = query_proj
    from_left = from_right = raw_own
    held, pieces = [raw_own], [(0, 0)]
    for step in range(steps):
        if step == steps - 1:
            from_left, from_right = from_left[: halves // 2], from_right[halves // 2 :]
        next_left = lax.ppermute(from_left, "sp", ahead)
        next_right = lax.ppermute(from_right, "sp", behind)
        after = (table,) if step == steps - 1 else ()
        out = attend(queries, tables, held, pieces, acc, sp_size, tp_size, after=after)
        if step == 0:
            queries, acc = out
        else:
            (acc,) = out
        from_left, from_right = next_left, next_right
        held = [from_left, from_right]
        pieces = [(-step - 1, 0), (step + 1, halves // 2 if step == steps - 1 else 0)]
    (acc,) = attend(queries, tables, held[1:], pieces[1:], acc, sp_size, tp_size)
    pieces = attend(queries, tables, held[:1], pieces[:1], acc, sp_size, tp_size, last=True)
    blocks = direct_exchange(pieces, tp_size)

    rows_shape = jax.ShapeDtypeStruct((row_count, model_width), jnp.bfloat16)
    slots_shape = jax.ShapeDtypeStruct((slots_total, model_width), jnp.bfloat16)
    stream, outgoing = pl.pallas_call(
        functools.partial(out_kernel, tp_size, top_count),
        out_shape=(rows_shape, slots_shape),
        in_specs=[VMEM] * (tp_size + 5),
        out_specs=(VMEM, VMEM),
        scratch_shapes=[
            pltpu.VMEM((row_count, model_width), jnp.bfloat16),
            pltpu.VMEM((row_count, model_width), jnp.float32),
        ],
        cost_estimate=pl.CostEstimate(
            flops=2 * row_count * model_width * (out_weight.shape[0] + slots_total),
            bytes_accessed=8 << 20,
            transcendentals=0,
        ),
        compiler_params=pltpu.CompilerParams(vmem_limit_bytes=12 * 1024 * 1024),
    )(*blocks, out_weight, residual, mix_gain[None, :], norm_gain[None, :], table)

    def exchange(slots):
        slots = slots.reshape(experts, capacity, model_width)
        slots = lax.all_to_all(slots, ("sp", "tp"), split_axis=0, concat_axis=0, tiled=True)
        return slots.reshape(slots_total, model_width)

    hidden = expert_gate.shape[2]
    done = pl.pallas_call(
        expert_kernel,
        out_shape=slots_shape,
        in_specs=[VMEM] * 4,
        out_specs=VMEM,
        scratch_shapes=[pltpu.VMEM((slots_total, hidden), jnp.bfloat16)],
        cost_estimate=pl.CostEstimate(
            flops=6 * slots_total * model_width * hidden,
            bytes_accessed=16 << 20,
            transcendentals=slots_total * hidden,
        ),
        compiler_params=pltpu.CompilerParams(vmem_limit_bytes=24 * 1024 * 1024),
    )(exchange(outgoing), expert_gate[0], expert_up[0], expert_down[0])
    return pl.pallas_call(
        functools.partial(gather_kernel, top_count),
        out_shape=rows_shape,
        in_specs=[VMEM] * 3,
        out_specs=HBM,
        scratch_shapes=[
            pltpu.VMEM((row_count, model_width), jnp.bfloat16),
            pltpu.SemaphoreType.DMA((4,)),
        ],
        cost_estimate=pl.CostEstimate(
            flops=4 * row_count * slots_total * model_width,
            bytes_accessed=3 << 20,
            transcendentals=0,
        ),
        compiler_params=pltpu.CompilerParams(vmem_limit_bytes=12 * 1024 * 1024),
    )(stream, exchange(done), table)


def solution(mesh):
    return jax.shard_map(
        functools.partial(layer, mesh.shape["sp"], mesh.shape["tp"]),
        mesh=mesh,
        in_specs=(
            P("sp", "tp"),
            P("sp", "tp"),
            P("sp", "tp"),
            P(("sp", "tp"), None),
            P(),
            P(),
            P(),
            P(("sp", "tp"), None),
            P(("sp", "tp"), None),
            P(("sp", "tp"), None, None),
            P(("sp", "tp"), None, None),
            P(("sp", "tp"), None, None),
        ),
        out_specs=P(("sp", "tp"), None),
        check_vma=False,
    )
```

```python
import functools
import math

import jax
import jax.numpy as jnp
from jax import lax
from jax.experimental import pallas as pl
from jax.experimental.pallas import tpu as pltpu
from jax.sharding import PartitionSpec as P


HEAD_SIZE = 64
GRID_W = 64
HALF_KEYS = 256
ONES_ROWS = 16

epsilon = 1e-06
base_theta = 10000.0

VMEM = pl.BlockSpec(memory_space=pltpu.VMEM)
HBM = pl.BlockSpec(memory_space=pltpu.HBM)


def rotation_tables(row_count, lanes):
    quarter = HEAD_SIZE // 4
    lane = jnp.arange(lanes, dtype=jnp.int32) % HEAD_SIZE
    index = jnp.arange(row_count + GRID_W, dtype=jnp.int32)
    place = jnp.where(index < row_count, index, index - row_count)
    frequency = base_theta ** (-(lane % quarter).astype(jnp.float32) / quarter)
    angle = place.astype(jnp.float32)[:, None] * frequency[None, :]
    sign = jnp.where((lane // quarter) % 2 == 0, -1.0, 1.0).astype(jnp.float32)
    return jnp.cos(angle), jnp.sin(angle) * sign[None, :]


class Rotation:
    def __init__(self, cos_ref, sin_ref, lanes):
        rows = lax.broadcasted_iota(jnp.int32, (lanes, lanes), 0)
        cols = lax.broadcasted_iota(jnp.int32, (lanes, lanes), 1)
        same_head = (rows // HEAD_SIZE) == (cols // HEAD_SIZE)
        self.mean_mat = jnp.where(same_head, 1.0 / HEAD_SIZE, 0.0).astype(jnp.bfloat16)
        self.swap_mat = jnp.where((rows ^ (HEAD_SIZE // 4)) == cols, 1.0, 0.0).astype(jnp.bfloat16)
        lane = lax.broadcasted_iota(jnp.int32, (GRID_W, lanes), 1)
        self.by_row = (lane % HEAD_SIZE) < HEAD_SIZE // 2
        self.refs = (cos_ref, sin_ref)

    def table(self, ref, first_row, count):
        total = ref.shape[0] - GRID_W
        cols = ref[total:, :]
        parts = [
            jnp.where(self.by_row, ref[pl.ds(first_row + i, 1), :], cols) for i in range(count)
        ]
        return jnp.concatenate(parts, axis=0)

    def ready(self, raw, first_row, factor):
        count = raw.shape[0] // GRID_W
        cos = self.table(self.refs[0], first_row, count)
        sin = self.table(self.refs[1], first_row, count)
        wide = raw.astype(jnp.float32)
        square = wide * wide
        high = square.astype(jnp.bfloat16)
        low = (square - high.astype(jnp.float32)).astype(jnp.bfloat16)
        mean = jnp.dot(high, self.mean_mat, preferred_element_type=jnp.float32) + jnp.dot(
            low, self.mean_mat, preferred_element_type=jnp.float32
        )
        swapped = jnp.dot(raw, self.swap_mat, preferred_element_type=jnp.float32)
        length = lax.rsqrt(mean + epsilon) * factor
        return (wide * cos + swapped * sin) * length


def ring_place(index, count):
    return jnp.where(index % 2 == 0, index // 2, count - (index + 1) // 2)


def ring_member(place, count):
    place = lax.rem(place + count, count)
    return jnp.where(2 * place < count, 2 * place, 2 * (count - place) - 1)


def attend_kernel(sp_size, pieces, last, raw_queries, after, *refs):
    refs = list(refs)
    first_ref = refs.pop(0)
    cos_ref, sin_ref = refs.pop(0), refs.pop(0)
    chunks = [refs.pop(0) for _ in pieces]
    acc_in = None if raw_queries else refs.pop(0)
    for _ in range(after):
        refs.pop(0)
    outs = [refs.pop(0) for _ in range(2 if raw_queries else 1)] if not last else None
    if last:
        outs, refs = refs[:-3], refs[-3:]
    keys_ref, values_ref = refs[0], refs[1]
    lanes = chunks[0].shape[-1]
    rotation = Rotation(cos_ref, sin_ref, lanes)
    me = lax.axis_index("sp")
    place = ring_place(me, sp_size)
    grid_rows = (cos_ref.shape[0] - GRID_W) // sp_size
    if raw_queries:
        q_ref = outs[0]
        factor = math.log2(math.e) * HEAD_SIZE ** (-0.5)
        tok_count, q_lanes = first_ref.shape
        group = q_lanes // lanes
        q_ref[...] = jnp.zeros_like(q_ref)
        for block in range(group):
            raw = first_ref[:, block * lanes : (block + 1) * lanes]
            turned = rotation.ready(raw, me * grid_rows, factor).T
            for inner in range(lanes // HEAD_SIZE):
                head = block * (lanes // HEAD_SIZE) + inner
                kv_head = head // group
                q_ref[
                    kv_head * HEAD_SIZE : (kv_head + 1) * HEAD_SIZE,
                    head * tok_count : (head + 1) * tok_count,
                ] = turned[inner * HEAD_SIZE : (inner + 1) * HEAD_SIZE].astype(jnp.bfloat16)
    else:
        q_ref = first_ref
    _, columns = q_ref.shape
    width = min(512, columns)
    blocks = columns // width
    kv_heads = lanes // HEAD_SIZE
    ones = jnp.ones((ONES_ROWS, HALF_KEYS), jnp.bfloat16)
    halves = 0
    for chunk, (distance, first_half) in zip(chunks, pieces):
        source = ring_member(place + distance, sp_size)
        for half in range(chunk.shape[0]):
            row = source * grid_rows + (first_half + half) * (HALF_KEYS // GRID_W)
            keys_ref[halves] = rotation.ready(chunk[half, 0], row, 1.0).astype(jnp.bfloat16)
            turned = chunk[half, 1].astype(jnp.float32).T.astype(jnp.bfloat16)
            for head in range(kv_heads):
                values_ref[halves, head, :HEAD_SIZE, :] = turned[
                    head * HEAD_SIZE : (head + 1) * HEAD_SIZE
                ]
                values_ref[halves, head, HEAD_SIZE:, :] = ones
            halves += 1
    waiting = None
    for block in range(blocks + 1):
        weights = []
        total = None
        for half in range(halves):
            if block < blocks:
                scores = jnp.dot(
                    keys_ref[half],
                    q_ref[:, block * width : (block + 1) * width],
                    preferred_element_type=jnp.float32,
                )
                weights.append(jnp.exp2(scores).astype(jnp.bfloat16))
            if waiting is not None:
                kv_head = (block - 1) * kv_heads // blocks
                piece = jnp.dot(
                    values_ref[half, kv_head], waiting[half], preferred_element_type=jnp.float32
                )
                total = piece if total is None else total + piece
        if waiting is not None:
            at = (block - 1) * width
            if acc_in is not None:
                total = total + acc_in[:, at : at + width]
            if not last:
                outs[-1][:, at : at + width] = total
            else:
                turn = refs[2]
                tp, _, per = turn.shape
                tok_count = tp * per
                ready = (total[:HEAD_SIZE] / total[HEAD_SIZE : HEAD_SIZE + 1]).astype(jnp.bfloat16)
                for piece in range(width // per):
                    head, spot = divmod(at + piece * per, tok_count)
                    turn[spot // per, head * HEAD_SIZE : (head + 1) * HEAD_SIZE, :] = ready[
                        :, piece * per : (piece + 1) * per
                    ]
        waiting = weights
    if last:
        me = lax.axis_index("tp")
        for rel, out in enumerate(outs):
            out[...] = refs[2][me ^ rel]


def attend(queries, tables, chunks, pieces, acc, sp_size, tp_size, last=False, after=()):
    raw_queries = acc is None
    lanes = chunks[0].shape[-1]
    rows = HEAD_SIZE + ONES_ROWS
    halves = sum(c.shape[0] for c in chunks)
    if raw_queries:
        columns = queries.shape[0] * queries.shape[1] // HEAD_SIZE
        tok_count = queries.shape[0]
    else:
        columns = queries.shape[1]
        tok_count = chunks[0].shape[0] * HALF_KEYS * 2
    scratch = [
        pltpu.VMEM((halves, HALF_KEYS, lanes), jnp.bfloat16),
        pltpu.VMEM((halves, lanes // HEAD_SIZE, rows, HALF_KEYS), jnp.bfloat16),
    ]
    if last:
        head_rows = columns // tok_count * HEAD_SIZE
        block = (head_rows, tok_count // tp_size)
        shape = [jax.ShapeDtypeStruct(block, jnp.bfloat16)] * tp_size
        scratch.append(pltpu.VMEM((tp_size, *block), jnp.bfloat16))
    else:
        shape = [jax.ShapeDtypeStruct((rows, columns), jnp.float32)]
        if raw_queries:
            shape = [jax.ShapeDtypeStruct((lanes, columns), jnp.bfloat16)] + shape
    operands = [queries, *tables, *chunks] + ([] if raw_queries else [acc])
    aliases = {} if (raw_queries or last) else {len(operands) - 1: 0}
    key_count = halves * HALF_KEYS
    return pl.pallas_call(
        functools.partial(attend_kernel, sp_size, pieces, last, raw_queries, len(after)),
        out_shape=shape,
        in_specs=[VMEM] * len(operands) + [HBM] * len(after),
        out_specs=[VMEM] * len(shape),
        scratch_shapes=scratch,
        input_output_aliases=aliases,
        cost_estimate=pl.CostEstimate(
            flops=2 * key_count * columns * 512,
            bytes_accessed=key_count * 1024,
            transcendentals=key_count * columns,
        ),
        compiler_params=pltpu.CompilerParams(vmem_limit_bytes=24 * 1024 * 1024),
    )(*operands, *after)


def direct_exchange(pieces, tp_size):
    held = {0: pieces[0]}
    for rel in reversed(range(1, tp_size)):
        held[rel] = lax.ppermute(pieces[rel], "tp", [(i, i ^ rel) for i in range(tp_size)])
    return [held[rel] for rel in range(tp_size)]


def out_kernel(tp_size, top_count, *refs):
    blocks = refs[:tp_size]
    w_ref, res_ref, mix_ref, norm_ref, table_ref = refs[tp_size : tp_size + 5]
    stream_ref, out_ref, normed_ref, mixed_ref = refs[tp_size + 5 :]
    me = lax.axis_index("tp")
    head_rows, row_count = blocks[0].shape
    width = w_ref.shape[1]
    step = min(512, width)
    turned = [b[...].astype(jnp.float32).T.astype(jnp.bfloat16) for b in blocks]
    power = jnp.zeros((row_count, 1), jnp.float32)
    for at in range(0, width, step):
        mixed = jnp.zeros((row_count, step), jnp.float32)
        for rel in range(tp_size):
            begin = pl.multiple_of((me ^ rel) * head_rows, head_rows)
            mixed = mixed + jnp.dot(
                turned[rel],
                w_ref[pl.ds(begin, head_rows), at : at + step],
                preferred_element_type=jnp.float32,
            )
        mixed_ref[:, at : at + step] = mixed
        power = power + jnp.sum(mixed * mixed, axis=1, keepdims=True)
    scale = lax.rsqrt(power / width + epsilon)
    power = jnp.zeros((row_count, 1), jnp.float32)
    for at in range(0, width, step):
        cols = slice(at, at + step)
        stream = (
            res_ref[:, cols].astype(jnp.float32) + mixed_ref[:, cols] * scale * mix_ref[:, cols]
        ).astype(jnp.bfloat16)
        stream_ref[:, cols] = stream
        wide = stream.astype(jnp.float32)
        power = power + jnp.sum(wide * wide, axis=1, keepdims=True)
    scale = lax.rsqrt(power / width + epsilon)
    for at in range(0, width, step):
        cols = slice(at, at + step)
        wide = stream_ref[:, cols].astype(jnp.float32)
        normed_ref[:, cols] = (wide * scale * norm_ref[:, cols]).astype(jnp.bfloat16)
    fill_slots(top_count, normed_ref, table_ref, out_ref)


def routes_kernel(capacity, expert_ref, weight_ref, out_ref):
    row_count, top_count = expert_ref.shape
    lanes = out_ref.shape[1]
    lane = lax.broadcasted_iota(jnp.int32, (row_count, lanes), 1)
    before = lax.broadcasted_iota(jnp.int32, (row_count, row_count), 0) > (
        lax.broadcasted_iota(jnp.int32, (row_count, row_count), 1)
    )
    before = jnp.where(before, 1.0, 0.0).astype(jnp.bfloat16)
    taken = jnp.zeros((1, lanes), jnp.float32)
    table = jnp.zeros((row_count, lanes), jnp.float32)
    for k in range(top_count):
        expert = expert_ref[:, k : k + 1]
        onehot = jnp.where(lane == expert, 1.0, 0.0)
        earlier = taken + jnp.dot(
            before, onehot.astype(jnp.bfloat16), preferred_element_type=jnp.float32
        )
        rank = jnp.sum(onehot * earlier, axis=1, keepdims=True)
        slot = expert.astype(jnp.float32) * capacity + rank
        taken = taken + jnp.sum(onehot, axis=0, keepdims=True)
        table = jnp.where(lane == k, slot, table)
        table = jnp.where(lane == top_count + k, weight_ref[:, k : k + 1], table)
    out_ref[...] = table.T[: out_ref.shape[0], :row_count]


def fill_slots(top_count, rows_ref, table_ref, out_ref):
    row_count, width = rows_ref.shape
    step = min(512, width)
    slot_count = out_ref.shape[0]
    slots = lax.broadcasted_iota(jnp.int32, (slot_count, row_count), 0)
    slots = slots.astype(jnp.float32)
    hit = slots == table_ref[0:1, :]
    for k in range(1, top_count):
        hit = hit | (slots == table_ref[k : k + 1, :])
    placing = jnp.where(hit, 1.0, 0.0).astype(jnp.bfloat16)
    for at in range(0, width, step):
        cols = slice(at, at + step)
        out_ref[:, cols] = jnp.dot(
            placing, rows_ref[:, cols], preferred_element_type=jnp.float32
        ).astype(jnp.bfloat16)


def gather_kernel(top_count, base_ref, slots_ref, table_ref, out_hbm, out_ref, sems):
    row_count, width = base_ref.shape
    step = width // sems.shape[0]
    table = table_ref[...].T
    slots = lax.broadcasted_iota(jnp.int32, (row_count, slots_ref.shape[0]), 1)
    slots = slots.astype(jnp.float32)
    picks = [
        jnp.where(slots == table[:, k : k + 1], 1.0, 0.0).astype(jnp.bfloat16)
        for k in range(top_count)
    ]
    picks = jnp.concatenate(picks, axis=0)
    copies = []
    for i in range(sems.shape[0]):
        cols = pl.ds(i * step, step)
        rows = jnp.dot(picks, slots_ref[:, cols], preferred_element_type=jnp.float32)
        total = None
        for k in range(top_count):
            row = rows[k * row_count : (k + 1) * row_count]
            row = row * table[:, top_count + k : top_count + k + 1]
            total = row if total is None else total + row
        out_ref[:, cols] = (base_ref[:, cols].astype(jnp.float32) + total).astype(out_ref.dtype)
        copies.append(
            pltpu.make_async_copy(out_ref.at[:, cols], out_hbm.at[:, cols], sems.at[i])
        )
        copies[-1].start()
    for copy in copies:
        copy.wait()


def expert_kernel(rows_ref, gate_ref, up_ref, down_ref, out_ref, act_ref):
    hidden = gate_ref.shape[1]
    width = down_ref.shape[1]
    step = min(256, hidden)
    for at in range(0, hidden, step):
        cols = slice(at, at + step)
        gate = jnp.dot(rows_ref[...], gate_ref[:, cols], preferred_element_type=jnp.float32)
        up = jnp.dot(rows_ref[...], up_ref[:, cols], preferred_element_type=jnp.float32)
        act_ref[:, cols] = (gate / (1.0 + jnp.exp(-gate)) * up).astype(jnp.bfloat16)
    step = min(512, width)
    for at in range(0, width, step):
        cols = slice(at, at + step)
        out_ref[:, cols] = jnp.dot(
            act_ref[...], down_ref[:, cols], preferred_element_type=jnp.float32
        ).astype(jnp.bfloat16)


def layer(
    sp_size,
    tp_size,
    query_proj,
    projected_keys,
    projected_values,
    residual,
    out_weight,
    mix_gain,
    norm_gain,
    route_expert,
    route_weight,
    expert_gate,
    expert_up,
    expert_down,
):
    tok_count, lanes = projected_keys.shape
    model_width = residual.shape[1]
    halves = tok_count // HALF_KEYS
    tables = rotation_tables(sp_size * tok_count // GRID_W, lanes)
    raw_own = jnp.stack(
        [part.reshape(halves, HALF_KEYS, lanes) for part in (projected_keys, projected_values)],
        axis=1,
    )

    row_count = residual.shape[0]
    top_count = route_expert.shape[1]
    experts = sp_size * tp_size
    capacity = max(2, 2 * top_count * row_count // experts)
    slots_total = experts * capacity
    table = pl.pallas_call(
        functools.partial(routes_kernel, capacity),
        out_shape=jax.ShapeDtypeStruct((8, row_count), jnp.float32),
        in_specs=[VMEM] * 2,
        out_specs=VMEM,
        cost_estimate=pl.CostEstimate(flops=1 << 22, bytes_accessed=1 << 17, transcendentals=0),
        compiler_params=pltpu.CompilerParams(vmem_limit_bytes=8 * 1024 * 1024),
    )(route_expert, route_weight)

    order = list(range(0, sp_size, 2)) + list(range(sp_size - 1, 0, -2))
    ahead = [(order[i], order[(i + 1) % sp_size]) for i in range(sp_size)]
    behind = [(b, a) for a, b in ahead]
    steps = sp_size // 2
    acc = None
    queries = query_proj
    from_left = from_right = [(raw_own, 0)]
    held, pieces = [raw_own], [(0, 0)]
    for step in range(steps):
        if step == 1:
            cuts = [(slice(0, halves // 2), 0), (slice(halves // 2, halves), halves // 2)]
            from_left = [(from_left[0][0][cut], first) for cut, first in cuts]
            from_right = [(from_right[0][0][cut], first) for cut, first in cuts]
        if step == steps - 1:
            from_left, from_right = from_left[:1], from_right[-1:]
        next_left, next_right = [], []
        for part in range(len(from_left)):
            left, first = from_left[part]
            next_left.append((lax.ppermute(left, "sp", ahead), first))
            right, first = from_right[part]
            next_right.append((lax.ppermute(right, "sp", behind), first))
        after = (table,) if step == steps - 1 else ()
        out = attend(queries, tables, held, pieces, acc, sp_size, tp_size, after=after)
        if step == 0:
            queries, acc = out
        else:
            (acc,) = out
        from_left, from_right = next_left, next_right
        held = [part for part, _ in from_left + from_right]
        pieces = [(-step - 1, first) for _, first in from_left]
        pieces += [(step + 1, first) for _, first in from_right]
    (acc,) = attend(queries, tables, held[1:], pieces[1:], acc, sp_size, tp_size)
    pieces = attend(queries, tables, held[:1], pieces[:1], acc, sp_size, tp_size, last=True)
    blocks = direct_exchange(pieces, tp_size)

    rows_shape = jax.ShapeDtypeStruct((row_count, model_width), jnp.bfloat16)
    slots_shape = jax.ShapeDtypeStruct((slots_total, model_width), jnp.bfloat16)
    stream, outgoing = pl.pallas_call(
        functools.partial(out_kernel, tp_size, top_count),
        out_shape=(rows_shape, slots_shape),
        in_specs=[VMEM] * (tp_size + 5),
        out_specs=(VMEM, VMEM),
        scratch_shapes=[
            pltpu.VMEM((row_count, model_width), jnp.bfloat16),
            pltpu.VMEM((row_count, model_width), jnp.float32),
        ],
        cost_estimate=pl.CostEstimate(
            flops=2 * row_count * model_width * (out_weight.shape[0] + slots_total),
            bytes_accessed=8 << 20,
            transcendentals=0,
        ),
        compiler_params=pltpu.CompilerParams(vmem_limit_bytes=12 * 1024 * 1024),
    )(*blocks, out_weight, residual, mix_gain[None, :], norm_gain[None, :], table)

    def exchange(slots):
        slots = slots.reshape(experts, capacity, model_width)
        slots = lax.all_to_all(slots, ("sp", "tp"), split_axis=0, concat_axis=0, tiled=True)
        return slots.reshape(slots_total, model_width)

    hidden = expert_gate.shape[2]
    done = pl.pallas_call(
        expert_kernel,
        out_shape=slots_shape,
        in_specs=[VMEM] * 4,
        out_specs=VMEM,
        scratch_shapes=[pltpu.VMEM((slots_total, hidden), jnp.bfloat16)],
        cost_estimate=pl.CostEstimate(
            flops=6 * slots_total * model_width * hidden,
            bytes_accessed=16 << 20,
            transcendentals=slots_total * hidden,
        ),
        compiler_params=pltpu.CompilerParams(vmem_limit_bytes=24 * 1024 * 1024),
    )(exchange(outgoing), expert_gate[0], expert_up[0], expert_down[0])
    return pl.pallas_call(
        functools.partial(gather_kernel, top_count),
        out_shape=rows_shape,
        in_specs=[VMEM] * 3,
        out_specs=HBM,
        scratch_shapes=[
            pltpu.VMEM((row_count, model_width), jnp.bfloat16),
            pltpu.SemaphoreType.DMA((4,)),
        ],
        cost_estimate=pl.CostEstimate(
            flops=4 * row_count * slots_total * model_width,
            bytes_accessed=3 << 20,
            transcendentals=0,
        ),
        compiler_params=pltpu.CompilerParams(vmem_limit_bytes=12 * 1024 * 1024),
    )(stream, exchange(done), table)


def solution(mesh):
    return jax.shard_map(
        functools.partial(layer, mesh.shape["sp"], mesh.shape["tp"]),
        mesh=mesh,
        in_specs=(
            P("sp", "tp"),
            P("sp", "tp"),
            P("sp", "tp"),
            P(("sp", "tp"), None),
            P(),
            P(),
            P(),
            P(("sp", "tp"), None),
            P(("sp", "tp"), None),
            P(("sp", "tp"), None, None),
            P(("sp", "tp"), None, None),
            P(("sp", "tp"), None, None),
        ),
        out_specs=P(("sp", "tp"), None),
        check_vma=False,
    )
```

```python
import functools
import math

import jax
import jax.numpy as jnp
from jax import lax
from jax.experimental import pallas as pl
from jax.experimental.pallas import tpu as pltpu
from jax.sharding import PartitionSpec as P

HEAD_SIZE = 64
GRID_W = 64
HALF_KEYS = 256
ONES_ROWS = 16

epsilon = 1e-06
base_theta = 10000.0

VMEM = pl.BlockSpec(memory_space=pltpu.VMEM)
HBM = pl.BlockSpec(memory_space=pltpu.HBM)


def rotation_tables(row_count, lanes):
    quarter = HEAD_SIZE // 4
    lane = jnp.arange(lanes, dtype=jnp.int32) % HEAD_SIZE
    index = jnp.arange(row_count + GRID_W, dtype=jnp.int32)
    place = jnp.where(index < row_count, index, index - row_count)
    frequency = base_theta ** (-(lane % quarter).astype(jnp.float32) / quarter)
    angle = place.astype(jnp.float32)[:, None] * frequency[None, :]
    sign = jnp.where((lane // quarter) % 2 == 0, -1.0, 1.0).astype(jnp.float32)
    return jnp.cos(angle), jnp.sin(angle) * sign[None, :]


class Rotation:
    def __init__(self, cos_ref, sin_ref, lanes):
        rows = lax.broadcasted_iota(jnp.int32, (lanes, lanes), 0)
        cols = lax.broadcasted_iota(jnp.int32, (lanes, lanes), 1)
        same_head = (rows // HEAD_SIZE) == (cols // HEAD_SIZE)
        self.mean_mat = jnp.where(same_head, 1.0 / HEAD_SIZE, 0.0).astype(jnp.bfloat16)
        self.swap_mat = jnp.where((rows ^ (HEAD_SIZE // 4)) == cols, 1.0, 0.0).astype(jnp.bfloat16)
        lane = lax.broadcasted_iota(jnp.int32, (GRID_W, lanes), 1)
        self.by_row = (lane % HEAD_SIZE) < HEAD_SIZE // 2
        self.refs = (cos_ref, sin_ref)

    def table(self, ref, first_row, count):
        total = ref.shape[0] - GRID_W
        cols = ref[total:, :]
        parts = [
            jnp.where(self.by_row, ref[pl.ds(first_row + i, 1), :], cols) for i in range(count)
        ]
        return jnp.concatenate(parts, axis=0)

    def ready(self, raw, first_row, factor):
        count = raw.shape[0] // GRID_W
        cos = self.table(self.refs[0], first_row, count)
        sin = self.table(self.refs[1], first_row, count)
        wide = raw.astype(jnp.float32)
        square = wide * wide
        high = square.astype(jnp.bfloat16)
        low = (square - high.astype(jnp.float32)).astype(jnp.bfloat16)
        mean = jnp.dot(high, self.mean_mat, preferred_element_type=jnp.float32) + jnp.dot(
            low, self.mean_mat, preferred_element_type=jnp.float32
        )
        swapped = jnp.dot(raw, self.swap_mat, preferred_element_type=jnp.float32)
        length = lax.rsqrt(mean + epsilon) * factor
        return (wide * cos + swapped * sin) * length


def ring_place(index, count):
    return jnp.where(index % 2 == 0, index // 2, count - (index + 1) // 2)


def ring_member(place, count):
    place = lax.rem(place + count, count)
    return jnp.where(2 * place < count, 2 * place, 2 * (count - place) - 1)


def attend_kernel(sp_size, pieces, last, raw_queries, after, *refs):
    refs = list(refs)
    first_ref = refs.pop(0)
    cos_ref, sin_ref = refs.pop(0), refs.pop(0)
    chunks = [refs.pop(0) for _ in pieces]
    acc_in = None if raw_queries else refs.pop(0)
    for _ in range(after):
        refs.pop(0)
    outs = [refs.pop(0) for _ in range(2 if raw_queries else 1)] if not last else None
    if last:
        outs, refs = refs[:-3], refs[-3:]
    keys_ref, values_ref = refs[0], refs[1]
    lanes = chunks[0].shape[-1]
    rotation = Rotation(cos_ref, sin_ref, lanes)
    me = lax.axis_index("sp")
    place = ring_place(me, sp_size)
    grid_rows = (cos_ref.shape[0] - GRID_W) // sp_size
    if raw_queries:
        q_ref = outs[0]
        factor = math.log2(math.e) * HEAD_SIZE ** (-0.5)
        tok_count, q_lanes = first_ref.shape
        group = q_lanes // lanes
        q_ref[...] = jnp.zeros_like(q_ref)
        for block in range(group):
            raw = first_ref[:, block * lanes : (block + 1) * lanes]
            turned = rotation.ready(raw, me * grid_rows, factor).T
            for inner in range(lanes // HEAD_SIZE):
                head = block * (lanes // HEAD_SIZE) + inner
                kv_head = head // group
                q_ref[
                    kv_head * HEAD_SIZE : (kv_head + 1) * HEAD_SIZE,
                    head * tok_count : (head + 1) * tok_count,
                ] = turned[inner * HEAD_SIZE : (inner + 1) * HEAD_SIZE].astype(jnp.bfloat16)
    else:
        q_ref = first_ref
    _, columns = q_ref.shape
    width = min(512, columns)
    blocks = columns // width
    kv_heads = lanes // HEAD_SIZE
    ones = jnp.ones((ONES_ROWS, HALF_KEYS), jnp.bfloat16)
    rows = HEAD_SIZE + ONES_ROWS
    halves = 0
    for chunk, (distance, first_half) in zip(chunks, pieces):
        source = ring_member(place + distance, sp_size)
        for half in range(chunk.shape[0]):
            row = source * grid_rows + (first_half + half) * (HALF_KEYS // GRID_W)
            keys_ref[halves] = rotation.ready(chunk[half, 0], row, 1.0).astype(jnp.bfloat16)
            turned = chunk[half, 1].astype(jnp.float32).T.astype(jnp.bfloat16)
            for head in range(kv_heads):
                values_ref[halves, head, :HEAD_SIZE, :] = turned[
                    head * HEAD_SIZE : (head + 1) * HEAD_SIZE
                ]
                values_ref[halves, head, HEAD_SIZE:, :] = ones
            halves += 1
    waiting = None
    for block in range(blocks + 1):
        weights = []
        total = None
        for half in range(halves):
            if block < blocks:
                scores = jnp.dot(
                    keys_ref[half],
                    q_ref[:, block * width : (block + 1) * width],
                    preferred_element_type=jnp.float32,
                )
                weights.append(jnp.exp2(scores).astype(jnp.bfloat16))
            if waiting is not None:
                kv_head = (block - 1) * kv_heads // blocks
                piece = jnp.dot(
                    values_ref[half, kv_head], waiting[half], preferred_element_type=jnp.float32
                )
                total = piece if total is None else total + piece
        if waiting is not None:
            at = (block - 1) * width
            if acc_in is not None:
                total = total + acc_in[:, at : at + width]
            if not last:
                outs[-1][:, at : at + width] = total
            else:
                turn = refs[2]
                tp, head_rows, per = turn.shape
                tok_count = tp * per
                ready = (total[:HEAD_SIZE] / total[HEAD_SIZE : HEAD_SIZE + 1]).astype(jnp.bfloat16)
                for piece in range(width // per):
                    head, spot = divmod(at + piece * per, tok_count)
                    turn[spot // per, head * HEAD_SIZE : (head + 1) * HEAD_SIZE, :] = ready[
                        :, piece * per : (piece + 1) * per
                    ]
        waiting = weights
    if last:
        me = lax.axis_index("tp")
        for rel, out in enumerate(outs):
            out[...] = refs[2][me ^ rel]


def attend(queries, tables, chunks, pieces, acc, sp_size, tp_size, last=False, after=()):
    raw_queries = acc is None
    lanes = chunks[0].shape[-1]
    rows = HEAD_SIZE + ONES_ROWS
    halves = sum(c.shape[0] for c in chunks)
    if raw_queries:
        columns = queries.shape[0] * queries.shape[1] // HEAD_SIZE
        tok_count = queries.shape[0]
    else:
        columns = queries.shape[1]
        tok_count = chunks[0].shape[0] * HALF_KEYS * 2
    scratch = [
        pltpu.VMEM((halves, HALF_KEYS, lanes), jnp.bfloat16),
        pltpu.VMEM((halves, lanes // HEAD_SIZE, rows, HALF_KEYS), jnp.bfloat16),
    ]
    if last:
        head_rows = columns // tok_count * HEAD_SIZE
        block = (head_rows, tok_count // tp_size)
        shape = [jax.ShapeDtypeStruct(block, jnp.bfloat16)] * tp_size
        scratch.append(pltpu.VMEM((tp_size, *block), jnp.bfloat16))
    else:
        shape = [jax.ShapeDtypeStruct((rows, columns), jnp.float32)]
        if raw_queries:
            shape = [jax.ShapeDtypeStruct((lanes, columns), jnp.bfloat16)] + shape
    operands = [queries, *tables, *chunks] + ([] if raw_queries else [acc])
    aliases = {} if (raw_queries or last) else {len(operands) - 1: 0}
    key_count = halves * HALF_KEYS
    return pl.pallas_call(
        functools.partial(attend_kernel, sp_size, pieces, last, raw_queries, len(after)),
        out_shape=shape,
        in_specs=[VMEM] * len(operands) + [HBM] * len(after),
        out_specs=[VMEM] * len(shape),
        scratch_shapes=scratch,
        input_output_aliases=aliases,
        cost_estimate=pl.CostEstimate(
            flops=2 * key_count * columns * 512,
            bytes_accessed=key_count * 1024,
            transcendentals=key_count * columns,
        ),
        compiler_params=pltpu.CompilerParams(vmem_limit_bytes=24 * 1024 * 1024),
    )(*operands, *after)


def direct_exchange(pieces, tp_size):
    held = {0: pieces[0]}
    for rel in reversed(range(1, tp_size)):
        held[rel] = lax.ppermute(pieces[rel], "tp", [(i, i ^ rel) for i in range(tp_size)])
    return [held[rel] for rel in range(tp_size)]


def out_kernel(tp_size, top_count, *refs):
    blocks = refs[:tp_size]
    w_ref, res_ref, mix_ref, norm_ref, table_ref = refs[tp_size : tp_size + 5]
    stream_ref, out_ref, normed_ref, mixed_ref = refs[tp_size + 5 :]
    me = lax.axis_index("tp")
    head_rows, row_count = blocks[0].shape
    width = w_ref.shape[1]
    step = min(512, width)
    turned = [b[...].astype(jnp.float32).T.astype(jnp.bfloat16) for b in blocks]
    power = jnp.zeros((row_count, 1), jnp.float32)
    for at in range(0, width, step):
        mixed = jnp.zeros((row_count, step), jnp.float32)
        for rel in range(tp_size):
            begin = pl.multiple_of((me ^ rel) * head_rows, head_rows)
            mixed = mixed + jnp.dot(
                turned[rel],
                w_ref[pl.ds(begin, head_rows), at : at + step],
                preferred_element_type=jnp.float32,
            )
        mixed_ref[:, at : at + step] = mixed
        power = power + jnp.sum(mixed * mixed, axis=1, keepdims=True)
    step = width
    scale = lax.rsqrt(power / width + epsilon)
    power = jnp.zeros((row_count, 1), jnp.float32)
    for at in range(0, width, step):
        cols = slice(at, at + step)
        stream = (
            res_ref[:, cols].astype(jnp.float32) + mixed_ref[:, cols] * scale * mix_ref[:, cols]
        ).astype(jnp.bfloat16)
        stream_ref[:, cols] = stream
        wide = stream.astype(jnp.float32)
        power = power + jnp.sum(wide * wide, axis=1, keepdims=True)
    scale = lax.rsqrt(power / width + epsilon)
    for at in range(0, width, step):
        cols = slice(at, at + step)
        wide = stream_ref[:, cols].astype(jnp.float32)
        normed_ref[:, cols] = (wide * scale * norm_ref[:, cols]).astype(jnp.bfloat16)
    fill_slots(top_count, normed_ref, table_ref, out_ref)


def routes_kernel(capacity, expert_ref, weight_ref, out_ref):
    row_count, top_count = expert_ref.shape
    lanes = out_ref.shape[1]
    lane = lax.broadcasted_iota(jnp.int32, (row_count, lanes), 1)
    before = lax.broadcasted_iota(jnp.int32, (row_count, row_count), 0) > (
        lax.broadcasted_iota(jnp.int32, (row_count, row_count), 1)
    )
    before = jnp.where(before, 1.0, 0.0).astype(jnp.bfloat16)
    taken = jnp.zeros((1, lanes), jnp.float32)
    table = jnp.zeros((row_count, lanes), jnp.float32)
    for k in range(top_count):
        expert = expert_ref[:, k : k + 1]
        onehot = jnp.where(lane == expert, 1.0, 0.0)
        earlier = taken + jnp.dot(
            before, onehot.astype(jnp.bfloat16), preferred_element_type=jnp.float32
        )
        rank = jnp.sum(onehot * earlier, axis=1, keepdims=True)
        slot = expert.astype(jnp.float32) * capacity + rank
        taken = taken + jnp.sum(onehot, axis=0, keepdims=True)
        table = jnp.where(lane == k, slot, table)
        table = jnp.where(lane == top_count + k, weight_ref[:, k : k + 1], table)
    out_ref[...] = table.T[: out_ref.shape[0], :row_count]


def fill_slots(top_count, rows_ref, table_ref, out_ref):
    row_count, width = rows_ref.shape
    step = min(512, width)
    slot_count = out_ref.shape[0]
    slots = lax.broadcasted_iota(jnp.int32, (slot_count, row_count), 0)
    slots = slots.astype(jnp.float32)
    hit = slots == table_ref[0:1, :]
    for k in range(1, top_count):
        hit = hit | (slots == table_ref[k : k + 1, :])
    placing = jnp.where(hit, 1.0, 0.0).astype(jnp.bfloat16)
    for at in range(0, width, step):
        cols = slice(at, at + step)
        out_ref[:, cols] = jnp.dot(
            placing, rows_ref[:, cols], preferred_element_type=jnp.float32
        ).astype(jnp.bfloat16)


def gather_kernel(top_count, base_ref, slots_ref, table_ref, out_hbm, out_ref, sems):
    row_count, width = base_ref.shape
    step = width // sems.shape[0]
    table = table_ref[...].T
    slots = lax.broadcasted_iota(jnp.int32, (row_count, slots_ref.shape[0]), 1)
    slots = slots.astype(jnp.float32)
    picks = [
        jnp.where(slots == table[:, k : k + 1], 1.0, 0.0).astype(jnp.bfloat16)
        for k in range(top_count)
    ]
    picks = jnp.concatenate(picks, axis=0)
    copies = []
    for i in range(sems.shape[0]):
        cols = pl.ds(i * step, step)
        rows = jnp.dot(picks, slots_ref[:, cols], preferred_element_type=jnp.float32)
        total = None
        for k in range(top_count):
            row = rows[k * row_count : (k + 1) * row_count]
            row = row * table[:, top_count + k : top_count + k + 1]
            total = row if total is None else total + row
        out_ref[:, cols] = (base_ref[:, cols].astype(jnp.float32) + total).astype(out_ref.dtype)
        copies.append(
            pltpu.make_async_copy(out_ref.at[:, cols], out_hbm.at[:, cols], sems.at[i])
        )
        copies[-1].start()
    for copy in copies:
        copy.wait()


def expert_kernel(rows_ref, gate_ref, up_ref, down_ref, out_ref, act_ref):
    hidden = gate_ref.shape[1]
    width = down_ref.shape[1]
    step = min(256, hidden)
    for at in range(0, hidden, step):
        cols = slice(at, at + step)
        gate = jnp.dot(rows_ref[...], gate_ref[:, cols], preferred_element_type=jnp.float32)
        up = jnp.dot(rows_ref[...], up_ref[:, cols], preferred_element_type=jnp.float32)
        act_ref[:, cols] = (gate / (1.0 + jnp.exp(-gate)) * up).astype(jnp.bfloat16)
    step = min(512, width)
    for at in range(0, width, step):
        cols = slice(at, at + step)
        out_ref[:, cols] = jnp.dot(
            act_ref[...], down_ref[:, cols], preferred_element_type=jnp.float32
        ).astype(jnp.bfloat16)


def local(
    sp_size,
    tp_size,
    query_proj,
    projected_keys,
    projected_values,
    residual,
    out_weight,
    mix_gain,
    norm_gain,
    route_expert,
    route_weight,
    expert_gate,
    expert_up,
    expert_down,
):
    tok_count, lanes = projected_keys.shape
    q_heads = query_proj.shape[1] // HEAD_SIZE
    model_width = residual.shape[1]
    halves = tok_count // HALF_KEYS
    tables = rotation_tables(sp_size * tok_count // GRID_W, lanes)
    raw_own = jnp.stack(
        [part.reshape(halves, HALF_KEYS, lanes) for part in (projected_keys, projected_values)],
        axis=1,
    )

    row_count = residual.shape[0]
    top_count = route_expert.shape[1]
    experts = sp_size * tp_size
    capacity = max(2, 2 * top_count * row_count // experts)
    slots_total = experts * capacity
    table = pl.pallas_call(
        functools.partial(routes_kernel, capacity),
        out_shape=jax.ShapeDtypeStruct((8, row_count), jnp.float32),
        in_specs=[VMEM] * 2,
        out_specs=VMEM,
        cost_estimate=pl.CostEstimate(flops=1 << 22, bytes_accessed=1 << 17, transcendentals=0),
        compiler_params=pltpu.CompilerParams(vmem_limit_bytes=8 * 1024 * 1024),
    )(route_expert, route_weight)

    order = list(range(0, sp_size, 2)) + list(range(sp_size - 1, 0, -2))
    ahead = [(order[i], order[(i + 1) % sp_size]) for i in range(sp_size)]
    behind = [(b, a) for a, b in ahead]
    steps = sp_size // 2
    acc = None
    queries = query_proj
    from_left = from_right = raw_own
    held, pieces = [raw_own], [(0, 0)]
    for step in range(steps):
        if step == steps - 1:
            from_left, from_right = from_left[: halves // 2], from_right[halves // 2 :]
        next_left = lax.ppermute(from_left, "sp", ahead)
        next_right = lax.ppermute(from_right, "sp", behind)
        after = (table,) if step == steps - 1 else ()
        out = attend(queries, tables, held, pieces, acc, sp_size, tp_size, after=after)
        if step == 0:
            queries, acc = out
        else:
            (acc,) = out
        from_left, from_right = next_left, next_right
        held = [from_left, from_right]
        pieces = [(-step - 1, 0), (step + 1, halves // 2 if step == steps - 1 else 0)]
    pieces = attend(queries, tables, held, pieces, acc, sp_size, tp_size, last=True)
    blocks = direct_exchange(pieces, tp_size)

    rows_shape = jax.ShapeDtypeStruct((row_count, model_width), jnp.bfloat16)
    slots_shape = jax.ShapeDtypeStruct((slots_total, model_width), jnp.bfloat16)
    stream, outgoing = pl.pallas_call(
        functools.partial(out_kernel, tp_size, top_count),
        out_shape=(rows_shape, slots_shape),
        in_specs=[VMEM] * (tp_size + 5),
        out_specs=(VMEM, VMEM),
        scratch_shapes=[
            pltpu.VMEM((row_count, model_width), jnp.bfloat16),
            pltpu.VMEM((row_count, model_width), jnp.float32),
        ],
        cost_estimate=pl.CostEstimate(
            flops=2 * row_count * model_width * (out_weight.shape[0] + slots_total),
            bytes_accessed=8 << 20,
            transcendentals=0,
        ),
        compiler_params=pltpu.CompilerParams(vmem_limit_bytes=12 * 1024 * 1024),
    )(*blocks, out_weight, residual, mix_gain[None, :], norm_gain[None, :], table)

    def exchange(slots):
        slots = slots.reshape(experts, capacity, model_width)
        slots = lax.all_to_all(slots, ("sp", "tp"), split_axis=0, concat_axis=0, tiled=True)
        return slots.reshape(slots_total, model_width)

    hidden = expert_gate.shape[2]
    done = pl.pallas_call(
        expert_kernel,
        out_shape=slots_shape,
        in_specs=[VMEM] * 4,
        out_specs=VMEM,
        scratch_shapes=[pltpu.VMEM((slots_total, hidden), jnp.bfloat16)],
        cost_estimate=pl.CostEstimate(
            flops=6 * slots_total * model_width * hidden,
            bytes_accessed=16 << 20,
            transcendentals=slots_total * hidden,
        ),
        compiler_params=pltpu.CompilerParams(vmem_limit_bytes=24 * 1024 * 1024),
    )(exchange(outgoing), expert_gate[0], expert_up[0], expert_down[0])
    return pl.pallas_call(
        functools.partial(gather_kernel, top_count),
        out_shape=rows_shape,
        in_specs=[VMEM] * 3,
        out_specs=HBM,
        scratch_shapes=[
            pltpu.VMEM((row_count, model_width), jnp.bfloat16),
            pltpu.SemaphoreType.DMA((4,)),
        ],
        cost_estimate=pl.CostEstimate(
            flops=4 * row_count * slots_total * model_width,
            bytes_accessed=3 << 20,
            transcendentals=0,
        ),
        compiler_params=pltpu.CompilerParams(vmem_limit_bytes=12 * 1024 * 1024),
    )(stream, exchange(done), table)


def solution(mesh):
    return jax.shard_map(
        functools.partial(local, mesh.shape["sp"], mesh.shape["tp"]),
        mesh=mesh,
        in_specs=(
            P("sp", "tp"),
            P("sp", "tp"),
            P("sp", "tp"),
            P(("sp", "tp"), None),
            P(),
            P(),
            P(),
            P(("sp", "tp"), None),
            P(("sp", "tp"), None),
            P(("sp", "tp"), None, None),
            P(("sp", "tp"), None, None),
            P(("sp", "tp"), None, None),
        ),
        out_specs=P(("sp", "tp"), None),
        check_vma=False,
    )
```
